128 devices in a mesh: rep: 2 (over z_hi), fs: 32 (over z_lo, y, x), tp: 2 (over core).
Axes of the slice: x: 4, y: 4, z: 4 (z_hi: 2, z_lo: 2; z = z_hi * 2 + z_lo), core: 2. Of those that a mesh axis runs over, the one named last changes fastest.
Arguments:
- tokens: bfloat16 [40960, 2048], P(('rep', 'fs', 'tp')), may hold values from -6 to 6
- mix_gain: float32 [2048], replicated, may hold values from 0.1 to 1.9
- w_bgate: bfloat16 [2048, 2048], P('fs', 'tp'), may hold values from -0.125 to 0.125
- w_cgate: bfloat16 [2048, 2048], P('fs', 'tp'), may hold values from -0.125 to 0.125
- w_value: bfloat16 [2048, 2048], P('fs', 'tp'), may hold values from -0.125 to 0.125
- conv_taps: float32 [3, 2048], replicated, may hold values from -3 to 3
- w_mixout: bfloat16 [2048, 2048], P('tp', 'fs'), may hold values from -0.125 to 0.125
- mlp_gain: float32 [2048], replicated, may hold values from 0.1 to 1.9
- w_gate: bfloat16 [2048, 2816], P('fs', 'tp'), may hold values from -0.125 to 0.125
- w_up: bfloat16 [2048, 2816], P('fs', 'tp'), may hold values from -0.125 to 0.125
- w_down: bfloat16 [2816, 2048], P('tp', 'fs'), may hold values from -0.109375 to 0.109375
Outputs:
- block_out: bfloat16 [40960, 2048], P(('rep', 'fs', 'tp'))
The draws below stay inside these ranges and needn't reach their ends.
All inputs are finite; a program needn't handle non-finite values.
Results may differ from the reference program's by a relative error of at most 0.0085.
Values may be sent and summed in bfloat16 or wider, within the bound.
A program may use at most 128 MiB of HBM per device.

```python
import jax
import jax.numpy as jnp
from jax import lax

D = 2048
FF = 2816
LENGTH = 640
TOKENS = 40960
N_TP = 2


def block_scale(key, extent, split, least, top_value):
    level, own = 1.0, jax.random.fold_in(key, 6)
    for dim, blocks in split:
        steps = jnp.exp(jax.random.uniform(jax.random.fold_in(own, dim), (blocks,), jnp.float32, least / len(split), top_value / len(split)))
        level = level * jnp.repeat(steps, extent[dim] // blocks).reshape([-1 if axis == dim else 1 for axis in range(len(extent))])
    return level


def centred(own_key, extent, width, bound, cuts=(), dtype=jnp.bfloat16):
    drawn = jax.random.normal(own_key, extent, jnp.float32) * width
    if len(cuts) > 0:
        drawn = block_scale(own_key, extent, cuts, -0.22, 0.18) * drawn
    return jnp.clip(drawn, min=-bound, max=bound).astype(dtype)


def setup_inputs(seed: int = 0) -> dict:
    key_of = jax.random.split(jax.random.key(seed), 12)
    tokens = centred(key_of[0], (TOKENS, D), 1.0, 6.0, ((0, 128),))
    mix_gain = jnp.clip(1.0 + 0.18 * jax.random.normal(key_of[1], (D,), jnp.float32), 0.1, 1.9)
    w_bgate = centred(key_of[2], (D, D), D ** -0.5, 0.125, ((0, 32), (1, 2)))
    w_cgate = centred(key_of[3], (D, D), D ** -0.5, 0.125, ((0, 32), (1, 2)))
    w_value = centred(key_of[4], (D, D), D ** -0.5, 0.125, ((0, 32), (1, 2)))
    conv_taps = centred(key_of[5], (3, D), 0.6, 3.0, (), jnp.float32)
    w_mixout = centred(key_of[6], (D, D), D ** -0.5, 0.125, ((0, 2), (1, 32)))
    mlp_gain = jnp.clip(1.0 + 0.18 * jax.random.normal(key_of[7], (D,), jnp.float32), 0.1, 1.9)
    w_gate = centred(key_of[8], (D, FF), D ** -0.5, 0.125, ((0, 32), (1, 2)))
    w_up = centred(key_of[9], (D, FF), D ** -0.5, 0.125, ((0, 32), (1, 2)))
    w_down = centred(key_of[10], (FF, D), FF ** -0.5, 0.109375, ((0, 2), (1, 32)))
    return {"tokens": tokens, "mix_gain": mix_gain, "w_bgate": w_bgate, "w_cgate": w_cgate, "w_value": w_value, "conv_taps": conv_taps, "w_mixout": w_mixout, "mlp_gain": mlp_gain, "w_gate": w_gate, "w_up": w_up, "w_down": w_down}


def rms_scale(matrix, gain):
    values = matrix.astype(jnp.float32)
    factor = lax.rsqrt(lax.optimization_barrier(jnp.mean(values * values, axis=-1, keepdims=True)) + 1e-06)
    return values * factor * gain.astype(jnp.float32)

def causal_taps(mixed, filters):
    length = mixed.shape[-2]
    widths = [(0, 0)] * (mixed.ndim - 2) + [(2, 0), (0, 0)]
    padded = jnp.pad(mixed, widths)
    return filters[0] * padded[..., 0:length, :] + filters[1] * padded[..., 1:length + 1, :] + filters[2] * padded[..., 2:length + 2, :]

def split_sum(left, right):
    portion = left.shape[1] // N_TP
    running = jnp.zeros((left.shape[0], right.shape[1]), jnp.float32)
    for member in range(N_TP):
        partial_out = jnp.dot(left[:, member * portion:(member + 1) * portion], right[member * portion:(member + 1) * portion], preferred_element_type=jnp.float32)
        partial_out = lax.optimization_barrier(partial_out.astype(jnp.bfloat16))
        running = running + partial_out.astype(jnp.float32)
    return running

def reference(tokens, mix_gain, w_bgate, w_cgate, w_value, conv_taps, w_mixout, mlp_gain, w_gate, w_up, w_down):
    normed = rms_scale(tokens, mix_gain).astype(jnp.bfloat16)
    b_proj = jnp.dot(normed, w_bgate, preferred_element_type=jnp.float32).astype(jnp.bfloat16)
    c_proj = jnp.dot(normed, w_cgate, preferred_element_type=jnp.float32).astype(jnp.bfloat16)
    u_proj = jnp.dot(normed, w_value, preferred_element_type=jnp.float32).astype(jnp.bfloat16)
    mixed_in = c_proj.astype(jnp.float32) * u_proj.astype(jnp.float32)
    mixed_in = mixed_in.reshape(TOKENS // LENGTH, LENGTH, D)
    convolved = causal_taps(mixed_in, conv_taps).reshape(TOKENS, D)
    gated = (b_proj.astype(jnp.float32) * convolved).astype(jnp.bfloat16)
    residual = tokens.astype(jnp.float32) + split_sum(gated, w_mixout)
    normed_two = rms_scale(residual, mlp_gain).astype(jnp.bfloat16)
    gate = jnp.dot(normed_two, w_gate, preferred_element_type=jnp.float32)
    up_value = jnp.dot(normed_two, w_up, preferred_element_type=jnp.float32)
    hidden = (jax.nn.silu(gate) * up_value).astype(jnp.bfloat16)
    return (residual + 0.5 * split_sum(hidden, w_down)).astype(jnp.bfloat16)
```

```python
import functools
import heapq

import jax
import jax.numpy as jnp
from jax import lax
from jax.experimental import pallas as pl
from jax.experimental.pallas import tpu as pltpu
from jax.sharding import Mesh
from jax.sharding import PartitionSpec as P

FS = ("fs_0", "fs_1", "fs_2")
REP_FS_TP = ("rep", "fs_0", "fs_1", "fs_2", "tp")
MESH = pl.DeviceIdType.MESH
BF16, F32 = jnp.bfloat16, jnp.float32

D = 2048
T = 640
H = 320
WIDTHS = (3072, 1024, 2816, 1408)
LINK = 46.0e3
LATENCY = 2.6
BACKLOG = 7.0

ALL = ("all",)
ME = ("rel", 0)


def half(k):
    return ("half", k)


def rel(k):
    return ("rel", k)


class Send:
    def __init__(self, stage, quarter, way, at, needs, rank, pieces):
        self.stage, self.quarter, self.way, self.at = stage, quarter, way, at
        self.needs, self.rank = needs, rank
        self.time = pieces * 16 * WIDTHS[stage] * 2 / LINK


def sends_of(stage):
    out = []

    def add(quarter, way, at, needs, rank, pieces):
        send = Send(stage, quarter, way, {"z": ME, "y": ME, "x": ME} | at, needs, rank, pieces)
        out.append(send)
        return send

    for quarter, (first, second) in enumerate((("x", "y"), ("y", "x"), ("x", "y"), ("y", "x"))):
        forth, back = first + "+", first + "-"
        plus = add(quarter, forth, {}, [], 0, 1)
        minus = add(quarter, back, {}, [], 0, 1)
        if quarter % 4 < 2:
            on = add(quarter, forth, {first: rel(-1)}, [plus], 1, 1)
        else:
            on = add(quarter, back, {first: rel(1)}, [minus], 1, 1)
        line = [plus, minus, on]
        forth, back = second + "+", second + "-"
        if quarter < 2:
            pa = add(quarter, forth, {first: half(0)}, line, 2, 2)
            pb = add(quarter, forth, {first: half(1)}, line, 3, 2)
            ma = add(quarter, back, {first: half(1)}, line, 2, 2)
            mb = add(quarter, back, {first: half(0)}, line, 3, 2)
            po = add(quarter, forth, {first: half(0), second: rel(-1)}, [pa], 4, 2)
            mo = add(quarter, back, {first: half(1), second: rel(1)}, [ma], 4, 2)
            add(quarter, "z+", {first: ALL}, line, 5, 4)
            add(quarter, "z+", {first: ALL, second: rel(-1)}, [pa, pb], 6, 4)
            add(quarter, "z-", {first: ALL, second: rel(1)}, [ma, mb], 6, 4)
            add(quarter, "z-", {first: ALL, second: rel(2)}, [po, mo], 7, 4)
        else:
            zp = add(quarter, "z+", {first: half(0)}, line, 2, 2)
            zm = add(quarter, "z-", {first: half(1)}, line, 2, 2)
            here, there = {first: ALL}, {first: ALL, "z": rel(1)}
            ph = add(quarter, forth, here, line, 3, 4)
            add(quarter, back, here, line, 3, 4)
            add(quarter, forth, there, [zp, zm], 4, 4)
            mt = add(quarter, back, there, [zp, zm], 4, 4)
            add(quarter, forth, here | {second: rel(-1)}, [ph], 5, 4)
            add(quarter, back, there | {second: rel(1)}, [mt], 5, 4)
    return out


def work_list():
    work = [("norm", 0, 4.0, None)]
    work += [("mix", j, 3.2, 0) for j in range(4)]
    work += [("out", j, 1.7, 1) for j in range(2)]
    work += [("again", 0, 5.0, None)]
    work += [("hide", j, 2.5, 2) for j in range(4)]
    return work


def plan():
    sends = [send for stage in range(4) for send in sends_of(stage)]
    waiting = sorted(range(len(sends)), key=lambda i: (sends[i].stage, sends[i].rank))
    number = {id(send): i for i, send in enumerate(sends)}
    left = [sum(send.stage == stage for send in sends) for stage in range(4)]
    free, arrived, flying, steps, now = {}, set(), [], [], 0.0
    work = work_list()

    def top_up():
        for i in list(waiting):
            send = sends[i]
            if free.get(send.way, 0.0) - now > BACKLOG:
                continue
            if all(number[id(need)] in arrived for need in send.needs):
                begin = max(free.get(send.way, 0.0), now)
                free[send.way] = begin + send.time
                heapq.heappush(flying, (free[send.way] + LATENCY, i))
                steps.append(("start", i))
                waiting.remove(i)

    top_up()
    while flying or work:
        while flying and flying[0][0] <= now:
            i = heapq.heappop(flying)[1]
            arrived.add(i)
            left[sends[i].stage] -= 1
            steps.append(("wait", i))
            top_up()
        if work and (work[0][3] is None or left[work[0][3]] == 0):
            name, j, time, _ = work.pop(0)
            steps.append((name, j))
            now += time
        elif flying:
            now = max(now, flying[0][0])
    return sends, steps, now


def region(send, place):
    at = []
    for dim, extent in (("z", 2), ("y", 4), ("x", 4)):
        how = send.at[dim]
        if how == ALL:
            at.append(pl.ds(0, extent))
        elif how[0] == "half":
            at.append(pl.ds(2 * how[1], 2))
        else:
            at.append(pl.ds(lax.rem(place[dim] + how[1] + extent, extent), 1))
    return (*at, pl.ds(16 * send.quarter, 16), pl.ds(0, WIDTHS[send.stage]))


def kernel(
    tokens, gain_one, w_b, w_c, w_v, taps, w_mix, gain_two, w_g, w_u, w_d, out,
    s0, s1, s2, s3, raw, normed, gated, part, came, came_two, resid, hidden, result,
    gain_v, taps_v, gain_two_v, acc_b, acc_c,
    local_sem, send_sem, recv_sem, pair_send, pair_recv,
):
    sends, steps, _ = plan()
    buffers = (s0, s1, s2, s3)
    rep, zl, y, x, tp = (lax.axis_index(name) for name in REP_FS_TP)
    me = {"z": zl, "y": y, "x": x}
    z = rep * 2 + zl

    def device(way):
        step = 1 if way[1] == "+" else 3
        if way[0] == "x":
            return (rep, zl, y, lax.rem(x + step, 4), tp)
        if way[0] == "y":
            return (rep, zl, lax.rem(y + step, 4), x, tp)
        there = lax.rem(z + step, 4)
        return (there // 2, lax.rem(there, 2), y, x, tp)

    partner = (rep, zl, y, x, 1 - tp)
    mine = pl.ds(pl.multiple_of(tp * H, H), H)
    other = pl.ds(pl.multiple_of((1 - tp) * H, H), H)

    def local(k, src, dst):
        return pltpu.make_async_copy(src, dst, local_sem.at[k])

    def slot(buffer, lo, n):
        return buffer.at[zl, y, x, pl.ds(0, 64), pl.ds(lo, n)]

    locals_ = [
        local(0, w_b, slot(s0, 0, 1024)),
        local(1, w_c, slot(s0, 1024, 1024)),
        local(2, w_v, slot(s0, 2048, 1024)),
        local(3, w_mix, slot(s1, 0, 1024)),
        local(4, w_g, slot(s2, 0, 1408)),
        local(5, w_u, slot(s2, 1408, 1408)),
        local(6, w_d, slot(s3, 0, 1408)),
        local(7, tokens, raw.at[mine, :]),
        local(8, gain_one, gain_v),
        local(9, taps, taps_v),
        local(10, gain_two, gain_two_v),
    ]
    ready_of = ((0, 1, 2), (3,), (4, 5), (6,))
    for copy in locals_:
        copy.start()

    barrier = pltpu.get_barrier_semaphore()
    greeted = [device(way) for way in ("x+", "x-", "y+", "y-", "z+", "z-")] + [partner]
    for peer in greeted:
        pl.semaphore_signal(barrier, inc=1, device_id=peer, device_id_type=MESH)
    pl.semaphore_wait(barrier, len(greeted))

    def to_partner(k, src, dst):
        return pltpu.make_async_remote_copy(
            src_ref=src, dst_ref=dst, send_sem=pair_send.at[k], recv_sem=pair_recv.at[k],
            device_id=partner, device_id_type=MESH,
        )

    def tokens_out():
        return to_partner(0, tokens, raw.at[mine, :])

    def tokens_in():
        return to_partner(0, tokens, raw.at[other, :])

    tokens_out().start()

    def outgoing(i):
        send = sends[i]
        where = buffers[send.stage].at[region(send, me)]
        return pltpu.make_async_remote_copy(
            src_ref=where, dst_ref=where, send_sem=send_sem.at[i], recv_sem=recv_sem.at[i],
            device_id=device(send.way), device_id_type=MESH,
        )

    def incoming(i):
        send = sends[i]
        back = send.way[0]
        place = dict(me)
        extent = 2 if back == "z" else 4
        place[back] = lax.rem(me[back] + (extent - 1 if send.way[1] == "+" else 1), extent)
        where = buffers[send.stage].at[region(send, place)]
        return pltpu.make_async_remote_copy(
            src_ref=where, dst_ref=where, send_sem=send_sem.at[i], recv_sem=recv_sem.at[i],
            device_id=device(send.way), device_id_type=MESH,
        )

    def scaled(values, gain):
        factor = lax.rsqrt(jnp.mean(values * values, axis=-1, keepdims=True) + 1e-06)
        return (values * factor * gain).astype(BF16)

    def norm(_):
        locals_[7].wait()
        locals_[8].wait()
        tokens_in().wait_recv()
        gain = gain_v[...]

        def chunk(r, carry):
            rows = pl.ds(pl.multiple_of(r * 32, 32), 32)
            normed[rows, :] = scaled(raw[rows, :].astype(F32), gain)
            return carry

        lax.fori_loop(0, T // 32, chunk, 0)

    def mix(j):
        if j == 0:
            locals_[9].wait()

        def columns(k):
            return s0[:, :, :, :, pl.ds(1024 * k + 256 * j, 256)].reshape(D, 256)

        def dot(k):
            return jnp.dot(normed[...], columns(k), preferred_element_type=F32).astype(BF16)

        acc_b[...] = dot(0)
        acc_c[...] = dot(1)
        mixed = acc_c[...].astype(F32) * dot(2).astype(F32)
        row = lax.broadcasted_iota(jnp.int32, (T, 256), 0)
        one = jnp.where(row >= 1, pltpu.roll(mixed, 1, 0), 0.0)
        two = jnp.where(row >= 2, pltpu.roll(mixed, 2, 0), 0.0)
        lanes = pl.ds(pl.multiple_of(tp * 1024 + 256 * j, 256), 256)
        tap = [taps_v[pl.ds(k, 1), lanes] for k in range(3)]
        convolved = tap[0] * two + tap[1] * one + tap[2] * mixed
        gated[:, pl.ds(256 * j, 256)] = (acc_b[...].astype(F32) * convolved).astype(BF16)

    def block(left, right):
        return lax.dot_general(
            left, right, (((1,), (1,)), ((), ())), preferred_element_type=F32
        ).astype(BF16)

    def part_out(j):
        cols = pl.ds(1024 * j, 1024)
        return to_partner(1 + j, part.at[:, cols], came.at[:, cols])

    def out_proj(j):
        def one(k, carry):
            cols = pl.ds(pl.multiple_of(1024 * j + 256 * k, 256), 256)
            part[:, cols] = block(gated[...], s1[j, k].reshape(256, 1024))
            return carry

        lax.fori_loop(0, 4, one, 0)
        part_out(j).start()

    def again(_):
        locals_[10].wait()
        part_out(0).wait_recv()
        part_out(1).wait_recv()
        gain = gain_two_v[...]

        def total(rows):
            sums = part[rows, :].astype(F32) + came[rows, :].astype(F32)
            return raw[rows, :].astype(F32) + sums

        def own(r, carry):
            rows = pl.ds(pl.multiple_of(tp * H + r * 32, 32), 32)
            values = total(rows)
            resid[pl.ds(pl.multiple_of(r * 32, 32), 32), :] = values
            normed[rows, :] = scaled(values, gain)
            return carry

        def others(r, carry):
            rows = pl.ds(pl.multiple_of((1 - tp) * H + r * 32, 32), 32)
            normed[rows, :] = scaled(total(rows), gain)
            return carry

        lax.fori_loop(0, H // 32, own, 0)
        lax.fori_loop(0, H // 32, others, 0)

    def hide(j):
        lo, n = ((0, 2), (2, 3), (5, 3), (8, 3))[j]

        def one(k, carry):
            at = pl.multiple_of(128 * (lo + k), 128)
            w_gate = s2[:, :, :, :, pl.ds(at, 128)].reshape(D, 128)
            w_up = s2[:, :, :, :, pl.ds(pl.multiple_of(at + 1408, 128), 128)].reshape(D, 128)
            both = jnp.dot(
                normed[...], jnp.concatenate([w_gate, w_up], axis=1), preferred_element_type=F32
            )
            gate, up = both[:, :128], both[:, 128:]
            hidden[:, pl.ds(at, 128)] = (gate / (1.0 + jnp.exp(-gate)) * up).astype(BF16)
            return carry

        lax.fori_loop(0, n, one, 0)

    act = {"norm": norm, "mix": mix, "out": out_proj, "again": again, "hide": hide}
    landed = set()
    for what, i in steps:
        if what == "start":
            stage = sends[i].stage
            if stage not in landed:
                landed.add(stage)
                for k in ready_of[stage]:
                    locals_[k].wait()
            outgoing(i).start()
        elif what == "wait":
            incoming(i).wait_recv()
        else:
            act[what](i)

    part_out(0).wait_send()
    part_out(1).wait_send()

    def down_out(k):
        cols = pl.ds(256 * k, 256)
        return to_partner(3 + k, part.at[other, cols], came_two.at[:, cols])

    for k in range(8):
        cols = pl.ds(256 * k, 256)
        part[:, cols] = block(hidden[...], s3[k // 4, k % 4].reshape(256, 1408))
        down_out(k).start()
    for k in range(8):
        cols = pl.ds(256 * k, 256)
        down_out(k).wait_recv()
        sums = part[mine, cols].astype(F32) + came_two[:, cols].astype(F32)
        result[:, cols] = (resid[:, cols] + 0.5 * sums).astype(BF16)
    done = local(0, result, out)
    done.start()
    for i in range(len(sends)):
        outgoing(i).wait_send()
    tokens_out().wait_send()
    for k in range(8):
        down_out(k).wait_send()
    done.wait()


def on_device(
    tokens, mix_gain, w_bgate, w_cgate, w_value, conv_taps, w_mixout, mlp_gain, w_gate, w_up, w_down
):
    count = len(plan()[0])
    anywhere = pl.BlockSpec(memory_space=pl.ANY)
    return pl.pallas_call(
        kernel,
        name="residual_block",
        out_shape=jax.ShapeDtypeStruct((H, D), BF16),
        in_specs=[anywhere] * 11,
        out_specs=anywhere,
        scratch_shapes=[
            *[pltpu.VMEM((2, 4, 4, 64, width), BF16) for width in WIDTHS],
            pltpu.VMEM((T, D), BF16),
            pltpu.VMEM((T, D), BF16),
            pltpu.VMEM((T, 1024), BF16),
            pltpu.VMEM((T, D), BF16),
            pltpu.VMEM((T, D), BF16),
            pltpu.VMEM((H, D), BF16),
            pltpu.VMEM((H, D), F32),
            pltpu.VMEM((T, 1408), BF16),
            pltpu.VMEM((H, D), BF16),
            pltpu.VMEM((1, D), F32),
            pltpu.VMEM((3, D), F32),
            pltpu.VMEM((1, D), F32),
            pltpu.VMEM((T, 256), BF16),
            pltpu.VMEM((T, 256), BF16),
            pltpu.SemaphoreType.DMA((11,)),
            pltpu.SemaphoreType.DMA((count,)),
            pltpu.SemaphoreType.DMA((count,)),
            pltpu.SemaphoreType.DMA((11,)),
            pltpu.SemaphoreType.DMA((11,)),
        ],
        compiler_params=pltpu.CompilerParams(
            collective_id=0, has_side_effects=True, vmem_limit_bytes=67043328
        ),
    )(
        tokens, mix_gain[None], w_bgate, w_cgate, w_value, conv_taps, w_mixout.T,
        mlp_gain[None], w_gate, w_up, w_down.T,
    )


def solution(mesh):
    finer = Mesh(
        mesh.devices.reshape(mesh.shape["rep"], 2, 4, 4, mesh.shape["tp"]),
        ("rep", "fs_0", "fs_1", "fs_2", "tp"),
    )
    return jax.shard_map(
        on_device,
        mesh=finer,
        in_specs=(
            P(REP_FS_TP, None),
            P(),
            P(FS, "tp"),
            P(FS, "tp"),
            P(FS, "tp"),
            P(),
            P("tp", FS),
            P(),
            P(FS, "tp"),
            P(FS, "tp"),
            P("tp", FS),
        ),
        out_specs=P(REP_FS_TP, None),
        check_vma=False,
    )
```

```python
import functools
import heapq

import jax
import jax.numpy as jnp
from jax import lax
from jax.experimental import pallas as pl
from jax.experimental.pallas import tpu as pltpu
from jax.sharding import Mesh
from jax.sharding import PartitionSpec as P

FS = ("fs_0", "fs_1", "fs_2")
REP_FS_TP = ("rep", "fs_0", "fs_1", "fs_2", "tp")
MESH = pl.DeviceIdType.MESH
BF16, F32 = jnp.bfloat16, jnp.float32

D = 2048
T = 640
H = 320
WIDTHS = (3072, 1024, 2816, 1408)
LINK = 45.6e3
LATENCY = 2.6
BACKLOG = 7.0

ALL = ("all",)
ME = ("rel", 0)


def half(k):
    return ("half", k)


def rel(k):
    return ("rel", k)


class Send:
    def __init__(self, stage, quarter, way, at, needs, rank, pieces):
        self.stage, self.quarter, self.way, self.at = stage, quarter, way, at
        self.needs, self.rank = needs, rank
        self.time = pieces * 16 * WIDTHS[stage] * 2 / LINK


def sends_of(stage):
    out = []

    def add(quarter, way, at, needs, rank, pieces):
        send = Send(stage, quarter, way, {"z": ME, "y": ME, "x": ME} | at, needs, rank, pieces)
        out.append(send)
        return send

    for quarter, (first, second) in enumerate((("x", "y"), ("y", "x"), ("x", "y"), ("y", "x"))):
        forth, back = first + "+", first + "-"
        plus = add(quarter, forth, {}, [], 0, 1)
        minus = add(quarter, back, {}, [], 0, 1)
        if quarter % 4 < 2:
            on = add(quarter, forth, {first: rel(-1)}, [plus], 1, 1)
        else:
            on = add(quarter, back, {first: rel(1)}, [minus], 1, 1)
        line = [plus, minus, on]
        forth, back = second + "+", second + "-"
        if quarter < 2:
            pa = add(quarter, forth, {first: half(0)}, line, 2, 2)
            pb = add(quarter, forth, {first: half(1)}, line, 3, 2)
            ma = add(quarter, back, {first: half(1)}, line, 2, 2)
            mb = add(quarter, back, {first: half(0)}, line, 3, 2)
            po = add(quarter, forth, {first: half(0), second: rel(-1)}, [pa], 4, 2)
            mo = add(quarter, back, {first: half(1), second: rel(1)}, [ma], 4, 2)
            up, down = ("z+", "z-") if quarter == 0 else ("z-", "z+")
            add(quarter, up, {}, [], 0, 1)
            add(quarter, up, {first: rel(-1)}, [plus], 2, 1)
            add(quarter, up, {first: rel(1)}, [minus], 2, 1)
            add(quarter, up, {first: rel(2)}, [on], 2, 1)
            add(quarter, up, {first: ALL, second: rel(-1)}, [pa, pb], 6, 4)
            add(quarter, down, {first: ALL, second: rel(1)}, [ma, mb], 6, 4)
            add(quarter, down, {first: ALL, second: rel(2)}, [po, mo], 7, 4)
        else:
            zp = add(quarter, "z+", {first: half(0)}, line, 2, 2)
            zm = add(quarter, "z-", {first: half(1)}, line, 2, 2)
            here, there = {first: ALL}, {first: ALL, "z": rel(1)}
            ph = add(quarter, forth, here, line, 3, 4)
            add(quarter, back, here, line, 3, 4)
            add(quarter, forth, there, [zp, zm], 4, 4)
            mt = add(quarter, back, there, [zp, zm], 4, 4)
            add(quarter, forth, here | {second: rel(-1)}, [ph], 5, 4)
            add(quarter, back, there | {second: rel(1)}, [mt], 5, 4)
    return out


def near(send):
    return (send.way[0] == "z") == (send.at["z"] != ME)


def work_list():
    work = [("norm", 0, 4.0, None)]
    work += [("mix", j, 3.2, 0) for j in range(4)]
    work += [("out", j, 1.7, 1) for j in range(2)]
    work += [("again", 0, 5.0, None)]
    work += [("hide", j, 2.5, 2) for j in range(4)]
    work += [("down", 0, 3.0, 4), ("down", 1, 3.0, 3)]
    return work


def plan():
    sends = [send for stage in range(4) for send in sends_of(stage)]
    waiting = sorted(range(len(sends)), key=lambda i: (sends[i].stage, sends[i].rank))
    number = {id(send): i for i, send in enumerate(sends)}
    left = [sum(send.stage == stage for send in sends) for stage in range(4)]
    left.append(sum(send.stage == 3 and near(send) for send in sends))
    free, arrived, flying, steps, now = {}, set(), [], [], 0.0
    work = work_list()

    def top_up():
        for i in list(waiting):
            send = sends[i]
            if free.get(send.way, 0.0) - now > BACKLOG:
                continue
            if all(number[id(need)] in arrived for need in send.needs):
                begin = max(free.get(send.way, 0.0), now)
                free[send.way] = begin + send.time
                heapq.heappush(flying, (free[send.way] + LATENCY, i))
                steps.append(("start", i))
                waiting.remove(i)

    top_up()
    while flying or work:
        while flying and flying[0][0] <= now:
            i = heapq.heappop(flying)[1]
            arrived.add(i)
            left[sends[i].stage] -= 1
            left[4] -= sends[i].stage == 3 and near(sends[i])
            steps.append(("wait", i))
            top_up()
        if work and (work[0][3] is None or left[work[0][3]] == 0):
            name, j, time, _ = work.pop(0)
            steps.append((name, j))
            now += time
        elif flying:
            now = max(now, flying[0][0])
    return sends, steps, now


def region(send, place):
    at = []
    for dim, extent in (("z", 2), ("y", 4), ("x", 4)):
        how = send.at[dim]
        if how == ALL:
            at.append(pl.ds(0, extent))
        elif how[0] == "half":
            at.append(pl.ds(2 * how[1], 2))
        else:
            at.append(pl.ds(lax.rem(place[dim] + how[1] + extent, extent), 1))
    return (*at, pl.ds(16 * send.quarter, 16), pl.ds(0, WIDTHS[send.stage]))


def kernel(
    tokens, gain_one, w_b, w_c, w_v, taps, w_mix, gain_two, w_g, w_u, w_d, total, came_two,
    s0, s1, s2, s3, raw, normed, gated, part, came, resid, hidden,
    gain_v, taps_v, gain_two_v, acc_b, acc_c,
    local_sem, send_sem, recv_sem, pair_send, pair_recv,
):
    sends, steps, _ = plan()
    buffers = (s0, s1, s2, s3)
    rep, zl, y, x, tp = (lax.axis_index(name) for name in REP_FS_TP)
    me = {"z": zl, "y": y, "x": x}
    z = rep * 2 + zl

    def device(way):
        step = 1 if way[1] == "+" else 3
        if way[0] == "x":
            return (rep, zl, y, lax.rem(x + step, 4), tp)
        if way[0] == "y":
            return (rep, zl, lax.rem(y + step, 4), x, tp)
        there = lax.rem(z + step, 4)
        return (there // 2, lax.rem(there, 2), y, x, tp)

    partner = (rep, zl, y, x, 1 - tp)
    mine = pl.ds(pl.multiple_of(tp * H, H), H)
    other = pl.ds(pl.multiple_of((1 - tp) * H, H), H)

    def local(k, src, dst):
        return pltpu.make_async_copy(src, dst, local_sem.at[k])

    def slot(buffer, lo, n):
        return buffer.at[zl, y, x, pl.ds(0, 64), pl.ds(lo, n)]

    locals_ = [
        local(0, w_b, slot(s0, 0, 1024)),
        local(1, w_c, slot(s0, 1024, 1024)),
        local(2, w_v, slot(s0, 2048, 1024)),
        local(3, w_mix, slot(s1, 0, 1024)),
        local(4, w_g, slot(s2, 0, 1408)),
        local(5, w_u, slot(s2, 1408, 1408)),
        local(6, w_d, slot(s3, 0, 1408)),
        local(7, tokens, raw.at[mine, :]),
        local(8, gain_one, gain_v),
        local(9, taps, taps_v),
        local(10, gain_two, gain_two_v),
    ]
    ready_of = ((0, 1, 2), (3,), (4, 5), (6,))
    for copy in locals_:
        copy.start()

    barrier = pltpu.get_barrier_semaphore()
    greeted = [device(way) for way in ("x+", "x-", "y+", "y-", "z+", "z-")] + [partner]
    for peer in greeted:
        pl.semaphore_signal(barrier, inc=1, device_id=peer, device_id_type=MESH)
    pl.semaphore_wait(barrier, len(greeted))

    def to_partner(k, src, dst):
        return pltpu.make_async_remote_copy(
            src_ref=src, dst_ref=dst, send_sem=pair_send.at[k], recv_sem=pair_recv.at[k],
            device_id=partner, device_id_type=MESH,
        )

    def tokens_out():
        return to_partner(0, tokens, raw.at[mine, :])

    def tokens_in():
        return to_partner(0, tokens, raw.at[other, :])

    tokens_out().start()

    def outgoing(i):
        send = sends[i]
        where = buffers[send.stage].at[region(send, me)]
        return pltpu.make_async_remote_copy(
            src_ref=where, dst_ref=where, send_sem=send_sem.at[i], recv_sem=recv_sem.at[i],
            device_id=device(send.way), device_id_type=MESH,
        )

    def incoming(i):
        send = sends[i]
        back = send.way[0]
        place = dict(me)
        extent = 2 if back == "z" else 4
        place[back] = lax.rem(me[back] + (extent - 1 if send.way[1] == "+" else 1), extent)
        where = buffers[send.stage].at[region(send, place)]
        return pltpu.make_async_remote_copy(
            src_ref=where, dst_ref=where, send_sem=send_sem.at[i], recv_sem=recv_sem.at[i],
            device_id=device(send.way), device_id_type=MESH,
        )

    def scaled(values, gain):
        factor = lax.rsqrt(jnp.mean(values * values, axis=-1, keepdims=True) + 1e-06)
        return (values * factor * gain).astype(BF16)

    def norm(_):
        locals_[7].wait()
        locals_[8].wait()
        tokens_in().wait_recv()
        gain = gain_v[...]

        def chunk(r, carry):
            rows = pl.ds(pl.multiple_of(r * 32, 32), 32)
            normed[rows, :] = scaled(raw[rows, :].astype(F32), gain)
            return carry

        lax.fori_loop(0, T // 32, chunk, 0)

    def mix(j):
        if j == 0:
            locals_[9].wait()

        def columns(k):
            return s0[:, :, :, :, pl.ds(1024 * k + 256 * j, 256)].reshape(D, 256)

        def dot(k):
            return jnp.dot(normed[...], columns(k), preferred_element_type=F32).astype(BF16)

        acc_b[...] = dot(0)
        acc_c[...] = dot(1)
        mixed = acc_c[...].astype(F32) * dot(2).astype(F32)
        row = lax.broadcasted_iota(jnp.int32, (T, 256), 0)
        one = jnp.where(row >= 1, pltpu.roll(mixed, 1, 0), 0.0)
        two = jnp.where(row >= 2, pltpu.roll(mixed, 2, 0), 0.0)
        lanes = pl.ds(pl.multiple_of(tp * 1024 + 256 * j, 256), 256)
        tap = [taps_v[pl.ds(k, 1), lanes] for k in range(3)]
        convolved = tap[0] * two + tap[1] * one + tap[2] * mixed
        gated[:, pl.ds(256 * j, 256)] = (acc_b[...].astype(F32) * convolved).astype(BF16)

    def block(left, right):
        return lax.dot_general(
            left, right, (((1,), (1,)), ((), ())), preferred_element_type=F32
        ).astype(BF16)

    def part_out(j):
        cols = pl.ds(1024 * j, 1024)
        return to_partner(1 + j, part.at[:, cols], came.at[:, cols])

    def out_proj(j):
        def one(k, carry):
            cols = pl.ds(pl.multiple_of(1024 * j + 256 * k, 256), 256)
            part[:, cols] = block(gated[...], s1[j, k].reshape(256, 1024))
            return carry

        lax.fori_loop(0, 4, one, 0)
        part_out(j).start()

    def again(_):
        locals_[10].wait()
        part_out(0).wait_recv()
        part_out(1).wait_recv()
        gain = gain_two_v[...]

        def joined(rows):
            sums = part[rows, :].astype(F32) + came[rows, :].astype(F32)
            return raw[rows, :].astype(F32) + sums

        def own(r, carry):
            rows = pl.ds(pl.multiple_of(tp * H + r * 32, 32), 32)
            values = joined(rows)
            resid[pl.ds(pl.multiple_of(r * 32, 32), 32), :] = values
            normed[rows, :] = scaled(values, gain)
            return carry

        def others(r, carry):
            rows = pl.ds(pl.multiple_of((1 - tp) * H + r * 32, 32), 32)
            normed[rows, :] = scaled(joined(rows), gain)
            return carry

        lax.fori_loop(0, H // 32, own, 0)
        lax.fori_loop(0, H // 32, others, 0)

    def hide(j):
        lo, n = ((0, 2), (2, 3), (5, 3), (8, 3))[j]

        def one(k, carry):
            at = pl.multiple_of(128 * (lo + k), 128)
            w_gate = s2[:, :, :, :, pl.ds(at, 128)].reshape(D, 128)
            w_up = s2[:, :, :, :, pl.ds(pl.multiple_of(at + 1408, 128), 128)].reshape(D, 128)
            both = jnp.dot(
                normed[...], jnp.concatenate([w_gate, w_up], axis=1), preferred_element_type=F32
            )
            gate, up = both[:, :128], both[:, 128:]
            hidden[:, pl.ds(at, 128)] = (gate / (1.0 + jnp.exp(-gate)) * up).astype(BF16)
            return carry

        lax.fori_loop(0, n, one, 0)

    def half_of(j):
        return pl.ds(pl.multiple_of(1024 * lax.rem(zl + j, 2), 1024), 1024)

    def down_out(j):
        cols = half_of(j)
        return to_partner(3 + j, part.at[other, cols], came_two.at[:, cols])

    def down_home(j):
        cols = half_of(j)
        return local(j, resid.at[:, cols], total.at[:, cols])

    def down(j):
        plane = lax.rem(zl + j, 2)
        if j == 0:
            part_out(0).wait_send()
            part_out(1).wait_send()

        def theirs(k, carry):
            cols = pl.ds(pl.multiple_of(1024 * plane + 256 * k, 256), 256)
            part[other, cols] = block(hidden[other, :], s3[plane, k].reshape(256, 1408))
            return carry

        def ours(k, carry):
            cols = pl.ds(pl.multiple_of(1024 * plane + 256 * k, 256), 256)
            own = block(hidden[mine, :], s3[plane, k].reshape(256, 1408))
            resid[:, cols] = resid[:, cols] + 0.5 * own.astype(F32)
            return carry

        lax.fori_loop(0, 4, theirs, 0)
        down_out(j).start()
        lax.fori_loop(0, 4, ours, 0)
        down_home(j).start()

    act = {"norm": norm, "mix": mix, "out": out_proj, "again": again, "hide": hide, "down": down}
    landed = set()
    for what, i in steps:
        if what == "start":
            stage = sends[i].stage
            if stage not in landed:
                landed.add(stage)
                for k in ready_of[stage]:
                    locals_[k].wait()
            outgoing(i).start()
        elif what == "wait":
            incoming(i).wait_recv()
        else:
            act[what](i)

    for i in range(len(sends)):
        outgoing(i).wait_send()
    tokens_out().wait_send()
    for j in range(2):
        down_out(j).wait()
        down_home(j).wait()


def on_device(
    tokens, mix_gain, w_bgate, w_cgate, w_value, conv_taps, w_mixout, mlp_gain, w_gate, w_up, w_down
):
    count = len(plan()[0])
    anywhere = pl.BlockSpec(memory_space=pl.ANY)
    total, came = pl.pallas_call(
        kernel,
        name="residual_block",
        out_shape=(jax.ShapeDtypeStruct((H, D), F32), jax.ShapeDtypeStruct((H, D), BF16)),
        in_specs=[anywhere] * 11,
        out_specs=(anywhere, anywhere),
        scratch_shapes=[
            *[pltpu.VMEM((2, 4, 4, 64, width), BF16) for width in WIDTHS],
            pltpu.VMEM((T, D), BF16),
            pltpu.VMEM((T, D), BF16),
            pltpu.VMEM((T, 1024), BF16),
            pltpu.VMEM((T, D), BF16),
            pltpu.VMEM((T, D), BF16),
            pltpu.VMEM((H, D), F32),
            pltpu.VMEM((T, 1408), BF16),
            pltpu.VMEM((1, D), F32),
            pltpu.VMEM((3, D), F32),
            pltpu.VMEM((1, D), F32),
            pltpu.VMEM((T, 256), BF16),
            pltpu.VMEM((T, 256), BF16),
            pltpu.SemaphoreType.DMA((11,)),
            pltpu.SemaphoreType.DMA((count,)),
            pltpu.SemaphoreType.DMA((count,)),
            pltpu.SemaphoreType.DMA((5,)),
            pltpu.SemaphoreType.DMA((5,)),
        ],
        compiler_params=pltpu.CompilerParams(
            collective_id=0, has_side_effects=True, vmem_limit_bytes=67043328
        ),
    )(
        tokens, mix_gain[None], w_bgate, w_cgate, w_value, conv_taps, w_mixout.T,
        mlp_gain[None], w_gate, w_up, w_down.T,
    )
    return (total + 0.5 * came.astype(F32)).astype(BF16)


def solution(mesh):
    finer = Mesh(
        mesh.devices.reshape(mesh.shape["rep"], 2, 4, 4, mesh.shape["tp"]),
        ("rep", "fs_0", "fs_1", "fs_2", "tp"),
    )
    return jax.shard_map(
        on_device,
        mesh=finer,
        in_specs=(
            P(REP_FS_TP, None),
            P(),
            P(FS, "tp"),
            P(FS, "tp"),
            P(FS, "tp"),
            P(),
            P("tp", FS),
            P(),
            P(FS, "tp"),
            P(FS, "tp"),
            P("tp", FS),
        ),
        out_specs=P(REP_FS_TP, None),
        check_vma=False,
    )
```

```python
import heapq

import jax
import jax.numpy as jnp
from jax import lax
from jax.experimental import pallas as pl
from jax.experimental.pallas import tpu as pltpu
from jax.sharding import Mesh
from jax.sharding import PartitionSpec as P

FS = ("fs_0", "fs_1", "fs_2")
REP_FS_TP = ("rep", "fs_0", "fs_1", "fs_2", "tp")
MESH = pl.DeviceIdType.MESH
BF16, F32 = jnp.bfloat16, jnp.float32

D = 2048
T = 640
H = 320
WIDTHS = (1536, 512, 2816, 1408)
LINK = 45.6e3
PAIR = 500.0e3
LATENCY = 2.6
PAIR_LATENCY = 1.5
BACKLOG = 2.7
HOLD = 0.0

RANKS = (
    -2, -2, -2, -2, -3, -4, -4, -4, -4, -4, -4, -4, -4, -4, -4, 1260, 1396, 1285, 1398, 1398,
    1232, 1347, 1278, 1292, 1311, 1343, 1281, 1343, 1379, 1237, 1376, 1398, 1253, 1336, 1303,
    1369, 1303, 1303, 1399, 1450, 1576, 1304, 1198, 1344, 1339, 1499, 1282, 1303, 1303, 1369,
    1303, 1375, 1376, 1220, 1336, 1398, 1472, 1253, 1209, 1376, 1209, 1328, 1376, 1313, 1216,
    1278, 1290, 1347, 1293, 1434, 1298, 1390, 1390, 1548, 1549, 1487, 1492, 1419, 1426, 1419,
    1365, 1514, 1499, 1465, 1489, 1482, 1387, 1460, 1387, 1515, 1415, 1388, 1365, 1443, 1354,
    1546, 1445, 1430, 1516, 1359, 1459, 1340, 1415, 1371, 1415, 1511, 1443, 1482, 1482, 1483,
    1598, 1467, 1384, 1267, 1415, 1415, 1441, 1482, 1533, 1468, 1423, 1451, 1431, 1449, 1482,
    1495, 1632, 1593, 1676, 1683, 1656, 1652, 1650, 1639, 1683, 1738, 1929, 1809, 1925, 1802,
    1736, 1521, 1624, 1632, 1625, 1739, 1727, 1714, 1739, 1739, 1895, 1780, 1888, 1842, 1802,
    1802, 1979, 1613, 1556, 1716, 1694, 1620, 1733, 1657, 1874, 2006, 1860, 1673, 1969, 1738,
    1613, 1568, 1613, 1703, 1733, 1599, 1657, 1732, 1925, 1722, 1701, 1802, 1714, 1555, 1667,
    1565, 1706, 1496, 1628, 1674, 1674, 1674, 2096, 2040, 2015, 2140, 2008, 1937, 2205, 1621,
    1534, 1591, 1704, 1698, 1684, 1674, 1737, 1733, 1908, 2057, 2037, 2096, 2008, 2034, 2008,
    1563, 1504, 1635, 1978, 1941, 1843, 1958, 1654, 1655, 1953, 1886, 1644, 2008, 1721, 1545,
    1632, 1853, 1910, 1911, 1939, 1673, 1721, 2008, 1945, 1703, 2008,
)

ALL = ("all",)
ME = ("rel", 0)


def half(k):
    return ("half", k)


def rel(k):
    return ("rel", k)


class Send:
    def __init__(self, kind, way, needs, rank, size, stage=None, quarter=None, at=None, index=None):
        self.kind, self.way, self.needs, self.rank = kind, way, needs, rank
        self.stage, self.quarter, self.at, self.index = stage, quarter, at, index
        self.time = size / (PAIR if way == "pair" else LINK)
        self.latency = PAIR_LATENCY if way == "pair" else LATENCY


def all_sends():
    out = []

    def add(quarter, way, at, needs, rank, pieces):
        at = {"z": ME, "y": ME, "x": ME} | at
        size = pieces * 16 * WIDTHS[stage] * 2
        send = Send("part", way, list(needs), rank, size, stage, quarter, at)
        out.append(send)
        return send

    def other(kind, way, needs, rank, size, index, stage=None):
        send = Send(kind, way, list(needs), rank, size, stage, None, None, index)
        out.append(send)
        return send

    row = D * 2
    for p in range(2):
        token = other("token", "zw", [], -2, 160 * row, p)
        other("relay", "pair", [token], -2, 160 * row, p)
    other("swap", "pair", [], -3, H * row, 0)
    for j in range(2):
        other("mate", "pair", [("mate", j)], -4, H * 1024 * 2, j)
        other("sum", "zw", [("sum", j)], -4, 160 * row, j)
        other("home", "pair", [("home", j)], -4, H * 1024 * 2, j)
        other("again", "pair", [("again", j)], -4, 160 * row, j)
        other("down", "pair", [("down", 2 * j)], -4, H * 1024 * 2, j)

    for stage in range(2):
        base = 10 * stage
        orders = (("x", "y"), ("x", "y"), ("y", "x"), ("y", "x") if stage == 0 else ("x", "y"))
        for quarter, (first, second) in enumerate(orders):
            if quarter == 3:
                over = [add(quarter, "zd", {}, [], base, 1)]
                for far in range(2):
                    z = {"z": rel(far)}
                    start = over if far else []
                    plus = add(quarter, first + "+", z, start, base + far, 1)
                    minus = add(quarter, first + "-", z, start, base + far, 1)
                    if far:
                        on = add(quarter, first + "-", z | {first: rel(1)}, [minus], base + 2, 1)
                    else:
                        on = add(quarter, first + "+", z | {first: rel(-1)}, [plus], base + 2, 1)
                    line = [plus, minus, on] + start
                    z = z | {first: ALL}
                    plus = add(quarter, second + "+", z, line, base + 3, 4)
                    minus = add(quarter, second + "-", z, line, base + 3, 4)
                    if far:
                        add(quarter, second + "-", z | {second: rel(1)}, [minus], base + 4, 4)
                    else:
                        add(quarter, second + "+", z | {second: rel(-1)}, [plus], base + 4, 4)
                continue
            forth, back = first + "+", first + "-"
            plus = add(quarter, forth, {}, [], base, 1)
            minus = add(quarter, back, {}, [], base, 1)
            if quarter == 1:
                on = add(quarter, back, {first: rel(1)}, [minus], base + 1, 1)
            else:
                on = add(quarter, forth, {first: rel(-1)}, [plus], base + 1, 1)
            line = [plus, minus, on]
            over = [
                add(quarter, "zd", {first: rel(k)}, needs, base + 1, 1)
                for k, needs in ((0, []), (-1, [plus]), (1, [minus]), (2, [on]))
            ]
            forth, back = second + "+", second + "-"
            if quarter == 0:
                pa = add(quarter, forth, {first: half(0)}, line, base + 2, 2)
                pb = add(quarter, forth, {first: half(1)}, line, base + 3, 2)
                ma = add(quarter, back, {first: half(1)}, line, base + 2, 2)
                mb = add(quarter, back, {first: half(0)}, line, base + 3, 2)
                po = add(quarter, forth, {first: half(0), second: rel(-1)}, [pa], base + 4, 2)
                mo = add(quarter, back, {first: half(1), second: rel(1)}, [ma], base + 4, 2)
                add(quarter, "zd", {first: ALL, second: rel(-1)}, [pa, pb], base + 5, 4)
                add(quarter, "zd", {first: ALL, second: rel(1)}, [ma, mb], base + 5, 4)
                add(quarter, "zd", {first: ALL, second: rel(2)}, [po, mo], base + 6, 4)
            else:
                here, there = {first: ALL}, {first: ALL, "z": rel(1)}
                ph = add(quarter, forth, here, line, base + 3, 4)
                add(quarter, back, here, line, base + 3, 4)
                add(quarter, forth, there, over, base + 4, 4)
                mt = add(quarter, back, there, over, base + 4, 4)
                add(quarter, forth, here | {second: rel(-1)}, [ph], base + 5, 4)
                add(quarter, back, there | {second: rel(1)}, [mt], base + 5, 4)
    orders = (("x", "y"), ("y", "x"), ("x", "y"), ("y", "x"))
    for stage in range(2, 4):
        base = 20 + 10 * (stage - 2)
        early = 14 + 8 * (stage - 2)
        for quarter, (first, second) in enumerate(orders):
            forth, back = first + "+", first + "-"
            plus = add(quarter, forth, {}, [], early, 1)
            minus = add(quarter, back, {}, [], early, 1)
            if quarter < 2:
                on = add(quarter, forth, {first: rel(-1)}, [plus], early, 1)
            else:
                on = add(quarter, back, {first: rel(1)}, [minus], early, 1)
            line = [plus, minus, on]
            forth, back = second + "+", second + "-"
            if quarter < 2:
                pa = add(quarter, forth, {first: half(0)}, line, base + 2, 2)
                pb = add(quarter, forth, {first: half(1)}, line, base + 3, 2)
                ma = add(quarter, back, {first: half(1)}, line, base + 2, 2)
                mb = add(quarter, back, {first: half(0)}, line, base + 3, 2)
                po = add(quarter, forth, {first: half(0), second: rel(-1)}, [pa], base + 4, 2)
                mo = add(quarter, back, {first: half(1), second: rel(1)}, [ma], base + 4, 2)
                add(quarter, "zw", {}, [], early, 1)
                add(quarter, "zw", {first: rel(-1)}, [plus], early, 1)
                add(quarter, "zw", {first: rel(1)}, [minus], early, 1)
                add(quarter, "zw", {first: rel(2)}, [on], early, 1)
                add(quarter, "zd", {first: ALL, second: rel(-1)}, [pa, pb], base + 5, 4)
                add(quarter, "zd", {first: ALL, second: rel(1)}, [ma, mb], base + 5, 4)
                add(quarter, "zw", {first: ALL, second: rel(2)}, [po, mo], base + 6, 4)
            else:
                over = [
                    add(quarter, "zd", {first: rel(k)}, needs, base + 2, 1)
                    for k, needs in ((0, []), (-1, [plus]), (1, [minus]), (2, [on]))
                ]
                here, there = {first: ALL}, {first: ALL, "z": rel(1)}
                ph = add(quarter, forth, here, line, base + 3, 4)
                add(quarter, back, here, line, base + 3, 4)
                add(quarter, forth, there, over, base + 4, 4)
                mt = add(quarter, back, there, over, base + 4, 4)
                add(quarter, forth, here | {second: rel(-1)}, [ph], base + 5, 4)
                add(quarter, back, there | {second: rel(1)}, [mt], base + 5, 4)
    return out


def near(send):
    return (send.way[0] == "z") == (send.at["z"] != ME)


def work_list(sends):
    def kind(name, *index):
        return [s for s in sends if s.kind == name and (not index or s.index in index)]

    def stage(k):
        return [s for s in sends if s.stage == k]

    last = stage(3)
    out = [("norm", k, 1.0, kind("swap")) for k in range(4)]
    out += [("norm", k, 1.0, kind("token") + kind("relay")) for k in range(4, 8)]
    out += [("mix", k, 1.6 if k % 3 == 2 else 0.8, stage(0)) for k in range(6)]
    out += [("mate", k, 1.0, stage(1)) for k in range(2)]
    out += [("sum", k, 0.7, kind("mate")) for k in range(2)]
    out += [("mix", k, 1.6 if k % 3 == 2 else 0.8, []) for k in range(6, 12)]
    out += [("home", k, 1.0, []) for k in range(2)]
    out += [("again", k, 1.4, kind("home") + kind("sum", k)) for k in range(2)]
    out += [("hide", k, 0.95, kind("again") + stage(2)) for k in range(11)]
    out += [("down", k, 1.5, [s for s in last if near(s)]) for k in range(2)]
    out += [("down", k, 1.5, last) for k in range(2, 4)]
    return out


def plan(ranks=RANKS):
    sends = all_sends()
    if ranks:
        for send, rank in zip(sends, ranks, strict=True):
            send.rank = rank
    work = work_list(sends)
    number = {id(send): i for i, send in enumerate(sends)}
    followers, missing = {}, []
    for i, send in enumerate(sends):
        missing.append(len(send.needs))
        for need in send.needs:
            key = need if isinstance(need, tuple) else number[id(need)]
            followers.setdefault(key, []).append(i)
    ready = {send.way: [] for send in sends}
    free = dict.fromkeys(ready, 0.0)
    got, flying, steps, held, now = set(), [], [], [], 0.0

    def release(i):
        if sends[i].kind == "part" and sends[i].stage > 1 and now < HOLD:
            held.append(i)
        else:
            heapq.heappush(ready[sends[i].way], (sends[i].rank, i))

    def arrive(key):
        got.add(key)
        for i in followers.get(key, ()):
            missing[i] -= 1
            if missing[i] == 0:
                release(i)

    def top_up():
        if now >= HOLD:
            while held:
                release(held.pop())
        for way, queue in ready.items():
            while queue and (queue[0][0] < 0 or free[way] - now <= BACKLOG):
                i = heapq.heappop(queue)[1]
                free[way] = max(free[way], now) + sends[i].time
                heapq.heappush(flying, (free[way] + sends[i].latency, i))
                steps.append(("start", i))

    for i, count in enumerate(missing):
        if count == 0:
            release(i)
    top_up()
    step = 0
    needs = [[number[id(need)] for need in piece[3]] for piece in work]
    while flying or step < len(work):
        while flying and flying[0][0] <= now:
            i = heapq.heappop(flying)[1]
            steps.append(("wait", i))
            arrive(i)
            top_up()
        if step < len(work) and got.issuperset(needs[step]):
            name, j, time, _ = work[step]
            step += 1
            steps.append((name, j))
            now += time
            arrive((name, j))
            top_up()
        elif flying:
            now = max(now, flying[0][0])
    return sends, steps, now


def region(send, place):
    at = []
    for dim, extent in (("z", 2), ("y", 4), ("x", 4)):
        how = send.at[dim]
        if how == ALL:
            at.append(pl.ds(0, extent))
        elif how[0] == "half":
            at.append(pl.ds(2 * how[1], 2))
        else:
            at.append(pl.ds(lax.rem(place[dim] + how[1] + extent, extent), 1))
    return (*at, pl.ds(16 * send.quarter, 16), pl.ds(0, WIDTHS[send.stage]))


def kernel(
    tokens, gain_one, w_b, w_c, w_v, taps, w_mix, gain_two, w_g, w_u, w_d, total, came_two,
    s0, s1, s2, s3, raw, normed, gated, to_mate, from_mate, summed, mate_sum, to_home, from_home,
    resid, hidden, gain_v, taps_v, gain_two_v, acc_b, acc_c, local_sem, send_sem, recv_sem,
):
    sends, steps, _ = plan()
    buffers = (s0, s1, s2, s3)
    rep, zl, y, x, tp = (lax.axis_index(name) for name in REP_FS_TP)
    me = {"z": zl, "y": y, "x": x}

    def device(way):
        if way == "pair":
            return (rep, zl, y, x, 1 - tp)
        if way == "zd":
            return (rep, 1 - zl, y, x, tp)
        if way == "zw":
            return (1 - rep, 1 - zl, y, x, tp)
        step = 1 if way[1] == "+" else 3
        if way[0] == "x":
            return (rep, zl, y, lax.rem(x + step, 4), tp)
        return (rep, zl, lax.rem(y + step, 4), x, tp)

    def rows_of(core, start=0, n=H):
        return pl.ds(pl.multiple_of(core * H + start, 32), n)

    mine, other = rows_of(tp), rows_of(1 - tp)

    def local(k, src, dst):
        return pltpu.make_async_copy(src, dst, local_sem.at[k])

    def slot(buffer, lo, n):
        return buffer.at[zl, y, x, pl.ds(0, 64), pl.ds(lo, n)]

    def share(weight):
        return weight.at[:, pl.ds(pl.multiple_of(rep * 512, 512), 512)]

    locals_ = [
        local(0, share(w_b), slot(s0, 0, 512)),
        local(1, share(w_c), slot(s0, 512, 512)),
        local(2, share(w_v), slot(s0, 1024, 512)),
        local(3, share(w_mix), slot(s1, 0, 512)),
        local(4, w_g, slot(s2, 0, 1408)),
        local(5, w_u, slot(s2, 1408, 1408)),
        local(6, w_d, slot(s3, 0, 1408)),
        local(7, tokens, raw.at[0, mine, :]),
        local(8, gain_one, gain_v),
        local(9, taps, taps_v),
        local(10, gain_two, gain_two_v),
    ]
    ready_of = ((0, 1, 2), (3,), (4, 5), (6,))
    for copy in locals_:
        copy.start()

    barrier = pltpu.get_barrier_semaphore()
    ways = ("x+", "x-", "y+", "y-", "zd", "zw", "pair")
    for way in ways:
        pl.semaphore_signal(barrier, inc=1, device_id=device(way), device_id_type=MESH)
    pl.semaphore_wait(barrier, len(ways))

    def ends(send, place, core):
        j = send.index
        cols = None if j is None else pl.ds(1024 * (j % 2), 1024)
        if send.kind == "part":
            where = buffers[send.stage].at[region(send, place)]
            return where, where
        if send.kind == "token":
            return tokens.at[pl.ds(160 * j, 160), :], raw.at[1, rows_of(core, 160 * j, 160), :]
        if send.kind == "relay":
            where = raw.at[1, rows_of(core, 160 * j, 160), :]
            return where, where
        if send.kind == "swap":
            return tokens, raw.at[0, rows_of(core), :]
        if send.kind == "mate":
            return to_mate.at[:, cols], from_mate.at[:, cols]
        if send.kind == "sum":
            rows = pl.ds(160 * j, 160)
            return summed.at[rows, :], mate_sum.at[rows, :]
        if send.kind == "home":
            return to_home.at[:, cols], from_home.at[:, cols]
        if send.kind == "again":
            where = normed.at[0, rows_of(core, 160 * j, 160), :]
            return where, where
        lanes = half_of(j, place["z"])
        return to_mate.at[:, lanes], came_two.at[:, lanes]

    def half_of(j, z):
        return pl.ds(pl.multiple_of(1024 * lax.rem(z + j, 2), 1024), 1024)

    def copy_of(i, place, core):
        src, dst = ends(sends[i], place, core)
        return pltpu.make_async_remote_copy(
            src_ref=src, dst_ref=dst, send_sem=send_sem.at[i], recv_sem=recv_sem.at[i],
            device_id=device(sends[i].way), device_id_type=MESH,
        )

    def outgoing(i):
        return copy_of(i, me, tp)

    def incoming(i):
        way, place = sends[i].way, dict(me)
        if way in ("zd", "zw"):
            place["z"] = 1 - zl
        elif way != "pair":
            place[way[0]] = lax.rem(me[way[0]] + (3 if way[1] == "+" else 1), 4)
        return copy_of(i, place, 1 - tp if way == "pair" else tp)

    def scaled(values, gain):
        factor = lax.rsqrt(jnp.mean(values * values, axis=-1, keepdims=True) + 1e-06)
        return (values * factor * gain).astype(BF16)

    def norm(step):
        c, part = step // 4, step % 4
        if step == 0:
            locals_[7].wait()
            locals_[8].wait()
        gain = gain_v[...]

        def chunk(r, carry):
            rows = pl.ds(pl.multiple_of(r * 32, 32), 32)
            normed[c, rows, :] = scaled(raw[c, rows, :].astype(F32), gain)
            return carry

        lax.fori_loop(5 * part, 5 * part + 5, chunk, 0)

    def mix(step):
        c, j, k = 1 - step // 6, step // 3 % 2, step % 3
        if step == 0:
            locals_[9].wait()

        def dot(k):
            w = s0[:, :, :, :, pl.ds(512 * k + 256 * j, 256)].reshape(D, 256)
            return jnp.dot(normed[c], w, preferred_element_type=F32).astype(BF16)

        if k < 2:
            (acc_b, acc_c)[k][...] = dot(k)
            return
        mixed = acc_c[...].astype(F32) * dot(2).astype(F32)
        row = lax.broadcasted_iota(jnp.int32, (T, 256), 0)
        one = jnp.where(row >= 1, pltpu.roll(mixed, 1, 0), 0.0)
        two = jnp.where(row >= 2, pltpu.roll(mixed, 2, 0), 0.0)
        lanes = pl.ds(pl.multiple_of(tp * 1024 + rep * 512 + 256 * j, 256), 256)
        tap = [taps_v[pl.ds(k, 1), lanes] for k in range(3)]
        convolved = tap[0] * two + tap[1] * one + tap[2] * mixed
        gated[c, :, pl.ds(256 * j, 256)] = (acc_b[...].astype(F32) * convolved).astype(BF16)

    def block(left, right):
        return lax.dot_general(left, right, (((1,), (1,)), ((), ())), preferred_element_type=F32)

    def product(c, j, away):
        def one(k, carry):
            cols = pl.ds(pl.multiple_of(1024 * j + 256 * k, 256), 256)
            w = s1[j, k].reshape(256, 512)
            away[:, cols] = block(gated[c, other, :], w).astype(BF16)
            resid[:, cols] = block(gated[c, mine, :], w)
            return carry

        lax.fori_loop(0, 4, one, 0)

    def mate(j):
        product(1, j, to_mate)

    def home(j):
        product(0, j, to_home)

    def add_up(p):
        def chunk(r, carry):
            rows = pl.ds(pl.multiple_of(160 * p + r * 32, 32), 32)
            summed[rows, :] = (resid[rows, :] + from_mate[rows, :].astype(F32)).astype(BF16)
            return carry

        lax.fori_loop(0, 5, chunk, 0)

    def again(p):
        if p == 0:
            locals_[10].wait()
        gain = gain_two_v[...]

        def chunk(r, carry):
            rows = pl.ds(pl.multiple_of(160 * p + r * 32, 32), 32)
            here = pl.ds(pl.multiple_of(tp * H + 160 * p + r * 32, 32), 32)
            sums = resid[rows, :] + from_home[rows, :].astype(F32)
            sums = sums + mate_sum[rows, :].astype(F32)
            values = raw[0, here, :].astype(F32) + sums
            resid[rows, :] = values
            normed[0, here, :] = scaled(values, gain)
            return carry

        lax.fori_loop(0, 5, chunk, 0)

    def hide(k):
        w_gate = s2[:, :, :, :, pl.ds(128 * k, 128)].reshape(D, 128)
        w_up = s2[:, :, :, :, pl.ds(1408 + 128 * k, 128)].reshape(D, 128)
        both = jnp.dot(
            normed[0], jnp.concatenate([w_gate, w_up], axis=1), preferred_element_type=F32
        )
        gate, up = both[:, :128], both[:, 128:]
        hidden[:, pl.ds(128 * k, 128)] = (gate / (1.0 + jnp.exp(-gate)) * up).astype(BF16)

    def down_home(j):
        cols = half_of(j, zl)
        return local(j, resid.at[:, cols], total.at[:, cols])

    def down(step):
        j = step // 2
        plane = lax.rem(zl + j, 2)

        def theirs(k, carry):
            cols = pl.ds(pl.multiple_of(1024 * plane + 256 * k, 256), 256)
            w = s3[plane, k].reshape(256, 1408)
            to_mate[:, cols] = block(hidden[other, :], w).astype(BF16)
            return carry

        def ours(k, carry):
            cols = pl.ds(pl.multiple_of(1024 * plane + 256 * k, 256), 256)
            own = block(hidden[mine, :], s3[plane, k].reshape(256, 1408)).astype(BF16)
            resid[:, cols] = resid[:, cols] + 0.5 * own.astype(F32)
            return carry

        if step == 0:
            for i, send in enumerate(sends):
                if send.kind == "mate":
                    outgoing(i).wait_send()
        if step % 2 == 0:
            lax.fori_loop(0, 4, theirs, 0)
        else:
            lax.fori_loop(0, 4, ours, 0)
            down_home(j).start()

    act = {
        "norm": norm, "mix": mix, "mate": mate, "sum": add_up, "home": home, "again": again,
        "hide": hide, "down": down,
    }
    landed = set()
    for what, i in steps:
        if what == "start":
            send = sends[i]
            if send.kind == "part" and send.stage not in landed:
                landed.add(send.stage)
                for k in ready_of[send.stage]:
                    locals_[k].wait()
            outgoing(i).start()
        elif what == "wait":
            incoming(i).wait_recv()
        else:
            act[what](i)

    for i, send in enumerate(sends):
        if send.kind != "mate":
            outgoing(i).wait_send()
    for j in range(2):
        down_home(j).wait()


def on_device(
    tokens, mix_gain, w_bgate, w_cgate, w_value, conv_taps, w_mixout, mlp_gain, w_gate, w_up, w_down
):
    count = len(all_sends())
    anywhere = pl.BlockSpec(memory_space=pl.ANY)
    total, came = pl.pallas_call(
        kernel,
        name="residual_block",
        out_shape=(jax.ShapeDtypeStruct((H, D), F32), jax.ShapeDtypeStruct((H, D), BF16)),
        in_specs=[anywhere] * 11,
        out_specs=(anywhere, anywhere),
        scratch_shapes=[
            *[pltpu.VMEM((2, 4, 4, 64, width), BF16) for width in WIDTHS],
            pltpu.VMEM((2, T, D), BF16),
            pltpu.VMEM((2, T, D), BF16),
            pltpu.VMEM((2, T, 512), BF16),
            *[pltpu.VMEM((H, D), BF16)] * 6,
            pltpu.VMEM((H, D), F32),
            pltpu.VMEM((T, 1408), BF16),
            pltpu.VMEM((1, D), F32),
            pltpu.VMEM((3, D), F32),
            pltpu.VMEM((1, D), F32),
            pltpu.VMEM((T, 256), BF16),
            pltpu.VMEM((T, 256), BF16),
            pltpu.SemaphoreType.DMA((11,)),
            pltpu.SemaphoreType.DMA((count,)),
            pltpu.SemaphoreType.DMA((count,)),
        ],
        compiler_params=pltpu.CompilerParams(
            collective_id=0, has_side_effects=True, vmem_limit_bytes=67043328
        ),
    )(
        tokens, mix_gain[None], w_bgate, w_cgate, w_value, conv_taps, w_mixout.T,
        mlp_gain[None], w_gate, w_up, w_down.T,
    )
    return (total + 0.5 * came.astype(F32)).astype(BF16)


def solution(mesh):
    finer = Mesh(
        mesh.devices.reshape(mesh.shape["rep"], 2, 4, 4, mesh.shape["tp"]),
        ("rep", "fs_0", "fs_1", "fs_2", "tp"),
    )
    return jax.shard_map(
        on_device,
        mesh=finer,
        in_specs=(
            P(REP_FS_TP, None),
            P(),
            P(FS, "tp"),
            P(FS, "tp"),
            P(FS, "tp"),
            P(),
            P("tp", FS),
            P(),
            P(FS, "tp"),
            P(FS, "tp"),
            P("tp", FS),
        ),
        out_specs=P(REP_FS_TP, None),
        check_vma=False,
    )
```

```python
import heapq

import jax
import jax.numpy as jnp
from jax import lax
from jax.experimental import pallas as pl
from jax.experimental.pallas import tpu as pltpu
from jax.sharding import Mesh
from jax.sharding import PartitionSpec as P

FS = ("fs_0", "fs_1", "fs_2")
REP_FS_TP = ("rep", "fs_0", "fs_1", "fs_2", "tp")
MESH = pl.DeviceIdType.MESH
BF16, F32 = jnp.bfloat16, jnp.float32

D = 2048
T = 640
H = 320
WIDTHS = (1536, 512, 2816, 1408)
LINK = 45.6e3
PAIR = 500.0e3
LATENCY = 2.6
PAIR_LATENCY = 1.5
BACKLOG = 2.75
HOLD = 0.0

RANKS = (
    -2, -2, -2, -2, -3, -4, -4, -4, -4, -4, -4, -4, -4, -4, -4, 492, 63, 454, 0, 290, 1432,
    314, 34, 0, 0, 375, 150, 0, 28, 811, 150, 0, 393, 0, 573, 0, 0, 1361, 0, 40, 501, 262,
    1309, 640, 915, 302, 0, 0, 356, 0, 0, 0, 106, 291, 0, 779, 0, 0, 0, 0, 0, 548, 0, 0, 468,
    1054, 0, 0, 0, 51, 0, 0, 0, 0, 0, 0, 0, 0, 0, 0, 0, 0, 0, 0, 0, 0, 0, 0, 0, 0, 0, 0, 0, 0,
    0, 621, 0, 0, 0, 0, 0, 309, 955, 0, 623, 0, 0, 0, 950, 0, 0, 0, 0, 0, 0, 0, 0, 0, 0, 0, 0,
    0, 0, 1131, 281, 575, 1257, 1552, 1547, 1543, 1225, 776, 1418, 2204, 0, 2680, 2569, 1574,
    887, 1925, 2595, 1362, 1412, 765, 1672, 1361, 2101, 1154, 2976, 2949, 2010, 2192, 2850,
    932, 2246, 1875, 1502, 0, 1087, 698, 1318, 1578, 1679, 78, 2113, 2575, 1672, 2158, 2132,
    1880, 0, 984, 2117, 1024, 825, 1075, 1235, 4064, 2301, 2442, 1256, 1700, 2357, 2885, 2992,
    1410, 1175, 2161, 2291, 769, 2794, 2363, 1753, 2634, 3794, 1175, 1926, 359, 1316, 349,
    2795, 675, 1848, 2322, 3078, 2550, 3003, 2491, 1092, 3045, 2981, 754, 925, 2185, 1422,
    1621, 1290, 3485, 2508, 2327, 1968, 1531, 1439, 3130, 1946, 2190, 3375, 2217, 1064, 530,
    3110, 1418, 3573, 2220, 1887, 1113, 1543, 1484,
)

ALL = ("all",)
ME = ("rel", 0)


def half(k):
    return ("half", k)


def rel(k):
    return ("rel", k)


class Send:
    def __init__(self, kind, way, needs, rank, size, stage=None, quarter=None, at=None, index=None):
        self.kind, self.way, self.needs, self.rank = kind, way, needs, rank
        self.stage, self.quarter, self.at, self.index = stage, quarter, at, index
        self.time = size / (PAIR if way == "pair" else LINK)
        self.latency = PAIR_LATENCY if way == "pair" else LATENCY


def all_sends():
    out = []

    def add(quarter, way, at, needs, rank, pieces):
        at = {"z": ME, "y": ME, "x": ME} | at
        size = pieces * 16 * WIDTHS[stage] * 2
        send = Send("part", way, list(needs), rank, size, stage, quarter, at)
        out.append(send)
        return send

    def other(kind, way, needs, rank, size, index, stage=None):
        send = Send(kind, way, list(needs), rank, size, stage, None, None, index)
        out.append(send)
        return send

    row = D * 2
    for p in range(2):
        token = other("token", "zw", [], -2, 160 * row, p)
        other("relay", "pair", [token], -2, 160 * row, p)
    other("swap", "pair", [], -3, H * row, 0)
    for j in range(2):
        other("mate", "pair", [("mate", j)], -4, H * 1024 * 2, j)
        other("sum", "zw", [("sum", j)], -4, 160 * row, j)
        other("home", "pair", [("home", j)], -4, H * 1024 * 2, j)
        other("again", "pair", [("again", j)], -4, 160 * row, j)
        other("down", "pair", [("down", 2 * j)], -4, H * 1024 * 2, j)

    for stage in range(2):
        base = 10 * stage
        orders = (("x", "y"), ("x", "y"), ("y", "x"), ("y", "x") if stage == 0 else ("x", "y"))
        for quarter, (first, second) in enumerate(orders):
            if quarter == 3:
                over = [add(quarter, "zd", {}, [], base, 1)]
                for far in range(2):
                    z = {"z": rel(far)}
                    start = over if far else []
                    plus = add(quarter, first + "+", z, start, base + far, 1)
                    minus = add(quarter, first + "-", z, start, base + far, 1)
                    if far:
                        on = add(quarter, first + "-", z | {first: rel(1)}, [minus], base + 2, 1)
                    else:
                        on = add(quarter, first + "+", z | {first: rel(-1)}, [plus], base + 2, 1)
                    line = [plus, minus, on] + start
                    z = z | {first: ALL}
                    plus = add(quarter, second + "+", z, line, base + 3, 4)
                    minus = add(quarter, second + "-", z, line, base + 3, 4)
                    if far:
                        add(quarter, second + "-", z | {second: rel(1)}, [minus], base + 4, 4)
                    else:
                        add(quarter, second + "+", z | {second: rel(-1)}, [plus], base + 4, 4)
                continue
            forth, back = first + "+", first + "-"
            plus = add(quarter, forth, {}, [], base, 1)
            minus = add(quarter, back, {}, [], base, 1)
            if quarter == 1:
                on = add(quarter, back, {first: rel(1)}, [minus], base + 1, 1)
            else:
                on = add(quarter, forth, {first: rel(-1)}, [plus], base + 1, 1)
            line = [plus, minus, on]
            over = [
                add(quarter, "zd", {first: rel(k)}, needs, base + 1, 1)
                for k, needs in ((0, []), (-1, [plus]), (1, [minus]), (2, [on]))
            ]
            forth, back = second + "+", second + "-"
            if quarter == 0:
                pa = add(quarter, forth, {first: half(0)}, line, base + 2, 2)
                pb = add(quarter, forth, {first: half(1)}, line, base + 3, 2)
                ma = add(quarter, back, {first: half(1)}, line, base + 2, 2)
                mb = add(quarter, back, {first: half(0)}, line, base + 3, 2)
                po = add(quarter, forth, {first: half(0), second: rel(-1)}, [pa], base + 4, 2)
                mo = add(quarter, back, {first: half(1), second: rel(1)}, [ma], base + 4, 2)
                add(quarter, "zd", {first: ALL, second: rel(-1)}, [pa, pb], base + 5, 4)
                add(quarter, "zd", {first: ALL, second: rel(1)}, [ma, mb], base + 5, 4)
                add(quarter, "zd", {first: ALL, second: rel(2)}, [po, mo], base + 6, 4)
            else:
                here, there = {first: ALL}, {first: ALL, "z": rel(1)}
                ph = add(quarter, forth, here, line, base + 3, 4)
                add(quarter, back, here, line, base + 3, 4)
                add(quarter, forth, there, over, base + 4, 4)
                mt = add(quarter, back, there, over, base + 4, 4)
                add(quarter, forth, here | {second: rel(-1)}, [ph], base + 5, 4)
                add(quarter, back, there | {second: rel(1)}, [mt], base + 5, 4)
    orders = (("x", "y"), ("y", "x"), ("x", "y"), ("y", "x"))
    for stage in range(2, 4):
        base = 20 + 10 * (stage - 2)
        early = 14 + 8 * (stage - 2)
        for quarter, (first, second) in enumerate(orders):
            forth, back = first + "+", first + "-"
            plus = add(quarter, forth, {}, [], early, 1)
            minus = add(quarter, back, {}, [], early, 1)
            if quarter < 2:
                on = add(quarter, forth, {first: rel(-1)}, [plus], early, 1)
            else:
                on = add(quarter, back, {first: rel(1)}, [minus], early, 1)
            line = [plus, minus, on]
            forth, back = second + "+", second + "-"
            if quarter < 4 - stage:
                pa = add(quarter, forth, {first: half(0)}, line, base + 2, 2)
                pb = add(quarter, forth, {first: half(1)}, line, base + 3, 2)
                ma = add(quarter, back, {first: half(1)}, line, base + 2, 2)
                mb = add(quarter, back, {first: half(0)}, line, base + 3, 2)
                po = add(quarter, forth, {first: half(0), second: rel(-1)}, [pa], base + 4, 2)
                mo = add(quarter, back, {first: half(1), second: rel(1)}, [ma], base + 4, 2)
                add(quarter, "zw", {}, [], early, 1)
                add(quarter, "zw", {first: rel(-1)}, [plus], early, 1)
                add(quarter, "zw", {first: rel(1)}, [minus], early, 1)
                add(quarter, "zw", {first: rel(2)}, [on], early, 1)
                late = "zw" if stage == 3 else "zd"
                add(quarter, late, {first: ALL, second: rel(-1)}, [pa, pb], base + 5, 4)
                add(quarter, "zd", {first: ALL, second: rel(1)}, [ma, mb], base + 5, 4)
                add(quarter, late, {first: ALL, second: rel(2)}, [po, mo], base + 6, 4)
            else:
                over = [
                    add(quarter, way, {first: rel(k)}, needs, base + 2, 1)
                    for way, k, needs in (
                        ("zw", 0, []), ("zd", -1, [plus]), ("zd", 1, [minus]), ("zw", 2, [on])
                    )
                ]
                here, there = {first: ALL}, {first: ALL, "z": rel(1)}
                ph = add(quarter, forth, here, line, base + 3, 4)
                add(quarter, back, here, line, base + 3, 4)
                add(quarter, forth, there, over, base + 4, 4)
                mt = add(quarter, back, there, over, base + 4, 4)
                add(quarter, forth, here | {second: rel(-1)}, [ph], base + 5, 4)
                add(quarter, back, there | {second: rel(1)}, [mt], base + 5, 4)
    return out


def near(send):
    return (send.way[0] == "z") == (send.at["z"] != ME)


def work_list(sends):
    def kind(name, *index):
        return [s for s in sends if s.kind == name and (not index or s.index in index)]

    def stage(k):
        return [s for s in sends if s.stage == k]

    last = stage(3)
    out = [("norm", k, 1.0, kind("swap")) for k in range(4)]
    out += [("norm", k, 1.0, kind("token") + kind("relay")) for k in range(4, 8)]
    out += [("mix", k, 1.6 if k % 3 == 2 else 0.8, stage(0)) for k in range(6)]
    out += [("mate", k, 1.0, stage(1)) for k in range(2)]
    out += [("sum", k, 0.7, kind("mate")) for k in range(2)]
    out += [("mix", k, 1.6 if k % 3 == 2 else 0.8, []) for k in range(6, 12)]
    out += [("home", k, 1.0, []) for k in range(2)]
    out += [("again", k, 1.4, kind("home") + kind("sum", k)) for k in range(2)]
    out += [("hide", k, 0.95, kind("again") + stage(2)) for k in range(11)]
    out += [("down", k, 1.5, [s for s in last if near(s)]) for k in range(2)]
    out += [("down", k, 1.5, last) for k in range(2, 4)]
    return out


def plan(ranks=RANKS):
    sends = all_sends()
    if ranks:
        for send, rank in zip(sends, ranks, strict=True):
            send.rank = rank
    work = work_list(sends)
    number = {id(send): i for i, send in enumerate(sends)}
    followers, missing = {}, []
    for i, send in enumerate(sends):
        missing.append(len(send.needs))
        for need in send.needs:
            key = need if isinstance(need, tuple) else number[id(need)]
            followers.setdefault(key, []).append(i)
    ready = {send.way: [] for send in sends}
    free = dict.fromkeys(ready, 0.0)
    got, flying, steps, held, now = set(), [], [], [], 0.0

    def release(i):
        if sends[i].kind == "part" and sends[i].stage > 1 and now < HOLD:
            held.append(i)
        else:
            heapq.heappush(ready[sends[i].way], (sends[i].rank, i))

    def arrive(key):
        got.add(key)
        for i in followers.get(key, ()):
            missing[i] -= 1
            if missing[i] == 0:
                release(i)

    def top_up():
        if now >= HOLD:
            while held:
                release(held.pop())
        for way, queue in ready.items():
            while queue and (queue[0][0] < 0 or free[way] - now <= BACKLOG):
                i = heapq.heappop(queue)[1]
                free[way] = max(free[way], now) + sends[i].time
                heapq.heappush(flying, (free[way] + sends[i].latency, i))
                steps.append(("start", i))

    for i, count in enumerate(missing):
        if count == 0:
            release(i)
    top_up()
    step = 0
    needs = [[number[id(need)] for need in piece[3]] for piece in work]
    while flying or step < len(work):
        while flying and flying[0][0] <= now:
            i = heapq.heappop(flying)[1]
            steps.append(("wait", i))
            arrive(i)
            top_up()
        if step < len(work) and got.issuperset(needs[step]):
            name, j, time, _ = work[step]
            step += 1
            steps.append((name, j))
            now += time
            arrive((name, j))
            top_up()
        elif flying:
            now = max(now, flying[0][0])
    return sends, steps, now


def region(send, place):
    at = []
    for dim, extent in (("z", 2), ("y", 4), ("x", 4)):
        how = send.at[dim]
        if how == ALL:
            at.append(pl.ds(0, extent))
        elif how[0] == "half":
            at.append(pl.ds(2 * how[1], 2))
        else:
            at.append(pl.ds(lax.rem(place[dim] + how[1] + extent, extent), 1))
    return (*at, pl.ds(16 * send.quarter, 16), pl.ds(0, WIDTHS[send.stage]))


def kernel(
    tokens, gain_one, w_b, w_c, w_v, taps, w_mix, gain_two, w_g, w_u, w_d, total, came_two,
    s0, s1, s2, s3, raw, normed, gated, to_mate, from_mate, summed, mate_sum, to_home, from_home,
    resid, hidden, gain_v, taps_v, gain_two_v, acc_b, acc_c, local_sem, send_sem, recv_sem,
):
    sends, steps, _ = plan()
    buffers = (s0, s1, s2, s3)
    rep, zl, y, x, tp = (lax.axis_index(name) for name in REP_FS_TP)
    me = {"z": zl, "y": y, "x": x}

    def device(way):
        if way == "pair":
            return (rep, zl, y, x, 1 - tp)
        if way == "zd":
            return (rep, 1 - zl, y, x, tp)
        if way == "zw":
            return (1 - rep, 1 - zl, y, x, tp)
        step = 1 if way[1] == "+" else 3
        if way[0] == "x":
            return (rep, zl, y, lax.rem(x + step, 4), tp)
        return (rep, zl, lax.rem(y + step, 4), x, tp)

    def rows_of(core, start=0, n=H):
        return pl.ds(pl.multiple_of(core * H + start, 32), n)

    mine, other = rows_of(tp), rows_of(1 - tp)

    def local(k, src, dst):
        return pltpu.make_async_copy(src, dst, local_sem.at[k])

    def slot(buffer, lo, n):
        return buffer.at[zl, y, x, pl.ds(0, 64), pl.ds(lo, n)]

    def share(weight):
        return weight.at[:, pl.ds(pl.multiple_of(rep * 512, 512), 512)]

    locals_ = [
        local(0, share(w_b), slot(s0, 0, 512)),
        local(1, share(w_c), slot(s0, 512, 512)),
        local(2, share(w_v), slot(s0, 1024, 512)),
        local(3, share(w_mix), slot(s1, 0, 512)),
        local(4, w_g, slot(s2, 0, 1408)),
        local(5, w_u, slot(s2, 1408, 1408)),
        local(6, w_d, slot(s3, 0, 1408)),
        local(7, tokens, raw.at[0, mine, :]),
        local(8, gain_one, gain_v),
        local(9, taps, taps_v),
        local(10, gain_two, gain_two_v),
    ]
    ready_of = ((0, 1, 2), (3,), (4, 5), (6,))
    for copy in locals_:
        copy.start()

    barrier = pltpu.get_barrier_semaphore()
    ways = ("x+", "x-", "y+", "y-", "zd", "zw", "pair")
    for way in ways:
        pl.semaphore_signal(barrier, inc=1, device_id=device(way), device_id_type=MESH)
    pl.semaphore_wait(barrier, len(ways))

    def ends(send, place, core):
        j = send.index
        cols = None if j is None else pl.ds(1024 * (j % 2), 1024)
        if send.kind == "part":
            where = buffers[send.stage].at[region(send, place)]
            return where, where
        if send.kind == "token":
            return tokens.at[pl.ds(160 * j, 160), :], raw.at[1, rows_of(core, 160 * j, 160), :]
        if send.kind == "relay":
            where = raw.at[1, rows_of(core, 160 * j, 160), :]
            return where, where
        if send.kind == "swap":
            return tokens, raw.at[0, rows_of(core), :]
        if send.kind == "mate":
            return to_mate.at[:, cols], from_mate.at[:, cols]
        if send.kind == "sum":
            rows = pl.ds(160 * j, 160)
            return summed.at[rows, :], mate_sum.at[rows, :]
        if send.kind == "home":
            return to_home.at[:, cols], from_home.at[:, cols]
        if send.kind == "again":
            where = normed.at[0, rows_of(core, 160 * j, 160), :]
            return where, where
        lanes = half_of(j, place["z"])
        return to_mate.at[:, lanes], came_two.at[:, lanes]

    def half_of(j, z):
        return pl.ds(pl.multiple_of(1024 * lax.rem(z + j, 2), 1024), 1024)

    def copy_of(i, place, core):
        src, dst = ends(sends[i], place, core)
        return pltpu.make_async_remote_copy(
            src_ref=src, dst_ref=dst, send_sem=send_sem.at[i], recv_sem=recv_sem.at[i],
            device_id=device(sends[i].way), device_id_type=MESH,
        )

    def outgoing(i):
        return copy_of(i, me, tp)

    def incoming(i):
        way, place = sends[i].way, dict(me)
        if way in ("zd", "zw"):
            place["z"] = 1 - zl
        elif way != "pair":
            place[way[0]] = lax.rem(me[way[0]] + (3 if way[1] == "+" else 1), 4)
        return copy_of(i, place, 1 - tp if way == "pair" else tp)

    def scaled(values, gain):
        factor = lax.rsqrt(jnp.mean(values * values, axis=-1, keepdims=True) + 1e-06)
        return (values * factor * gain).astype(BF16)

    def norm(step):
        c, part = step // 4, step % 4
        if step == 0:
            locals_[7].wait()
            locals_[8].wait()
        gain = gain_v[...]

        def chunk(r, carry):
            rows = pl.ds(pl.multiple_of(r * 32, 32), 32)
            normed[c, rows, :] = scaled(raw[c, rows, :].astype(F32), gain)
            return carry

        lax.fori_loop(5 * part, 5 * part + 5, chunk, 0)

    def mix(step):
        c, j, k = 1 - step // 6, step // 3 % 2, step % 3
        if step == 0:
            locals_[9].wait()

        def dot(k):
            w = s0[:, :, :, :, pl.ds(512 * k + 256 * j, 256)].reshape(D, 256)
            return jnp.dot(normed[c], w, preferred_element_type=F32).astype(BF16)

        if k < 2:
            (acc_b, acc_c)[k][...] = dot(k)
            return
        mixed = acc_c[...].astype(F32) * dot(2).astype(F32)
        row = lax.broadcasted_iota(jnp.int32, (T, 256), 0)
        one = jnp.where(row >= 1, pltpu.roll(mixed, 1, 0), 0.0)
        two = jnp.where(row >= 2, pltpu.roll(mixed, 2, 0), 0.0)
        lanes = pl.ds(pl.multiple_of(tp * 1024 + rep * 512 + 256 * j, 256), 256)
        tap = [taps_v[pl.ds(k, 1), lanes] for k in range(3)]
        convolved = tap[0] * two + tap[1] * one + tap[2] * mixed
        gated[c, :, pl.ds(256 * j, 256)] = (acc_b[...].astype(F32) * convolved).astype(BF16)

    def block(left, right):
        return lax.dot_general(left, right, (((1,), (1,)), ((), ())), preferred_element_type=F32)

    def product(c, j, away):
        def one(k, carry):
            cols = pl.ds(pl.multiple_of(1024 * j + 256 * k, 256), 256)
            w = s1[j, k].reshape(256, 512)
            away[:, cols] = block(gated[c, other, :], w).astype(BF16)
            resid[:, cols] = block(gated[c, mine, :], w)
            return carry

        lax.fori_loop(0, 4, one, 0)

    def mate(j):
        product(1, j, to_mate)

    def home(j):
        product(0, j, to_home)

    def add_up(p):
        def chunk(r, carry):
            rows = pl.ds(pl.multiple_of(160 * p + r * 32, 32), 32)
            summed[rows, :] = (resid[rows, :] + from_mate[rows, :].astype(F32)).astype(BF16)
            return carry

        lax.fori_loop(0, 5, chunk, 0)

    def again(p):
        if p == 0:
            locals_[10].wait()
        gain = gain_two_v[...]

        def chunk(r, carry):
            rows = pl.ds(pl.multiple_of(160 * p + r * 32, 32), 32)
            here = pl.ds(pl.multiple_of(tp * H + 160 * p + r * 32, 32), 32)
            sums = resid[rows, :] + from_home[rows, :].astype(F32)
            sums = sums + mate_sum[rows, :].astype(F32)
            values = raw[0, here, :].astype(F32) + sums
            resid[rows, :] = values
            normed[0, here, :] = scaled(values, gain)
            return carry

        lax.fori_loop(0, 5, chunk, 0)

    def hide(k):
        w_gate = s2[:, :, :, :, pl.ds(128 * k, 128)].reshape(D, 128)
        w_up = s2[:, :, :, :, pl.ds(1408 + 128 * k, 128)].reshape(D, 128)
        both = jnp.dot(
            normed[0], jnp.concatenate([w_gate, w_up], axis=1), preferred_element_type=F32
        )
        gate, up = both[:, :128], both[:, 128:]
        hidden[:, pl.ds(128 * k, 128)] = (gate / (1.0 + jnp.exp(-gate)) * up).astype(BF16)

    def down_home(j):
        cols = half_of(j, zl)
        return local(j, resid.at[:, cols], total.at[:, cols])

    def down(step):
        j = step // 2
        plane = lax.rem(zl + j, 2)

        def theirs(k, carry):
            cols = pl.ds(pl.multiple_of(1024 * plane + 256 * k, 256), 256)
            w = s3[plane, k].reshape(256, 1408)
            to_mate[:, cols] = block(hidden[other, :], w).astype(BF16)
            return carry

        def ours(k, carry):
            cols = pl.ds(pl.multiple_of(1024 * plane + 256 * k, 256), 256)
            own = block(hidden[mine, :], s3[plane, k].reshape(256, 1408)).astype(BF16)
            resid[:, cols] = resid[:, cols] + 0.5 * own.astype(F32)
            return carry

        if step == 0:
            for i, send in enumerate(sends):
                if send.kind == "mate":
                    outgoing(i).wait_send()
        if step % 2 == 0:
            lax.fori_loop(0, 4, theirs, 0)
        else:
            lax.fori_loop(0, 4, ours, 0)
            down_home(j).start()

    act = {
        "norm": norm, "mix": mix, "mate": mate, "sum": add_up, "home": home, "again": again,
        "hide": hide, "down": down,
    }
    landed = set()
    for what, i in steps:
        if what == "start":
            send = sends[i]
            if send.kind == "part" and send.stage not in landed:
                landed.add(send.stage)
                for k in ready_of[send.stage]:
                    locals_[k].wait()
            outgoing(i).start()
        elif what == "wait":
            incoming(i).wait_recv()
        else:
            act[what](i)

    for i, send in enumerate(sends):
        if send.kind != "mate":
            outgoing(i).wait_send()
    for j in range(2):
        down_home(j).wait()


def on_device(
    tokens, mix_gain, w_bgate, w_cgate, w_value, conv_taps, w_mixout, mlp_gain, w_gate, w_up, w_down
):
    count = len(all_sends())
    anywhere = pl.BlockSpec(memory_space=pl.ANY)
    total, came = pl.pallas_call(
        kernel,
        name="residual_block",
        out_shape=(jax.ShapeDtypeStruct((H, D), F32), jax.ShapeDtypeStruct((H, D), BF16)),
        in_specs=[anywhere] * 11,
        out_specs=(anywhere, anywhere),
        scratch_shapes=[
            *[pltpu.VMEM((2, 4, 4, 64, width), BF16) for width in WIDTHS],
            pltpu.VMEM((2, T, D), BF16),
            pltpu.VMEM((2, T, D), BF16),
            pltpu.VMEM((2, T, 512), BF16),
            *[pltpu.VMEM((H, D), BF16)] * 6,
            pltpu.VMEM((H, D), F32),
            pltpu.VMEM((T, 1408), BF16),
            pltpu.VMEM((1, D), F32),
            pltpu.VMEM((3, D), F32),
            pltpu.VMEM((1, D), F32),
            pltpu.VMEM((T, 256), BF16),
            pltpu.VMEM((T, 256), BF16),
            pltpu.SemaphoreType.DMA((11,)),
            pltpu.SemaphoreType.DMA((count,)),
            pltpu.SemaphoreType.DMA((count,)),
        ],
        compiler_params=pltpu.CompilerParams(
            collective_id=0, has_side_effects=True, vmem_limit_bytes=67043328
        ),
    )(
        tokens, mix_gain[None], w_bgate, w_cgate, w_value, conv_taps, w_mixout.T,
        mlp_gain[None], w_gate, w_up, w_down.T,
    )
    return (total + 0.5 * came.astype(F32)).astype(BF16)


def solution(mesh):
    finer = Mesh(
        mesh.devices.reshape(mesh.shape["rep"], 2, 4, 4, mesh.shape["tp"]),
        ("rep", "fs_0", "fs_1", "fs_2", "tp"),
    )
    return jax.shard_map(
        on_device,
        mesh=finer,
        in_specs=(
            P(REP_FS_TP, None),
            P(),
            P(FS, "tp"),
            P(FS, "tp"),
            P(FS, "tp"),
            P(),
            P("tp", FS),
            P(),
            P(FS, "tp"),
            P(FS, "tp"),
            P("tp", FS),
        ),
        out_specs=P(REP_FS_TP, None),
        check_vma=False,
    )
```

```python
import heapq

import jax
import jax.numpy as jnp
from jax import lax
from jax.experimental import pallas as pl
from jax.experimental.pallas import tpu as pltpu
from jax.sharding import Mesh
from jax.sharding import PartitionSpec as P

FS = ("fs_0", "fs_1", "fs_2")
REP_FS_TP = ("rep", "fs_0", "fs_1", "fs_2", "tp")
MESH = pl.DeviceIdType.MESH
BF16, F32 = jnp.bfloat16, jnp.float32

D = 2048
T = 640
H = 320
WIDTHS = (1536, 512, 2816, 1408)
LINK = 45.6e3
PAIR = 500.0e3
LATENCY = 2.6
PAIR_LATENCY = 1.5
BACKLOG = 3.63
HOLD = 0.0

RANKS = (
    -2, -2, -2, -2, -3, -4, -4, -4, -4, -4, -4, -4, -4, -4, -4, 0, 0, 0, 0, 180, 0, 0, 0, 86,
    610, 932, 0, 0, 253, 1060, 152, 152, 0, 0, 657, 0, 76, 66, 0, 1303, 0, 0, 0, 0, 0, 174, 0,
    0, 1304, 0, 347, 0, 0, 38, 0, 0, 0, 0, 0, 0, 0, 0, 0, 0, 191, 0, 133, 0, 305, 142, 758,
    1182, 976, 844, 1933, 1743, 2379, 382, 1059, 2039, 960, 383, 810, 501, 1142, 911, 159,
    279, 0, 336, 1479, 508, 2417, 1070, 2346, 1253, 1178, 1180, 1781, 937, 543, 872, 36, 835,
    619, 0, 409, 1297, 605, 1329, 1832, 599, 0, 0, 1089, 2275, 0, 0, 903, 0, 512, 301, 2029,
    62, 733, 1508, 2212, 2892, 1842, 2040, 2501, 2127, 1964, 2098, 1464, 2393, 1730, 2390,
    1605, 2886, 3497, 85, 1970, 2672, 2035, 2441, 2542, 1890, 3075, 1917, 3166, 1683, 1850,
    1351, 2360, 2190, 2195, 2128, 1539, 2430, 2304, 1355, 2861, 3162, 2038, 2675, 1621, 2660,
    2806, 2379, 2168, 1408, 1888, 645, 2875, 3370, 2129, 1855, 2554, 2152, 2733, 878, 2605,
    3136, 2152, 2804, 2540, 2990, 2399, 4163, 2270, 2567, 2758, 4079, 2763, 3264, 4850, 3769,
    2914, 3168, 3413, 3179, 3976, 3214, 3858, 2758, 3674, 2067, 4128, 4220, 3085, 4208, 2998,
    1946, 3153, 3902, 3715, 3731, 4469, 3206, 4713, 3271, 4368, 4244, 4523, 2114, 2052, 2732,
    3026, 3628, 2666, 1819, 2988, 3263, 4367, 2146, 2494, 3611,
)

ALL = ("all",)
ME = ("rel", 0)


def half(k):
    return ("half", k)


def rel(k):
    return ("rel", k)


class Send:
    def __init__(self, kind, way, needs, rank, size, stage=None, quarter=None, at=None, index=None):
        self.kind, self.way, self.needs, self.rank = kind, way, needs, rank
        self.stage, self.quarter, self.at, self.index = stage, quarter, at, index
        self.time = size / (PAIR if way == "pair" else LINK)
        self.latency = PAIR_LATENCY if way == "pair" else LATENCY


def all_sends():
    out = []

    def add(quarter, way, at, needs, rank, pieces):
        at = {"z": ME, "y": ME, "x": ME} | at
        size = pieces * 16 * WIDTHS[stage] * 2
        send = Send("part", way, list(needs), rank, size, stage, quarter, at)
        out.append(send)
        return send

    def other(kind, way, needs, rank, size, index, stage=None):
        send = Send(kind, way, list(needs), rank, size, stage, None, None, index)
        out.append(send)
        return send

    row = D * 2
    for p in range(2):
        token = other("token", "zw", [], -2, 160 * row, p)
        other("relay", "pair", [token], -2, 160 * row, p)
    other("swap", "pair", [], -3, H * row, 0)
    for j in range(2):
        other("mate", "pair", [("mate", j)], -4, H * 1024 * 2, j)
        other("sum", "zw", [("sum", j)], -4, 160 * row, j)
        other("home", "pair", [("home", j)], -4, H * 1024 * 2, j)
        other("again", "pair", [("again", j)], -4, 160 * row, j)
        other("down", "pair", [("down", 2 * j)], -4, H * 1024 * 2, j)

    for stage in range(2):
        base = 10 * stage
        orders = (("x", "y"), ("x", "y"), ("y", "x"), ("y", "x") if stage == 0 else ("x", "y"))
        for quarter, (first, second) in enumerate(orders):
            if quarter == 3:
                over = [add(quarter, "zd", {}, [], base, 1)]
                for far in range(2):
                    z = {"z": rel(far)}
                    start = over if far else []
                    plus = add(quarter, first + "+", z, start, base + far, 1)
                    minus = add(quarter, first + "-", z, start, base + far, 1)
                    if far:
                        on = add(quarter, first + "-", z | {first: rel(1)}, [minus], base + 2, 1)
                    else:
                        on = add(quarter, first + "+", z | {first: rel(-1)}, [plus], base + 2, 1)
                    line = [plus, minus, on] + start
                    z = z | {first: ALL}
                    plus = add(quarter, second + "+", z, line, base + 3, 4)
                    minus = add(quarter, second + "-", z, line, base + 3, 4)
                    if far:
                        add(quarter, second + "-", z | {second: rel(1)}, [minus], base + 4, 4)
                    else:
                        add(quarter, second + "+", z | {second: rel(-1)}, [plus], base + 4, 4)
                continue
            forth, back = first + "+", first + "-"
            plus = add(quarter, forth, {}, [], base, 1)
            minus = add(quarter, back, {}, [], base, 1)
            if quarter == 1:
                on = add(quarter, back, {first: rel(1)}, [minus], base + 1, 1)
            else:
                on = add(quarter, forth, {first: rel(-1)}, [plus], base + 1, 1)
            line = [plus, minus, on]
            over = [
                add(quarter, "zd", {first: rel(k)}, needs, base + 1, 1)
                for k, needs in ((0, []), (-1, [plus]), (1, [minus]), (2, [on]))
            ]
            forth, back = second + "+", second + "-"
            if quarter == 0:
                pa = add(quarter, forth, {first: half(0)}, line, base + 2, 2)
                pb = add(quarter, forth, {first: half(1)}, line, base + 3, 2)
                ma = add(quarter, back, {first: half(1)}, line, base + 2, 2)
                mb = add(quarter, back, {first: half(0)}, line, base + 3, 2)
                po = add(quarter, forth, {first: half(0), second: rel(-1)}, [pa], base + 4, 2)
                mo = add(quarter, back, {first: half(1), second: rel(1)}, [ma], base + 4, 2)
                add(quarter, "zd", {first: ALL, second: rel(-1)}, [pa, pb], base + 5, 4)
                add(quarter, "zd", {first: ALL, second: rel(1)}, [ma, mb], base + 5, 4)
                add(quarter, "zd", {first: ALL, second: rel(2)}, [po, mo], base + 6, 4)
            else:
                here, there = {first: ALL}, {first: ALL, "z": rel(1)}
                ph = add(quarter, forth, here, line, base + 3, 4)
                add(quarter, back, here, line, base + 3, 4)
                add(quarter, forth, there, over, base + 4, 4)
                mt = add(quarter, back, there, over, base + 4, 4)
                add(quarter, forth, here | {second: rel(-1)}, [ph], base + 5, 4)
                add(quarter, back, there | {second: rel(1)}, [mt], base + 5, 4)
    orders = (("x", "y"), ("y", "x"), ("x", "y"), ("y", "x"))
    for stage in range(2, 4):
        base = 20 + 10 * (stage - 2)
        early = 14 + 8 * (stage - 2)
        wrap = "zw" if stage == 2 else "zd"
        for quarter, (first, second) in enumerate(orders):
            forth, back = first + "+", first + "-"
            plus = add(quarter, forth, {}, [], early, 1)
            minus = add(quarter, back, {}, [], early, 1)
            if quarter < 2:
                on = add(quarter, forth, {first: rel(-1)}, [plus], early, 1)
            else:
                on = add(quarter, back, {first: rel(1)}, [minus], early, 1)
            line = [plus, minus, on]
            forth, back = second + "+", second + "-"
            if quarter < 4 - stage:
                pa = add(quarter, forth, {first: half(0)}, line, base + 2, 2)
                pb = add(quarter, forth, {first: half(1)}, line, base + 3, 2)
                ma = add(quarter, back, {first: half(1)}, line, base + 2, 2)
                mb = add(quarter, back, {first: half(0)}, line, base + 3, 2)
                po = add(quarter, forth, {first: half(0), second: rel(-1)}, [pa], base + 4, 2)
                mo = add(quarter, back, {first: half(1), second: rel(1)}, [ma], base + 4, 2)
                add(quarter, "zw", {}, [], early, 1)
                add(quarter, "zw", {first: rel(-1)}, [plus], early, 1)
                add(quarter, "zw", {first: rel(1)}, [minus], early, 1)
                add(quarter, "zw", {first: rel(2)}, [on], early, 1)
                soon = "zw" if stage == 2 and quarter == 0 else "zd"
                add(quarter, soon, {first: ALL, second: rel(-1)}, [pa, pb], base + 5, 4)
                add(quarter, "zd", {first: ALL, second: rel(1)}, [ma, mb], base + 5, 4)
                add(quarter, "zd", {first: ALL, second: rel(2)}, [po, mo], base + 6, 4)
            else:
                over = [
                    add(quarter, way, {first: rel(k)}, needs, base + 2, 1)
                    for way, k, needs in (
                        (wrap, 0, []), (wrap, -1, [plus]), ("zd", 1, [minus]), (wrap, 2, [on])
                    )
                ]
                here, there = {first: ALL}, {first: ALL, "z": rel(1)}
                ph = add(quarter, forth, here, line, base + 3, 4)
                add(quarter, back, here, line, base + 3, 4)
                add(quarter, forth, there, over, base + 4, 4)
                mt = add(quarter, back, there, over, base + 4, 4)
                add(quarter, forth, here | {second: rel(-1)}, [ph], base + 5, 4)
                add(quarter, back, there | {second: rel(1)}, [mt], base + 5, 4)
    return out


def near(send):
    return (send.way[0] == "z") == (send.at["z"] != ME)


def work_list(sends):
    def kind(name, *index):
        return [s for s in sends if s.kind == name and (not index or s.index in index)]

    def stage(k):
        return [s for s in sends if s.stage == k]

    last = stage(3)
    out = [("norm", k, 1.0, kind("swap")) for k in range(4)]
    out += [("norm", k, 1.0, kind("token") + kind("relay")) for k in range(4, 8)]
    out += [("mix", k, 1.3 if k % 3 == 2 else 0.7, stage(0)) for k in range(6)]
    out += [("mate", k, 1.0, stage(1)) for k in range(2)]
    out += [("sum", k, 0.7, kind("mate")) for k in range(2)]
    out += [("mix", k, 1.3 if k % 3 == 2 else 0.7, []) for k in range(6, 12)]
    out += [("home", k, 1.0, []) for k in range(2)]
    out += [("again", k, 1.4, kind("home") + kind("sum", k)) for k in range(2)]
    out += [("hide", k, 0.72, kind("again") + stage(2)) for k in range(11)]
    out += [("down", k, 1.5, [s for s in last if near(s)]) for k in range(2)]
    out += [("down", k, 1.5, last) for k in range(2, 4)]
    return out


def plan(ranks=RANKS):
    sends = all_sends()
    if ranks:
        for send, rank in zip(sends, ranks, strict=True):
            send.rank = rank
    work = work_list(sends)
    number = {id(send): i for i, send in enumerate(sends)}
    followers, missing = {}, []
    for i, send in enumerate(sends):
        missing.append(len(send.needs))
        for need in send.needs:
            key = need if isinstance(need, tuple) else number[id(need)]
            followers.setdefault(key, []).append(i)
    ready = {send.way: [] for send in sends}
    free = dict.fromkeys(ready, 0.0)
    got, flying, steps, held, now = set(), [], [], [], 0.0

    def release(i):
        if sends[i].kind == "part" and sends[i].stage > 1 and now < HOLD:
            held.append(i)
        else:
            heapq.heappush(ready[sends[i].way], (sends[i].rank, i))

    def arrive(key):
        got.add(key)
        for i in followers.get(key, ()):
            missing[i] -= 1
            if missing[i] == 0:
                release(i)

    def top_up():
        if now >= HOLD:
            while held:
                release(held.pop())
        for way, queue in ready.items():
            while queue and (queue[0][0] < 0 or free[way] - now <= BACKLOG):
                i = heapq.heappop(queue)[1]
                free[way] = max(free[way], now) + sends[i].time
                heapq.heappush(flying, (free[way] + sends[i].latency, i))
                steps.append(("start", i))

    for i, count in enumerate(missing):
        if count == 0:
            release(i)
    top_up()
    step = 0
    needs = [[number[id(need)] for need in piece[3]] for piece in work]
    while flying or step < len(work):
        while flying and flying[0][0] <= now:
            i = heapq.heappop(flying)[1]
            steps.append(("wait", i))
            arrive(i)
            top_up()
        if step < len(work) and got.issuperset(needs[step]):
            name, j, time, _ = work[step]
            step += 1
            steps.append((name, j))
            now += time
            arrive((name, j))
            top_up()
        elif flying:
            now = max(now, flying[0][0])
    return sends, eager(sends, steps, work, number), now


def eager(sends, steps, work, number):
    queues, followed, pieces = {}, set(), {(piece[0], piece[1]): piece for piece in work}
    for what, i in steps:
        if what == "start":
            queues.setdefault(sends[i].way, []).append(i)
    needs = {}
    for i, send in enumerate(sends):
        needs[i] = [n if isinstance(n, tuple) else number[id(n)] for n in send.needs]
        followed.update(needs[i])
    out, got = [], set()

    def start_all():
        for queue in queues.values():
            while queue and got.issuperset(needs[queue[0]]):
                out.append(("start", queue.pop(0)))

    def wait_for(i):
        if i not in got:
            got.add(i)
            out.append(("wait", i))
            start_all()

    start_all()
    for what, i in steps:
        if what == "wait" and i in followed:
            wait_for(i)
        elif what not in ("start", "wait"):
            for need in pieces[what, i][3]:
                wait_for(number[id(need)])
            out.append((what, i))
            got.add((what, i))
            start_all()
    for i in range(len(sends)):
        wait_for(i)
    return out


def region(send, place):
    at = []
    for dim, extent in (("z", 2), ("y", 4), ("x", 4)):
        how = send.at[dim]
        if how == ALL:
            at.append(pl.ds(0, extent))
        elif how[0] == "half":
            at.append(pl.ds(2 * how[1], 2))
        else:
            at.append(pl.ds(lax.rem(place[dim] + how[1] + extent, extent), 1))
    return (*at, pl.ds(16 * send.quarter, 16), pl.ds(0, WIDTHS[send.stage]))


def kernel(
    tokens, gain_one, w_b, w_c, w_v, taps, w_mix, gain_two, w_g, w_u, w_d, total, came_two,
    s0, s1, s2, s3, raw, normed, gated, to_mate, from_mate, summed, mate_sum, to_home, from_home,
    resid, hidden, gain_v, taps_v, gain_two_v, acc_b, acc_c, local_sem, send_sem, recv_sem,
):
    sends, steps, _ = plan()
    buffers = (s0, s1, s2, s3)
    rep, zl, y, x, tp = (lax.axis_index(name) for name in REP_FS_TP)
    me = {"z": zl, "y": y, "x": x}

    def device(way):
        if way == "pair":
            return (rep, zl, y, x, 1 - tp)
        if way == "zd":
            return (rep, 1 - zl, y, x, tp)
        if way == "zw":
            return (1 - rep, 1 - zl, y, x, tp)
        step = 1 if way[1] == "+" else 3
        if way[0] == "x":
            return (rep, zl, y, lax.rem(x + step, 4), tp)
        return (rep, zl, lax.rem(y + step, 4), x, tp)

    def rows_of(core, start=0, n=H):
        return pl.ds(pl.multiple_of(core * H + start, 32), n)

    mine, other = rows_of(tp), rows_of(1 - tp)

    def local(k, src, dst):
        return pltpu.make_async_copy(src, dst, local_sem.at[k])

    def slot(buffer, lo, n):
        return buffer.at[zl, y, x, pl.ds(0, 64), pl.ds(lo, n)]

    def share(weight):
        return weight.at[:, pl.ds(pl.multiple_of(rep * 512, 512), 512)]

    locals_ = [
        local(0, share(w_b), slot(s0, 0, 512)),
        local(1, share(w_c), slot(s0, 512, 512)),
        local(2, share(w_v), slot(s0, 1024, 512)),
        local(3, share(w_mix), slot(s1, 0, 512)),
        local(4, w_g, slot(s2, 0, 1408)),
        local(5, w_u, slot(s2, 1408, 1408)),
        local(6, w_d, slot(s3, 0, 1408)),
        local(7, tokens, raw.at[0, mine, :]),
        local(8, gain_one, gain_v),
        local(9, taps, taps_v),
        local(10, gain_two, gain_two_v),
    ]
    ready_of = ((0, 1, 2), (3,), (4, 5), (6,))
    for copy in locals_:
        copy.start()

    barrier = pltpu.get_barrier_semaphore()
    ways = ("x+", "x-", "y+", "y-", "zd", "zw", "pair")
    for way in ways:
        pl.semaphore_signal(barrier, inc=1, device_id=device(way), device_id_type=MESH)
    pl.semaphore_wait(barrier, len(ways))

    def ends(send, place, core):
        j = send.index
        cols = None if j is None else pl.ds(1024 * (j % 2), 1024)
        if send.kind == "part":
            where = buffers[send.stage].at[region(send, place)]
            return where, where
        if send.kind == "token":
            return tokens.at[pl.ds(160 * j, 160), :], raw.at[1, rows_of(core, 160 * j, 160), :]
        if send.kind == "relay":
            where = raw.at[1, rows_of(core, 160 * j, 160), :]
            return where, where
        if send.kind == "swap":
            return tokens, raw.at[0, rows_of(core), :]
        if send.kind == "mate":
            return to_mate.at[:, cols], from_mate.at[:, cols]
        if send.kind == "sum":
            rows = pl.ds(160 * j, 160)
            return summed.at[rows, :], mate_sum.at[rows, :]
        if send.kind == "home":
            return to_home.at[:, cols], from_home.at[:, cols]
        if send.kind == "again":
            where = normed.at[0, rows_of(core, 160 * j, 160), :]
            return where, where
        lanes = half_of(j, place["z"])
        return to_mate.at[:, lanes], came_two.at[:, lanes]

    def half_of(j, z):
        return pl.ds(pl.multiple_of(1024 * lax.rem(z + j, 2), 1024), 1024)

    def copy_of(i, place, core):
        src, dst = ends(sends[i], place, core)
        return pltpu.make_async_remote_copy(
            src_ref=src, dst_ref=dst, send_sem=send_sem.at[i], recv_sem=recv_sem.at[i],
            device_id=device(sends[i].way), device_id_type=MESH,
        )

    def outgoing(i):
        return copy_of(i, me, tp)

    def incoming(i):
        way, place = sends[i].way, dict(me)
        if way in ("zd", "zw"):
            place["z"] = 1 - zl
        elif way != "pair":
            place[way[0]] = lax.rem(me[way[0]] + (3 if way[1] == "+" else 1), 4)
        return copy_of(i, place, 1 - tp if way == "pair" else tp)

    def scaled(values, gain):
        factor = lax.rsqrt(jnp.mean(values * values, axis=-1, keepdims=True) + 1e-06)
        return (values * factor * gain).astype(BF16)

    def norm(step):
        c, part = step // 4, step % 4
        if step == 0:
            locals_[7].wait()
            locals_[8].wait()
        gain = gain_v[...]

        def chunk(r, carry):
            rows = pl.ds(pl.multiple_of(r * 32, 32), 32)
            normed[c, rows, :] = scaled(raw[c, rows, :].astype(F32), gain)
            return carry

        lax.fori_loop(5 * part, 5 * part + 5, chunk, 0)

    def mix(step):
        c, j, k = 1 - step // 6, step // 3 % 2, step % 3
        if step == 0:
            locals_[9].wait()

        def dot(k):
            w = s0[:, :, :, :, pl.ds(512 * k + 256 * j, 256)].reshape(D, 256)
            return jnp.dot(normed[c], w, preferred_element_type=F32).astype(BF16)

        if k < 2:
            (acc_b, acc_c)[k][...] = dot(k)
            return
        mixed = acc_c[...].astype(F32) * dot(2).astype(F32)
        row = lax.broadcasted_iota(jnp.int32, (T, 256), 0)
        one = jnp.where(row >= 1, pltpu.roll(mixed, 1, 0), 0.0)
        two = jnp.where(row >= 2, pltpu.roll(mixed, 2, 0), 0.0)
        lanes = pl.ds(pl.multiple_of(tp * 1024 + rep * 512 + 256 * j, 256), 256)
        tap = [taps_v[pl.ds(k, 1), lanes] for k in range(3)]
        convolved = tap[0] * two + tap[1] * one + tap[2] * mixed
        gated[c, :, pl.ds(256 * j, 256)] = (acc_b[...].astype(F32) * convolved).astype(BF16)

    def block(left, right):
        return lax.dot_general(left, right, (((1,), (1,)), ((), ())), preferred_element_type=F32)

    def product(c, j, away):
        def one(k, carry):
            cols = pl.ds(pl.multiple_of(1024 * j + 256 * k, 256), 256)
            w = s1[j, k].reshape(256, 512)
            away[:, cols] = block(gated[c, other, :], w).astype(BF16)
            resid[:, cols] = block(gated[c, mine, :], w)
            return carry

        lax.fori_loop(0, 4, one, 0)

    def mate(j):
        product(1, j, to_mate)

    def home(j):
        product(0, j, to_home)

    def add_up(p):
        def chunk(r, carry):
            rows = pl.ds(pl.multiple_of(160 * p + r * 32, 32), 32)
            summed[rows, :] = (resid[rows, :] + from_mate[rows, :].astype(F32)).astype(BF16)
            return carry

        lax.fori_loop(0, 5, chunk, 0)

    def again(p):
        if p == 0:
            locals_[10].wait()
        gain = gain_two_v[...]

        def chunk(r, carry):
            rows = pl.ds(pl.multiple_of(160 * p + r * 32, 32), 32)
            here = pl.ds(pl.multiple_of(tp * H + 160 * p + r * 32, 32), 32)
            sums = resid[rows, :] + from_home[rows, :].astype(F32)
            sums = sums + mate_sum[rows, :].astype(F32)
            values = raw[0, here, :].astype(F32) + sums
            resid[rows, :] = values
            normed[0, here, :] = scaled(values, gain)
            return carry

        lax.fori_loop(0, 5, chunk, 0)

    def hide(k):
        w_gate = s2[:, :, :, :, pl.ds(128 * k, 128)].reshape(D, 128)
        w_up = s2[:, :, :, :, pl.ds(1408 + 128 * k, 128)].reshape(D, 128)
        both = jnp.dot(
            normed[0], jnp.concatenate([w_gate, w_up], axis=1), preferred_element_type=F32
        )
        gate, up = both[:, :128], both[:, 128:]
        hidden[:, pl.ds(128 * k, 128)] = (gate / (1.0 + jnp.exp(-gate)) * up).astype(BF16)

    def down(step):
        j = step // 2
        plane = lax.rem(zl + j, 2)

        def theirs(k, carry):
            cols = pl.ds(pl.multiple_of(1024 * plane + 256 * k, 256), 256)
            w = s3[plane, k].reshape(256, 1408)
            to_mate[:, cols] = block(hidden[other, :], w).astype(BF16)
            return carry

        def ours(k, carry):
            cols = pl.ds(pl.multiple_of(1024 * plane + 256 * k, 256), 256)
            own = block(hidden[mine, :], s3[plane, k].reshape(256, 1408)).astype(BF16)
            total[:, cols] = resid[:, cols] + 0.5 * own.astype(F32)
            return carry

        if step == 0:
            for i, send in enumerate(sends):
                if send.kind == "mate":
                    outgoing(i).wait_send()
        if step % 2 == 0:
            lax.fori_loop(0, 4, theirs, 0)
        else:
            lax.fori_loop(0, 4, ours, 0)

    act = {
        "norm": norm, "mix": mix, "mate": mate, "sum": add_up, "home": home, "again": again,
        "hide": hide, "down": down,
    }
    landed = set()
    for what, i in steps:
        if what == "start":
            send = sends[i]
            if send.kind == "part" and send.stage not in landed:
                landed.add(send.stage)
                for k in ready_of[send.stage]:
                    locals_[k].wait()
            outgoing(i).start()
        elif what == "wait":
            incoming(i).wait_recv()
        else:
            act[what](i)

    for i, send in enumerate(sends):
        if send.kind != "mate":
            outgoing(i).wait_send()


def on_device(
    tokens, mix_gain, w_bgate, w_cgate, w_value, conv_taps, w_mixout, mlp_gain, w_gate, w_up, w_down
):
    count = len(all_sends())
    anywhere = pl.BlockSpec(memory_space=pl.ANY)
    total, came = pl.pallas_call(
        kernel,
        name="residual_block",
        out_shape=(pltpu.VMEM((H, D), F32), pltpu.VMEM((H, D), BF16)),
        in_specs=[anywhere] * 11,
        out_specs=(pl.BlockSpec(memory_space=pltpu.VMEM),) * 2,
        scratch_shapes=[
            *[pltpu.VMEM((2, 4, 4, 64, width), BF16) for width in WIDTHS],
            pltpu.VMEM((2, T, D), BF16),
            pltpu.VMEM((2, T, D), BF16),
            pltpu.VMEM((2, T, 512), BF16),
            *[pltpu.VMEM((H, D), BF16)] * 6,
            pltpu.VMEM((H, D), F32),
            pltpu.VMEM((T, 1408), BF16),
            pltpu.VMEM((1, D), F32),
            pltpu.VMEM((3, D), F32),
            pltpu.VMEM((1, D), F32),
            pltpu.VMEM((T, 256), BF16),
            pltpu.VMEM((T, 256), BF16),
            pltpu.SemaphoreType.DMA((11,)),
            pltpu.SemaphoreType.DMA((count,)),
            pltpu.SemaphoreType.DMA((count,)),
        ],
        compiler_params=pltpu.CompilerParams(
            collective_id=0, has_side_effects=True, vmem_limit_bytes=60 * 2**20
        ),
    )(
        tokens, mix_gain[None], w_bgate, w_cgate, w_value, conv_taps, w_mixout.T,
        mlp_gain[None], w_gate, w_up, w_down.T,
    )
    return (total + 0.5 * came.astype(F32)).astype(BF16)


def solution(mesh):
    finer = Mesh(
        mesh.devices.reshape(mesh.shape["rep"], 2, 4, 4, mesh.shape["tp"]),
        ("rep", "fs_0", "fs_1", "fs_2", "tp"),
    )
    return jax.shard_map(
        on_device,
        mesh=finer,
        in_specs=(
            P(REP_FS_TP, None),
            P(),
            P(FS, "tp"),
            P(FS, "tp"),
            P(FS, "tp"),
            P(),
            P("tp", FS),
            P(),
            P(FS, "tp"),
            P(FS, "tp"),
            P("tp", FS),
        ),
        out_specs=P(REP_FS_TP, None),
        check_vma=False,
    )
```

```python
import heapq

import jax
import jax.numpy as jnp
from jax import lax
from jax.experimental import pallas as pl
from jax.experimental.pallas import tpu as pltpu
from jax.sharding import Mesh
from jax.sharding import PartitionSpec as P

FS = ("fs_0", "fs_1", "fs_2")
REP_FS_TP = ("rep", "fs_0", "fs_1", "fs_2", "tp")
MESH = pl.DeviceIdType.MESH
BF16, F32 = jnp.bfloat16, jnp.float32

D = 2048
T = 640
H = 320
WIDTHS = (1536, 512, 2816, 1408)
LINK = 45.1e3
PAIR = 500.0e3
LATENCY = 3.4
PAIR_LATENCY = 1.8
BACKLOG = 2.93
HOLD = 0.0

RANKS = (
    -2, -2, -2, -2, -3, -4, -4, -4, -4, -4, -4, -4, -4, -4, -4, 1002, 1057, 1057, 1292, 1292,
    1292, 1292, 1113, 1182, 1113, 1182, 1182, 1182, 1252, 1252, 1252, 1198, 988, 946, 1100,
    1100, 1100, 1140, 1155, 1252, 1252, 1155, 1252, 1246, 988, 1044, 1044, 1100, 1100, 1100,
    1075, 1155, 1252, 1252, 1155, 1272, 1405, 988, 1044, 1100, 1100, 1155, 1138, 1252, 1102,
    989, 1100, 1252, 1155, 1252, 1142, 1202, 1266, 1337, 1337, 1337, 1310, 1229, 1277, 1229,
    1277, 1277, 1274, 1416, 1355, 1324, 1181, 1138, 1181, 1225, 1287, 1225, 1399, 1268, 1297,
    1324, 1268, 1324, 1324, 1203, 1181, 1181, 1225, 1225, 1395, 1225, 1268, 1324, 1245, 1268,
    1161, 1324, 1138, 1181, 1225, 1225, 1268, 1324, 1324, 1225, 1181, 1290, 1324, 1268, 1414,
    1526, 1573, 1548, 1620, 1716, 1637, 1685, 1685, 1685, 1801, 1833, 1801, 1796, 1749, 1749,
    1714, 1526, 1573, 1546, 1620, 1685, 1620, 1685, 1685, 1685, 1893, 1627, 1854, 1801, 1749,
    1749, 1749, 1556, 1509, 1556, 1603, 1603, 1639, 1603, 1650, 1749, 1749, 1650, 1855, 1749,
    1486, 1509, 1556, 1603, 1603, 1603, 1603, 1588, 1749, 1749, 1650, 1749, 1761, 1815, 1787,
    1947, 1755, 1849, 1804, 1849, 1736, 1843, 1948, 1829, 2034, 1948, 1824, 1921, 1921, 1728,
    1781, 1781, 1815, 1843, 1815, 1749, 1863, 1883, 1921, 1938, 1883, 1981, 1781, 1753, 1812,
    1815, 1815, 1815, 1821, 1755, 1883, 1921, 1854, 1860, 1964, 1781, 1754, 1781, 1815, 1815,
    1698, 1815, 1836, 1883, 1921, 1854, 1883, 1921,
)

ALL = ("all",)
ME = ("rel", 0)


def half(k):
    return ("half", k)


def rel(k):
    return ("rel", k)


class Send:
    def __init__(self, kind, way, needs, rank, size, stage=None, quarter=None, at=None, index=None):
        self.kind, self.way, self.needs, self.rank = kind, way, needs, rank
        self.stage, self.quarter, self.at, self.index = stage, quarter, at, index
        self.time = size / (PAIR if way == "pair" else LINK)
        self.latency = PAIR_LATENCY if way == "pair" else LATENCY


def all_sends():
    out = []

    def add(quarter, way, at, needs, rank, pieces):
        at = {"z": ME, "y": ME, "x": ME} | at
        size = pieces * 16 * WIDTHS[stage] * 2
        send = Send("part", way, list(needs), rank, size, stage, quarter, at)
        out.append(send)
        return send

    def other(kind, way, needs, rank, size, index, stage=None):
        send = Send(kind, way, list(needs), rank, size, stage, None, None, index)
        out.append(send)
        return send

    row = D * 2
    for p in range(2):
        token = other("token", "zw", [], -2, 160 * row, p)
        other("relay", "pair", [token], -2, 160 * row, p)
    other("swap", "pair", [], -3, H * row, 0)
    for j in range(2):
        other("mate", "pair", [("mate", j)], -4, H * 1024 * 2, j)
        other("sum", "zw", [("sum", j)], -4, 160 * row, j)
        other("home", "pair", [("home", j)], -4, H * 1024 * 2, j)
        other("again", "pair", [("again", j)], -4, 160 * row, j)
        other("down", "pair", [("down", 2 * j)], -4, H * 1024 * 2, j)

    for stage in range(2):
        base = 10 * stage
        orders = (("x", "y"), ("x", "y"), ("y", "x"), ("y", "x"))
        for quarter, (first, second) in enumerate(orders):
            if quarter == 3:
                over = [add(quarter, "zd", {}, [], base, 1)]
                for far in range(2):
                    if far and stage == 0:
                        first, second = second, first
                    z = {"z": rel(far)}
                    start = over if far else []
                    plus = add(quarter, first + "+", z, start, base + far, 1)
                    minus = add(quarter, first + "-", z, start, base + far, 1)
                    if far:
                        on = add(quarter, first + "-", z | {first: rel(1)}, [minus], base + 2, 1)
                    else:
                        on = add(quarter, first + "+", z | {first: rel(-1)}, [plus], base + 2, 1)
                    line = [plus, minus, on] + start
                    z = z | {first: ALL}
                    plus = add(quarter, second + "+", z, line, base + 3, 4)
                    minus = add(quarter, second + "-", z, line, base + 3, 4)
                    if far:
                        add(quarter, second + "-", z | {second: rel(1)}, [minus], base + 4, 4)
                    else:
                        add(quarter, second + "+", z | {second: rel(-1)}, [plus], base + 4, 4)
                continue
            forth, back = first + "+", first + "-"
            plus = add(quarter, forth, {}, [], base, 1)
            minus = add(quarter, back, {}, [], base, 1)
            if quarter == 1:
                on = add(quarter, back, {first: rel(1)}, [minus], base + 1, 1)
            else:
                on = add(quarter, forth, {first: rel(-1)}, [plus], base + 1, 1)
            line = [plus, minus, on]
            over = [
                add(quarter, "zd", {first: rel(k)}, needs, base + 1, 1)
                for k, needs in ((0, []), (-1, [plus]), (1, [minus]), (2, [on]))
            ]
            forth, back = second + "+", second + "-"
            if quarter == 0:
                pa = add(quarter, forth, {first: half(0)}, line, base + 2, 2)
                pb = add(quarter, forth, {first: half(1)}, line, base + 3, 2)
                ma = add(quarter, back, {first: half(1)}, line, base + 2, 2)
                mb = add(quarter, back, {first: half(0)}, line, base + 3, 2)
                po = add(quarter, forth, {first: half(0), second: rel(-1)}, [pa], base + 4, 2)
                mo = add(quarter, back, {first: half(1), second: rel(1)}, [ma], base + 4, 2)
                add(quarter, "zd", {first: ALL, second: rel(-1)}, [pa, pb], base + 5, 4)
                add(quarter, "zd", {first: ALL, second: rel(1)}, [ma, mb], base + 5, 4)
                final = "zw" if stage == 3 else "zd"
                add(quarter, final, {first: ALL, second: rel(2)}, [po, mo], base + 6, 4)
            else:
                here, there = {first: ALL}, {first: ALL, "z": rel(1)}
                ph = add(quarter, forth, here, line, base + 3, 4)
                add(quarter, back, here, line, base + 3, 4)
                add(quarter, forth, there, over, base + 4, 4)
                mt = add(quarter, back, there, over, base + 4, 4)
                add(quarter, forth, here | {second: rel(-1)}, [ph], base + 5, 4)
                add(quarter, back, there | {second: rel(1)}, [mt], base + 5, 4)
    orders = (("x", "y"), ("y", "x"), ("x", "y"), ("y", "x"))
    for stage in range(2, 4):
        base = 20 + 10 * (stage - 2)
        early = 14 + 8 * (stage - 2)
        wrap = "zw" if stage == 2 else "zd"
        for quarter, (first, second) in enumerate(orders):
            forth, back = first + "+", first + "-"
            plus = add(quarter, forth, {}, [], early, 1)
            minus = add(quarter, back, {}, [], early, 1)
            if quarter < 2:
                on = add(quarter, forth, {first: rel(-1)}, [plus], early, 1)
            else:
                on = add(quarter, back, {first: rel(1)}, [minus], early, 1)
            line = [plus, minus, on]
            forth, back = second + "+", second + "-"
            if quarter < 4 - stage:
                pa = add(quarter, forth, {first: half(0)}, line, base + 2, 2)
                pb = add(quarter, forth, {first: half(1)}, line, base + 3, 2)
                ma = add(quarter, back, {first: half(1)}, line, base + 2, 2)
                mb = add(quarter, back, {first: half(0)}, line, base + 3, 2)
                po = add(quarter, forth, {first: half(0), second: rel(-1)}, [pa], base + 4, 2)
                mo = add(quarter, back, {first: half(1), second: rel(1)}, [ma], base + 4, 2)
                add(quarter, "zw", {}, [], early, 1)
                add(quarter, "zw", {first: rel(-1)}, [plus], early, 1)
                add(quarter, "zw", {first: rel(1)}, [minus], early, 1)
                add(quarter, "zw", {first: rel(2)}, [on], early, 1)
                soon = "zw" if stage == 2 and quarter == 0 else "zd"
                add(quarter, soon, {first: ALL, second: rel(-1)}, [pa, pb], base + 5, 4)
                add(quarter, "zd", {first: ALL, second: rel(1)}, [ma, mb], base + 5, 4)
                final = "zw" if stage == 3 else "zd"
                add(quarter, final, {first: ALL, second: rel(2)}, [po, mo], base + 6, 4)
            else:
                over = [
                    add(quarter, way, {first: rel(k)}, needs, base + 2, 1)
                    for way, k, needs in (
                        (wrap, 0, []), (wrap, -1, [plus]), ("zd", 1, [minus]), (wrap, 2, [on])
                    )
                ]
                here, there = {first: ALL}, {first: ALL, "z": rel(1)}
                ph = add(quarter, forth, here, line, base + 3, 4)
                add(quarter, back, here, line, base + 3, 4)
                add(quarter, forth, there, over, base + 4, 4)
                mt = add(quarter, back, there, over, base + 4, 4)
                add(quarter, forth, here | {second: rel(-1)}, [ph], base + 5, 4)
                add(quarter, back, there | {second: rel(1)}, [mt], base + 5, 4)
    return out


def near(send):
    return (send.way[0] == "z") == (send.at["z"] != ME)


def work_list(sends):
    def kind(name, *index):
        return [s for s in sends if s.kind == name and (not index or s.index in index)]

    def stage(k):
        return [s for s in sends if s.stage == k]

    last = stage(3)
    out = [("norm", k, 1.0, kind("swap")) for k in range(4)]
    out += [("norm", k, 1.0, kind("token") + kind("relay")) for k in range(4, 8)]
    out += [("mix", k, 1.3 if k % 3 == 2 else 0.7, stage(0)) for k in range(6)]
    out += [("mate", k, 1.0, stage(1)) for k in range(2)]
    out += [("sum", k, 0.7, kind("mate")) for k in range(2)]
    out += [("mix", k, 1.3 if k % 3 == 2 else 0.7, []) for k in range(6, 12)]
    out += [("home", k, 1.0, []) for k in range(2)]
    out += [("again", k, 1.4, kind("home") + kind("sum", k)) for k in range(2)]
    out += [("pre", k, 0.4, kind("again") + [s for s in stage(2) if near(s)]) for k in range(11)]
    out += [("hide", k, 0.42, stage(2)) for k in range(11)]
    out += [("down", 0, 2.1, [s for s in last if near(s)])]
    out += [("down", k, 1.5, last) for k in range(2, 4)]
    return out


def plan(ranks=RANKS):
    sends = all_sends()
    if ranks:
        for send, rank in zip(sends, ranks, strict=True):
            send.rank = rank
    work = work_list(sends)
    number = {id(send): i for i, send in enumerate(sends)}
    followers, missing = {}, []
    for i, send in enumerate(sends):
        missing.append(len(send.needs))
        for need in send.needs:
            key = need if isinstance(need, tuple) else number[id(need)]
            followers.setdefault(key, []).append(i)
    ready = {send.way: [] for send in sends}
    free = dict.fromkeys(ready, 0.0)
    got, flying, steps, held, now = set(), [], [], [], 0.0

    def release(i):
        if sends[i].kind == "part" and sends[i].stage > 1 and now < HOLD:
            held.append(i)
        else:
            heapq.heappush(ready[sends[i].way], (sends[i].rank, i))

    def arrive(key):
        got.add(key)
        for i in followers.get(key, ()):
            missing[i] -= 1
            if missing[i] == 0:
                release(i)

    def top_up():
        if now >= HOLD:
            while held:
                release(held.pop())
        for way, queue in ready.items():
            while queue and (queue[0][0] < 0 or free[way] - now <= BACKLOG):
                i = heapq.heappop(queue)[1]
                free[way] = max(free[way], now) + sends[i].time
                heapq.heappush(flying, (free[way] + sends[i].latency, i))
                steps.append(("start", i))

    for i, count in enumerate(missing):
        if count == 0:
            release(i)
    top_up()
    step = 0
    needs = [[number[id(need)] for need in piece[3]] for piece in work]
    while flying or step < len(work):
        while flying and flying[0][0] <= now:
            i = heapq.heappop(flying)[1]
            steps.append(("wait", i))
            arrive(i)
            top_up()
        if step < len(work) and got.issuperset(needs[step]):
            name, j, time, _ = work[step]
            step += 1
            steps.append((name, j))
            now += time
            arrive((name, j))
            top_up()
        elif flying:
            now = max(now, flying[0][0])
    return sends, eager(sends, steps, work, number), now


def eager(sends, steps, work, number):
    queues, followed, pieces = {}, set(), {(piece[0], piece[1]): piece for piece in work}
    for what, i in steps:
        if what == "start":
            queues.setdefault(sends[i].way, []).append(i)
    needs = {}
    for i, send in enumerate(sends):
        needs[i] = [n if isinstance(n, tuple) else number[id(n)] for n in send.needs]
        followed.update(needs[i])
    out, got = [], set()

    def start_all():
        for queue in queues.values():
            while queue and got.issuperset(needs[queue[0]]):
                out.append(("start", queue.pop(0)))

    def wait_for(i):
        if i not in got:
            got.add(i)
            out.append(("wait", i))
            start_all()

    start_all()
    for what, i in steps:
        if what == "wait" and i in followed:
            wait_for(i)
        elif what not in ("start", "wait"):
            for need in pieces[what, i][3]:
                wait_for(number[id(need)])
            out.append((what, i))
            got.add((what, i))
            start_all()
    for i in range(len(sends)):
        wait_for(i)
    return out


def region(send, place):
    at = []
    for dim, extent in (("z", 2), ("y", 4), ("x", 4)):
        how = send.at[dim]
        if how == ALL:
            at.append(pl.ds(0, extent))
        elif how[0] == "half":
            at.append(pl.ds(2 * how[1], 2))
        else:
            at.append(pl.ds(lax.rem(place[dim] + how[1] + extent, extent), 1))
    return (*at, pl.ds(16 * send.quarter, 16), pl.ds(0, WIDTHS[send.stage]))


def kernel(
    tokens, gain_one, w_b, w_c, w_v, taps, w_mix, gain_two, w_g, w_u, w_d, total, came_two,
    s0, s1, s2, s3, raw, normed, gated, to_mate, from_mate, summed, mate_sum, to_home, from_home,
    resid, partial, hidden, gain_v, taps_v, gain_two_v, acc_b, acc_c, local_sem, send_sem, recv_sem,
):
    sends, steps, _ = plan()
    buffers = (s0, s1, s2, s3)
    rep, zl, y, x, tp = (lax.axis_index(name) for name in REP_FS_TP)
    me = {"z": zl, "y": y, "x": x}

    def device(way):
        if way == "pair":
            return (rep, zl, y, x, 1 - tp)
        if way == "zd":
            return (rep, 1 - zl, y, x, tp)
        if way == "zw":
            return (1 - rep, 1 - zl, y, x, tp)
        step = 1 if way[1] == "+" else 3
        if way[0] == "x":
            return (rep, zl, y, lax.rem(x + step, 4), tp)
        return (rep, zl, lax.rem(y + step, 4), x, tp)

    def rows_of(core, start=0, n=H):
        return pl.ds(pl.multiple_of(core * H + start, 32), n)

    mine, other = rows_of(tp), rows_of(1 - tp)

    def local(k, src, dst):
        return pltpu.make_async_copy(src, dst, local_sem.at[k])

    def slot(buffer, lo, n):
        return buffer.at[zl, y, x, pl.ds(0, 64), pl.ds(lo, n)]

    def share(weight):
        return weight.at[:, pl.ds(pl.multiple_of(rep * 512, 512), 512)]

    locals_ = [
        local(0, share(w_b), slot(s0, 0, 512)),
        local(1, share(w_c), slot(s0, 512, 512)),
        local(2, share(w_v), slot(s0, 1024, 512)),
        local(3, share(w_mix), slot(s1, 0, 512)),
        local(4, w_g, slot(s2, 0, 1408)),
        local(5, w_u, slot(s2, 1408, 1408)),
        local(6, w_d, slot(s3, 0, 1408)),
        local(7, tokens, raw.at[0, mine, :]),
        local(8, gain_one, gain_v),
        local(9, taps, taps_v),
        local(10, gain_two, gain_two_v),
    ]
    ready_of = ((0, 1, 2), (3,), (4, 5), (6,))
    for copy in locals_:
        copy.start()

    barrier = pltpu.get_barrier_semaphore()
    ways = ("x+", "x-", "y+", "y-", "zd", "zw", "pair")
    for way in ways:
        pl.semaphore_signal(barrier, inc=1, device_id=device(way), device_id_type=MESH)
    pl.semaphore_wait(barrier, len(ways))

    def ends(send, place, core):
        j = send.index
        cols = None if j is None else pl.ds(1024 * (j % 2), 1024)
        if send.kind == "part":
            where = buffers[send.stage].at[region(send, place)]
            return where, where
        if send.kind == "token":
            return tokens.at[pl.ds(160 * j, 160), :], raw.at[1, rows_of(core, 160 * j, 160), :]
        if send.kind == "relay":
            where = raw.at[1, rows_of(core, 160 * j, 160), :]
            return where, where
        if send.kind == "swap":
            return tokens, raw.at[0, rows_of(core), :]
        if send.kind == "mate":
            return to_mate.at[:, cols], from_mate.at[:, cols]
        if send.kind == "sum":
            rows = pl.ds(160 * j, 160)
            return summed.at[rows, :], mate_sum.at[rows, :]
        if send.kind == "home":
            return to_home.at[:, cols], from_home.at[:, cols]
        if send.kind == "again":
            where = normed.at[rows_of(core, 160 * j, 160), :]
            return where, where
        lanes = half_of(j, place["z"])
        return to_mate.at[:, lanes], came_two.at[:, lanes]

    def half_of(j, z):
        return pl.ds(pl.multiple_of(1024 * lax.rem(z + j, 2), 1024), 1024)

    def copy_of(i, place, core):
        src, dst = ends(sends[i], place, core)
        return pltpu.make_async_remote_copy(
            src_ref=src, dst_ref=dst, send_sem=send_sem.at[i], recv_sem=recv_sem.at[i],
            device_id=device(sends[i].way), device_id_type=MESH,
        )

    def outgoing(i):
        return copy_of(i, me, tp)

    def incoming(i):
        way, place = sends[i].way, dict(me)
        if way in ("zd", "zw"):
            place["z"] = 1 - zl
        elif way != "pair":
            place[way[0]] = lax.rem(me[way[0]] + (3 if way[1] == "+" else 1), 4)
        return copy_of(i, place, 1 - tp if way == "pair" else tp)

    def scaled(values, gain):
        factor = lax.rsqrt(jnp.mean(values * values, axis=-1, keepdims=True) + 1e-06)
        return (values * factor * gain).astype(BF16)

    def norm(step):
        c, part = step // 4, step % 4
        if step == 0:
            locals_[7].wait()
            locals_[8].wait()
        if step == 4:
            for i, send in enumerate(sends):
                if send.kind == "relay":
                    outgoing(i).wait_send()
        gain = gain_v[...]

        def chunk(r, carry):
            rows = pl.ds(pl.multiple_of(r * 32, 32), 32)
            values = scaled(raw[c, rows, :].astype(F32), gain)
            if c == 0:
                normed[rows, :] = values
            else:
                raw[c, rows, :] = values
            return carry

        lax.fori_loop(5 * part, 5 * part + 5, chunk, 0)

    def mix(step):
        c, j, k = 1 - step // 6, step // 3 % 2, step % 3
        if step == 0:
            locals_[9].wait()

        def dot(k):
            w = s0[:, :, :, :, pl.ds(512 * k + 256 * j, 256)].reshape(D, 256)
            left = raw[1] if c == 1 else normed[...]
            return jnp.dot(left, w, preferred_element_type=F32).astype(BF16)

        if k < 2:
            (acc_b, acc_c)[k][...] = dot(k)
            return
        mixed = acc_c[...].astype(F32) * dot(2).astype(F32)
        row = lax.broadcasted_iota(jnp.int32, (T, 256), 0)
        one = jnp.where(row >= 1, pltpu.roll(mixed, 1, 0), 0.0)
        two = jnp.where(row >= 2, pltpu.roll(mixed, 2, 0), 0.0)
        lanes = pl.ds(pl.multiple_of(tp * 1024 + rep * 512 + 256 * j, 256), 256)
        tap = [taps_v[pl.ds(k, 1), lanes] for k in range(3)]
        convolved = tap[0] * two + tap[1] * one + tap[2] * mixed
        gated[c, :, pl.ds(256 * j, 256)] = (acc_b[...].astype(F32) * convolved).astype(BF16)

    def block(left, right):
        return lax.dot_general(left, right, (((1,), (1,)), ((), ())), preferred_element_type=F32)

    def product(c, j, away):
        def one(k, carry):
            cols = pl.ds(pl.multiple_of(1024 * j + 256 * k, 256), 256)
            w = s1[j, k].reshape(256, 512)
            away[:, cols] = block(gated[c, other, :], w).astype(BF16)
            resid[:, cols] = block(gated[c, mine, :], w)
            return carry

        lax.fori_loop(0, 4, one, 0)

    def mate(j):
        product(1, j, to_mate)

    def home(j):
        product(0, j, to_home)

    def add_up(p):
        def chunk(r, carry):
            rows = pl.ds(pl.multiple_of(160 * p + r * 32, 32), 32)
            summed[rows, :] = (resid[rows, :] + from_mate[rows, :].astype(F32)).astype(BF16)
            return carry

        lax.fori_loop(0, 5, chunk, 0)

    def again(p):
        if p == 0:
            locals_[10].wait()
        gain = gain_two_v[...]

        def chunk(r, carry):
            rows = pl.ds(pl.multiple_of(160 * p + r * 32, 32), 32)
            here = pl.ds(pl.multiple_of(tp * H + 160 * p + r * 32, 32), 32)
            sums = resid[rows, :] + from_home[rows, :].astype(F32)
            sums = sums + mate_sum[rows, :].astype(F32)
            values = raw[0, here, :].astype(F32) + sums
            resid[rows, :] = values
            normed[here, :] = scaled(values, gain)
            return carry

        lax.fori_loop(0, 5, chunk, 0)

    def half_product(k, plane):
        w_gate = s2[plane, :, :, :, pl.ds(128 * k, 128)].reshape(D // 2, 128)
        w_up = s2[plane, :, :, :, pl.ds(1408 + 128 * k, 128)].reshape(D // 2, 128)
        left = normed[:, pl.ds(pl.multiple_of(1024 * plane, 1024), 1024)]
        return jnp.dot(
            left, jnp.concatenate([w_gate, w_up], axis=1), preferred_element_type=F32
        )

    def pre(k):
        partial[k] = half_product(k, zl)

    def hide(k):
        both = partial[k] + half_product(k, 1 - zl)
        gate, up = both[:, :128], both[:, 128:]
        hidden[:, pl.ds(128 * k, 128)] = (gate / (1.0 + jnp.exp(-gate)) * up).astype(BF16)

    def down(step):
        j = step // 2
        plane = lax.rem(zl + j, 2)

        def both(k, carry):
            cols = pl.ds(pl.multiple_of(1024 * plane + 256 * k, 256), 256)
            acc_b[...] = block(hidden[...], s3[plane, k].reshape(256, 1408)).astype(BF16)
            to_mate[:, cols] = acc_b[other, :]
            total[:, cols] = resid[:, cols] + 0.5 * acc_b[mine, :].astype(F32)
            return carry

        def theirs(k, carry):
            cols = pl.ds(pl.multiple_of(1024 * plane + 256 * k, 256), 256)
            w = s3[plane, k].reshape(256, 1408)
            to_mate[:, cols] = block(hidden[other, :], w).astype(BF16)
            return carry

        def ours(k, carry):
            cols = pl.ds(pl.multiple_of(1024 * plane + 256 * k, 256), 256)
            own = block(hidden[mine, :], s3[plane, k].reshape(256, 1408)).astype(BF16)
            total[:, cols] = resid[:, cols] + 0.5 * own.astype(F32)
            return carry

        if step == 0:
            for i, send in enumerate(sends):
                if send.kind == "mate":
                    outgoing(i).wait_send()
        lax.fori_loop(0, 4, (both, None, theirs, ours)[step], 0)

    act = {
        "norm": norm, "mix": mix, "mate": mate, "sum": add_up, "home": home, "again": again,
        "pre": pre, "hide": hide, "down": down,
    }
    landed = set()
    for what, i in steps:
        if what == "start":
            send = sends[i]
            if send.kind == "part" and send.stage not in landed:
                landed.add(send.stage)
                for k in ready_of[send.stage]:
                    locals_[k].wait()
            outgoing(i).start()
        elif what == "wait":
            incoming(i).wait_recv()
        else:
            act[what](i)

    for i, send in enumerate(sends):
        if send.kind not in ("mate", "relay"):
            outgoing(i).wait_send()


def on_device(
    tokens, mix_gain, w_bgate, w_cgate, w_value, conv_taps, w_mixout, mlp_gain, w_gate, w_up, w_down
):
    count = len(all_sends())
    anywhere = pl.BlockSpec(memory_space=pl.ANY)
    total, came = pl.pallas_call(
        kernel,
        name="residual_block",
        out_shape=(pltpu.VMEM((H, D), F32), pltpu.VMEM((H, D), BF16)),
        in_specs=[anywhere] * 11,
        out_specs=(pl.BlockSpec(memory_space=pltpu.VMEM),) * 2,
        scratch_shapes=[
            *[pltpu.VMEM((2, 4, 4, 64, width), BF16) for width in WIDTHS],
            pltpu.VMEM((2, T, D), BF16),
            pltpu.VMEM((T, D), BF16),
            pltpu.VMEM((2, T, 512), BF16),
            *[pltpu.VMEM((H, D), BF16)] * 6,
            pltpu.VMEM((H, D), F32),
            pltpu.VMEM((11, T, 256), F32),
            pltpu.VMEM((T, 1408), BF16),
            pltpu.VMEM((1, D), F32),
            pltpu.VMEM((3, D), F32),
            pltpu.VMEM((1, D), F32),
            pltpu.VMEM((T, 256), BF16),
            pltpu.VMEM((T, 256), BF16),
            pltpu.SemaphoreType.DMA((11,)),
            pltpu.SemaphoreType.DMA((count,)),
            pltpu.SemaphoreType.DMA((count,)),
        ],
        compiler_params=pltpu.CompilerParams(
            collective_id=0, has_side_effects=True, vmem_limit_bytes=60 * 2**20
        ),
    )(
        tokens, mix_gain[None], w_bgate, w_cgate, w_value, conv_taps, w_mixout.T,
        mlp_gain[None], w_gate, w_up, w_down.T,
    )
    return (total + 0.5 * came.astype(F32)).astype(BF16)


def solution(mesh):
    finer = Mesh(
        mesh.devices.reshape(mesh.shape["rep"], 2, 4, 4, mesh.shape["tp"]),
        ("rep", "fs_0", "fs_1", "fs_2", "tp"),
    )
    return jax.shard_map(
        on_device,
        mesh=finer,
        in_specs=(
            P(REP_FS_TP, None),
            P(),
            P(FS, "tp"),
            P(FS, "tp"),
            P(FS, "tp"),
            P(),
            P("tp", FS),
            P(),
            P(FS, "tp"),
            P(FS, "tp"),
            P("tp", FS),
        ),
        out_specs=P(REP_FS_TP, None),
        check_vma=False,
    )
```

```python
import heapq

import jax
import jax.numpy as jnp
from jax import lax
from jax.experimental import pallas as pl
from jax.experimental.pallas import tpu as pltpu
from jax.sharding import Mesh
from jax.sharding import PartitionSpec as P

FS = ("fs_0", "fs_1", "fs_2")
REP_FS_TP = ("rep", "fs_0", "fs_1", "fs_2", "tp")
MESH = pl.DeviceIdType.MESH
BF16, F32 = jnp.bfloat16, jnp.float32

D = 2048
T = 640
H = 320
WIDTHS = (1536, 512, 2816, 1408)
LINK = 45.1e3
PAIR = 500.0e3
LATENCY = 3.4
PAIR_LATENCY = 1.8
BACKLOG = 2.95
HOLD = 0.0

RANKS = (
    -2, -2, -2, -2, -3, -4, -4, -4, -4, 0, 88, 187, 1590, 957, 1545, 184, 423, 493, 24, 812,
    36, 637, 1224, 670, 757, 0, 0, 0, 0, 68, 0, 691, 400, 571, 1576, 633, 600, 1738, 120, 0,
    0, 0, 358, 0, 0, 561, 776, 42, 671, 530, 474, 348, 108, 229, 889, 531, 168, 852, 1144,
    819, 31, 0, 366, 555, 1355, 821, 409, 1017, 1145, 1346, 1295, 2765, 1203, 382, 1016, 608,
    553, 920, 1731, 1495, 1297, 624, 879, 366, 595, 2046, 412, 957, 776, 873, 1105, 1602,
    1168, 1061, 1407, 0, 1342, 849, 292, 650, 1034, 1494, 964, 1239, 988, 834, 654, 858, 177,
    976, 1513, 1131, 0, 732, 669, 727, 248, 1074, 687, 1048, 1010, 1056, 1644, -4, -4, -4, -4,
    -4, -4, -4, -4, -4, 1832, 2023, 1566, 2106, 2229, 2086, 2079, 2213, 2709, 2195, 3090,
    2502, 1936, 1397, 2530, 3318, 1319, 1669, 1282, 1291, 1180, 1451, 2163, 2091, 2290, 2416,
    3194, 2408, 2621, 2022, 2447, 2862, 1054, 1191, 2081, 1579, 1751, 1318, 2660, 1630, 2416,
    2667, 1884, 2554, 2715, 1209, 829, 1283, 1872, 1569, 2177, 1888, 2460, 2398, 1997, 1737,
    2884, 1606, 1381, 2229, 1643, 2400, 3414, 2461, 2657, 3025, 2783, 5092, 4152, 4053, 4506,
    4593, 4308, 3832, 1437, 2203, 1824, 3287, 2864, 4034, 3451, 2958, 3064, 4362, 4200, 4078,
    4107, 2520, 1039, 1527, 3538, 2839, 3301, 3279, 1794, 2685, 4717, 3921, 2142, 4068, 1247,
    2118, 1921, 2860, 3493, 3912, 3426, 2120, 2597, 4884, 2976, 2666, 4244,
)

SPANS = ((0, 160), (160, 96), (256, 64))

ALL = ("all",)
ME = ("rel", 0)


def half(k):
    return ("half", k)


def rel(k):
    return ("rel", k)


class Send:
    def __init__(self, kind, way, needs, rank, size, stage=None, quarter=None, at=None, index=None):
        self.kind, self.way, self.needs, self.rank = kind, way, needs, rank
        self.stage, self.quarter, self.at, self.index = stage, quarter, at, index
        self.time = size / (PAIR if way == "pair" else LINK)
        self.latency = PAIR_LATENCY if way == "pair" else LATENCY


def all_sends():
    out = []

    def add(quarter, way, at, needs, rank, pieces):
        at = {"z": ME, "y": ME, "x": ME} | at
        size = pieces * 16 * WIDTHS[stage] * 2
        send = Send("part", way, list(needs), rank, size, stage, quarter, at)
        out.append(send)
        return send

    def other(kind, way, needs, rank, size, index, stage=None):
        send = Send(kind, way, list(needs), rank, size, stage, None, None, index)
        out.append(send)
        return send

    row = D * 2
    for p in range(2):
        token = other("token", "zw", [], -2, 160 * row, p)
        other("relay", "pair", [token], -2, 160 * row, p)
    other("swap", "pair", [], -3, H * row, 0)
    for j in range(2):
        other("mate", "pair", [("mate", j)], -4, H * 1024 * 2, j)
        other("home", "pair", [("home", j)], -4, H * 1024 * 2, j)

    for stage in range(2):
        base = 10 * stage
        orders = (("x", "y"), ("x", "y"), ("y", "x"), ("y", "x"))
        for quarter, (first, second) in enumerate(orders):
            if quarter == 3:
                over = [add(quarter, "zd", {}, [], base, 1)]
                for far in range(2):
                    if far and stage == 0:
                        first, second = second, first
                    z = {"z": rel(far)}
                    start = over if far else []
                    plus = add(quarter, first + "+", z, start, base + far, 1)
                    minus = add(quarter, first + "-", z, start, base + far, 1)
                    if far:
                        on = add(quarter, first + "-", z | {first: rel(1)}, [minus], base + 2, 1)
                    else:
                        on = add(quarter, first + "+", z | {first: rel(-1)}, [plus], base + 2, 1)
                    line = [plus, minus, on] + start
                    z = z | {first: ALL}
                    plus = add(quarter, second + "+", z, line, base + 3, 4)
                    minus = add(quarter, second + "-", z, line, base + 3, 4)
                    z = {"z": rel(far)}
                    on, back = z | {second: rel(-1)}, z | {second: rel(1)}
                    add(quarter, second + "+", on | {first: half(0)}, [plus], base + 4, 2)
                    add(quarter, second + "-", back | {first: half(1)}, [minus], base + 4, 2)
                continue
            forth, back = first + "+", first + "-"
            plus = add(quarter, forth, {}, [], base, 1)
            minus = add(quarter, back, {}, [], base, 1)
            if quarter == 1:
                on = add(quarter, back, {first: rel(1)}, [minus], base + 1, 1)
            else:
                on = add(quarter, forth, {first: rel(-1)}, [plus], base + 1, 1)
            line = [plus, minus, on]
            over = [
                add(quarter, "zd", {first: rel(k)}, needs, base + 1, 1)
                for k, needs in ((0, []), (-1, [plus]), (1, [minus]), (2, [on]))
            ]
            forth, back = second + "+", second + "-"
            if quarter == 0:
                pa = add(quarter, forth, {first: half(0)}, line, base + 2, 2)
                pb = add(quarter, forth, {first: half(1)}, line, base + 3, 2)
                ma = add(quarter, back, {first: half(1)}, line, base + 2, 2)
                mb = add(quarter, back, {first: half(0)}, line, base + 3, 2)
                po = add(quarter, forth, {first: half(0), second: rel(-1)}, [pa], base + 4, 2)
                mo = add(quarter, back, {first: half(1), second: rel(1)}, [ma], base + 4, 2)
                add(quarter, "zd", {first: ALL, second: rel(-1)}, [pa, pb], base + 5, 4)
                add(quarter, "zd", {first: ALL, second: rel(1)}, [ma, mb], base + 5, 4)
                final = "zw" if stage == 3 else "zd"
                add(quarter, final, {first: ALL, second: rel(2)}, [po, mo], base + 6, 4)
            else:
                here, there = {first: ALL}, {first: ALL, "z": rel(1)}
                ph = add(quarter, forth, here, line, base + 3, 4)
                add(quarter, back, here, line, base + 3, 4)
                add(quarter, forth, there, over, base + 4, 4)
                mt = add(quarter, back, there, over, base + 4, 4)
                add(quarter, forth, here | {second: rel(-1)}, [ph], base + 5, 4)
                add(quarter, back, there | {second: rel(1)}, [mt], base + 5, 4)
    for j, (_, n) in enumerate(SPANS):
        other("sum", "zw", [("sum", j)], -4, n * row, j)
        other("again", "pair", [("again", j)], -4, n * row, j)
    for j, step in enumerate((0, 2, 3)):
        other("down", "pair", [("down", step)], -4, H * (512 if j else 1024) * 2, j)
    orders = (("x", "y"), ("y", "x"), ("x", "y"), ("y", "x"))
    for stage in range(2, 4):
        base = 20 + 10 * (stage - 2)
        early = 14 + 8 * (stage - 2)
        wrap = "zw" if stage == 2 else "zd"
        for quarter, (first, second) in enumerate(orders):
            forth, back = first + "+", first + "-"
            plus = add(quarter, forth, {}, [], early, 1)
            minus = add(quarter, back, {}, [], early, 1)
            if quarter < 2:
                on = add(quarter, forth, {first: rel(-1)}, [plus], early, 1)
            else:
                on = add(quarter, back, {first: rel(1)}, [minus], early, 1)
            line = [plus, minus, on]
            forth, back = second + "+", second + "-"
            if quarter < 4 - stage:
                pa = add(quarter, forth, {first: half(0)}, line, base + 2, 2)
                pb = add(quarter, forth, {first: half(1)}, line, base + 3, 2)
                ma = add(quarter, back, {first: half(1)}, line, base + 2, 2)
                mb = add(quarter, back, {first: half(0)}, line, base + 3, 2)
                po = add(quarter, forth, {first: half(0), second: rel(-1)}, [pa], base + 4, 2)
                mo = add(quarter, back, {first: half(1), second: rel(1)}, [ma], base + 4, 2)
                add(quarter, "zw", {}, [], early, 1)
                add(quarter, "zw", {first: rel(-1)}, [plus], early, 1)
                add(quarter, "zw", {first: rel(1)}, [minus], early, 1)
                add(quarter, "zw", {first: rel(2)}, [on], early, 1)
                soon = "zw" if stage == 2 and quarter == 0 else "zd"
                add(quarter, soon, {first: ALL, second: rel(-1)}, [pa, pb], base + 5, 4)
                add(quarter, "zd", {first: ALL, second: rel(1)}, [ma, mb], base + 5, 4)
                final = "zw" if stage == 3 else "zd"
                add(quarter, final, {first: ALL, second: rel(2)}, [po, mo], base + 6, 4)
            else:
                over = [
                    add(quarter, way, {first: rel(k)}, needs, base + 2, 1)
                    for way, k, needs in (
                        (wrap, 0, []), (wrap, -1, [plus]), ("zd", 1, [minus]), (wrap, 2, [on])
                    )
                ]
                here, there = {first: ALL}, {first: ALL, "z": rel(1)}
                ph = add(quarter, forth, here, line, base + 3, 4)
                add(quarter, back, here, line, base + 3, 4)
                add(quarter, forth, there, over, base + 4, 4)
                mt = add(quarter, back, there, over, base + 4, 4)
                add(quarter, forth, here | {second: rel(-1)}, [ph], base + 5, 4)
                add(quarter, back, there | {second: rel(1)}, [mt], base + 5, 4)
    return out


def near(send):
    return (send.way[0] == "z") == (send.at["z"] != ME)


def work_list(sends):
    def kind(name, *index):
        return [s for s in sends if s.kind == name and (not index or s.index in index)]

    def stage(k):
        return [s for s in sends if s.stage == k]

    last = stage(3)
    out = [("norm", k, 1.0, kind("swap")) for k in range(4)]
    out += [("norm", k, 1.0, kind("token") + kind("relay")) for k in range(4, 8)]
    out += [("mix", k, 1.3 if k % 3 == 2 else 0.7, stage(0)) for k in range(6)]
    out += [("mate", k, 1.0, stage(1)) for k in range(2)]
    out += [("sum", k, n / 230, kind("mate")) for k, (_, n) in enumerate(SPANS)]
    out += [("mix", k, 1.3 if k % 3 == 2 else 0.7, []) for k in range(6, 12)]
    out += [("home", k, 1.0, []) for k in range(2)]
    for k, (_, n) in enumerate(SPANS):
        out.append(("again", k, n / 115, kind("home") + kind("sum", k)))
    out += [("pre", k, 0.4, kind("again") + [s for s in stage(2) if near(s)]) for k in range(11)]
    out += [("hide", k, 0.42, stage(2)) for k in range(11)]
    out += [("down", 0, 2.1, [s for s in last if near(s)])]
    out += [("down", k, 1.5 if k == 4 else 0.75, last) for k in range(2, 5)]
    return out


def plan(ranks=RANKS):
    sends = all_sends()
    if ranks:
        for send, rank in zip(sends, ranks, strict=True):
            send.rank = rank
    work = work_list(sends)
    number = {id(send): i for i, send in enumerate(sends)}
    followers, missing = {}, []
    for i, send in enumerate(sends):
        missing.append(len(send.needs))
        for need in send.needs:
            key = need if isinstance(need, tuple) else number[id(need)]
            followers.setdefault(key, []).append(i)
    ready = {send.way: [] for send in sends}
    free = dict.fromkeys(ready, 0.0)
    got, flying, steps, held, now = set(), [], [], [], 0.0

    def release(i):
        if sends[i].kind == "part" and sends[i].stage > 1 and now < HOLD:
            held.append(i)
        else:
            heapq.heappush(ready[sends[i].way], (sends[i].rank, i))

    def arrive(key):
        got.add(key)
        for i in followers.get(key, ()):
            missing[i] -= 1
            if missing[i] == 0:
                release(i)

    def top_up():
        if now >= HOLD:
            while held:
                release(held.pop())
        for way, queue in ready.items():
            while queue and (queue[0][0] < 0 or free[way] - now <= BACKLOG):
                i = heapq.heappop(queue)[1]
                free[way] = max(free[way], now) + sends[i].time
                heapq.heappush(flying, (free[way] + sends[i].latency, i))
                steps.append(("start", i))

    for i, count in enumerate(missing):
        if count == 0:
            release(i)
    top_up()
    step = 0
    needs = [[number[id(need)] for need in piece[3]] for piece in work]
    while flying or step < len(work):
        while flying and flying[0][0] <= now:
            i = heapq.heappop(flying)[1]
            steps.append(("wait", i))
            arrive(i)
            top_up()
        if step < len(work) and got.issuperset(needs[step]):
            name, j, time, _ = work[step]
            step += 1
            steps.append((name, j))
            now += time
            arrive((name, j))
            top_up()
        elif flying:
            now = max(now, flying[0][0])
    return sends, eager(sends, steps, work, number), now


def eager(sends, steps, work, number):
    queues, followed, pieces = {}, set(), {(piece[0], piece[1]): piece for piece in work}
    for what, i in steps:
        if what == "start":
            queues.setdefault(sends[i].way, []).append(i)
    needs = {}
    for i, send in enumerate(sends):
        needs[i] = [n if isinstance(n, tuple) else number[id(n)] for n in send.needs]
        followed.update(needs[i])
    out, got = [], set()

    def start_all():
        for queue in queues.values():
            while queue and got.issuperset(needs[queue[0]]):
                out.append(("start", queue.pop(0)))

    def wait_for(i):
        if i not in got:
            got.add(i)
            out.append(("wait", i))
            start_all()

    start_all()
    for what, i in steps:
        if what == "wait" and i in followed:
            wait_for(i)
        elif what not in ("start", "wait"):
            for need in pieces[what, i][3]:
                wait_for(number[id(need)])
            out.append((what, i))
            got.add((what, i))
            start_all()
    for i in range(len(sends)):
        wait_for(i)
    return out


def region(send, place):
    at = []
    for dim, extent in (("z", 2), ("y", 4), ("x", 4)):
        how = send.at[dim]
        if how == ALL:
            at.append(pl.ds(0, extent))
        elif how[0] == "half":
            at.append(pl.ds(2 * how[1], 2))
        else:
            at.append(pl.ds(lax.rem(place[dim] + how[1] + extent, extent), 1))
    return (*at, pl.ds(16 * send.quarter, 16), pl.ds(0, WIDTHS[send.stage]))


def kernel(
    tokens, gain_one, w_b, w_c, w_v, taps, w_mix, gain_two, w_g, w_u, w_d, total, came_two,
    s0, s1, s2, s3, raw, normed, gated, to_mate, from_mate, summed, mate_sum, to_home, from_home,
    resid, partial, hidden, gain_v, taps_v, gain_two_v, acc_b, acc_c, local_sem, send_sem, recv_sem,
):
    sends, steps, _ = plan()
    buffers = (s0, s1, s2, s3)
    rep, zl, y, x, tp = (lax.axis_index(name) for name in REP_FS_TP)
    me = {"z": zl, "y": y, "x": x}

    def device(way):
        if way == "pair":
            return (rep, zl, y, x, 1 - tp)
        if way == "zd":
            return (rep, 1 - zl, y, x, tp)
        if way == "zw":
            return (1 - rep, 1 - zl, y, x, tp)
        step = 1 if way[1] == "+" else 3
        if way[0] == "x":
            return (rep, zl, y, lax.rem(x + step, 4), tp)
        return (rep, zl, lax.rem(y + step, 4), x, tp)

    def rows_of(core, start=0, n=H):
        return pl.ds(pl.multiple_of(core * H + start, 32), n)

    mine, other = rows_of(tp), rows_of(1 - tp)

    def local(k, src, dst):
        return pltpu.make_async_copy(src, dst, local_sem.at[k])

    def slot(buffer, lo, n):
        return buffer.at[zl, y, x, pl.ds(0, 64), pl.ds(lo, n)]

    def share(weight):
        return weight.at[:, pl.ds(pl.multiple_of(rep * 512, 512), 512)]

    locals_ = [
        local(0, share(w_b), slot(s0, 0, 512)),
        local(1, share(w_c), slot(s0, 512, 512)),
        local(2, share(w_v), slot(s0, 1024, 512)),
        local(3, share(w_mix), slot(s1, 0, 512)),
        local(4, w_g, slot(s2, 0, 1408)),
        local(5, w_u, slot(s2, 1408, 1408)),
        local(6, w_d, slot(s3, 0, 1408)),
        local(7, tokens, raw.at[0, mine, :]),
        local(8, gain_one, gain_v),
        local(9, taps, taps_v),
        local(10, gain_two, gain_two_v),
    ]
    ready_of = ((0, 1, 2), (3,), (4, 5), (6,))
    for copy in locals_:
        copy.start()

    barrier = pltpu.get_barrier_semaphore()
    ways = ("x+", "x-", "y+", "y-", "zd", "zw", "pair")
    for way in ways:
        pl.semaphore_signal(barrier, inc=1, device_id=device(way), device_id_type=MESH)
    pl.semaphore_wait(barrier, len(ways))

    def ends(send, place, core):
        j = send.index
        cols = None if j is None else pl.ds(1024 * (j % 2), 1024)
        if send.kind == "part":
            where = buffers[send.stage].at[region(send, place)]
            return where, where
        if send.kind == "token":
            return tokens.at[pl.ds(160 * j, 160), :], raw.at[1, rows_of(core, 160 * j, 160), :]
        if send.kind == "relay":
            where = raw.at[1, rows_of(core, 160 * j, 160), :]
            return where, where
        if send.kind == "swap":
            return tokens, raw.at[0, rows_of(core), :]
        if send.kind == "mate":
            return to_mate.at[:, cols], from_mate.at[:, cols]
        if send.kind == "sum":
            rows = pl.ds(*SPANS[j])
            return summed.at[rows, :], mate_sum.at[rows, :]
        if send.kind == "home":
            return to_home.at[:, cols], from_home.at[:, cols]
        if send.kind == "again":
            where = normed.at[rows_of(core, *SPANS[j]), :]
            return where, where
        start = 1024 * lax.rem(place["z"] + (j > 0), 2) + (512 if j == 2 else 0)
        lanes = pl.ds(pl.multiple_of(start, 512), 512 if j else 1024)
        return to_mate.at[:, lanes], came_two.at[:, lanes]

    def copy_of(i, place, core):
        src, dst = ends(sends[i], place, core)
        return pltpu.make_async_remote_copy(
            src_ref=src, dst_ref=dst, send_sem=send_sem.at[i], recv_sem=recv_sem.at[i],
            device_id=device(sends[i].way), device_id_type=MESH,
        )

    def outgoing(i):
        return copy_of(i, me, tp)

    def incoming(i):
        way, place = sends[i].way, dict(me)
        if way in ("zd", "zw"):
            place["z"] = 1 - zl
        elif way != "pair":
            place[way[0]] = lax.rem(me[way[0]] + (3 if way[1] == "+" else 1), 4)
        return copy_of(i, place, 1 - tp if way == "pair" else tp)

    def scaled(values, gain):
        factor = lax.rsqrt(jnp.mean(values * values, axis=-1, keepdims=True) + 1e-06)
        return (values * factor * gain).astype(BF16)

    def norm(step):
        c, part = step // 4, step % 4
        if step == 0:
            locals_[7].wait()
            locals_[8].wait()
        if step == 4:
            for i, send in enumerate(sends):
                if send.kind == "relay":
                    outgoing(i).wait_send()
        gain = gain_v[...]

        def chunk(r, carry):
            rows = pl.ds(pl.multiple_of(r * 32, 32), 32)
            values = scaled(raw[c, rows, :].astype(F32), gain)
            if c == 0:
                normed[rows, :] = values
            else:
                raw[c, rows, :] = values
            return carry

        lax.fori_loop(5 * part, 5 * part + 5, chunk, 0)

    def mix(step):
        c, j, k = 1 - step // 6, step // 3 % 2, step % 3
        if step == 0:
            locals_[9].wait()

        def dot(k):
            w = s0[:, :, :, :, pl.ds(512 * k + 256 * j, 256)].reshape(D, 256)
            left = raw[1] if c == 1 else normed[...]
            return jnp.dot(left, w, preferred_element_type=F32).astype(BF16)

        if k < 2:
            (acc_b, acc_c)[k][...] = dot(k)
            return
        mixed = acc_c[...].astype(F32) * dot(2).astype(F32)
        row = lax.broadcasted_iota(jnp.int32, (T, 256), 0)
        one = jnp.where(row >= 1, pltpu.roll(mixed, 1, 0), 0.0)
        two = jnp.where(row >= 2, pltpu.roll(mixed, 2, 0), 0.0)
        lanes = pl.ds(pl.multiple_of(tp * 1024 + rep * 512 + 256 * j, 256), 256)
        tap = [taps_v[pl.ds(k, 1), lanes] for k in range(3)]
        convolved = tap[0] * two + tap[1] * one + tap[2] * mixed
        gated[c, :, pl.ds(256 * j, 256)] = (acc_b[...].astype(F32) * convolved).astype(BF16)

    def block(left, right):
        return lax.dot_general(left, right, (((1,), (1,)), ((), ())), preferred_element_type=F32)

    def product(c, j, away):
        def one(k, carry):
            cols = pl.ds(pl.multiple_of(1024 * j + 256 * k, 256), 256)
            w = s1[j, k].reshape(256, 512)
            away[:, cols] = block(gated[c, other, :], w).astype(BF16)
            resid[:, cols] = block(gated[c, mine, :], w)
            return carry

        lax.fori_loop(0, 4, one, 0)

    def mate(j):
        product(1, j, to_mate)

    def home(j):
        product(0, j, to_home)

    def add_up(p):
        start, n = SPANS[p]

        def chunk(r, carry):
            rows = pl.ds(pl.multiple_of(start + r * 32, 32), 32)
            summed[rows, :] = (resid[rows, :] + from_mate[rows, :].astype(F32)).astype(BF16)
            return carry

        lax.fori_loop(0, n // 32, chunk, 0)

    def again(p):
        start, n = SPANS[p]
        if p == 0:
            locals_[10].wait()
        gain = gain_two_v[...]

        def chunk(r, carry):
            rows = pl.ds(pl.multiple_of(start + r * 32, 32), 32)
            here = pl.ds(pl.multiple_of(tp * H + start + r * 32, 32), 32)
            sums = resid[rows, :] + from_home[rows, :].astype(F32)
            sums = sums + mate_sum[rows, :].astype(F32)
            values = raw[0, here, :].astype(F32) + sums
            resid[rows, :] = values
            normed[here, :] = scaled(values, gain)
            return carry

        lax.fori_loop(0, n // 32, chunk, 0)

    def half_product(k, plane):
        w_gate = s2[plane, :, :, :, pl.ds(128 * k, 128)].reshape(D // 2, 128)
        w_up = s2[plane, :, :, :, pl.ds(1408 + 128 * k, 128)].reshape(D // 2, 128)
        left = normed[:, pl.ds(pl.multiple_of(1024 * plane, 1024), 1024)]
        return jnp.dot(
            left, jnp.concatenate([w_gate, w_up], axis=1), preferred_element_type=F32
        )

    def pre(k):
        partial[k] = half_product(k, zl)

    def hide(k):
        both = partial[k] + half_product(k, 1 - zl)
        gate, up = both[:, :128], both[:, 128:]
        hidden[:, pl.ds(128 * k, 128)] = (gate / (1.0 + jnp.exp(-gate)) * up).astype(BF16)

    def down(step):
        plane = 1 - zl if step else zl

        def both(k, carry):
            cols = pl.ds(pl.multiple_of(1024 * plane + 256 * k, 256), 256)
            acc_b[...] = block(hidden[...], s3[plane, k].reshape(256, 1408)).astype(BF16)
            to_mate[:, cols] = acc_b[other, :]
            total[:, cols] = resid[:, cols] + 0.5 * acc_b[mine, :].astype(F32)
            return carry

        def theirs(k, carry):
            cols = pl.ds(pl.multiple_of(1024 * plane + 256 * k, 256), 256)
            w = s3[plane, k].reshape(256, 1408)
            to_mate[:, cols] = block(hidden[other, :], w).astype(BF16)
            return carry

        def ours(k, carry):
            cols = pl.ds(pl.multiple_of(1024 * plane + 256 * k, 256), 256)
            own = block(hidden[mine, :], s3[plane, k].reshape(256, 1408)).astype(BF16)
            total[:, cols] = resid[:, cols] + 0.5 * own.astype(F32)
            return carry

        if step == 0:
            for i, send in enumerate(sends):
                if send.kind == "mate":
                    outgoing(i).wait_send()
        lo, hi = ((0, 4), None, (0, 2), (2, 4), (0, 4))[step]
        lax.fori_loop(lo, hi, (both, None, theirs, theirs, ours)[step], 0)

    act = {
        "norm": norm, "mix": mix, "mate": mate, "sum": add_up, "home": home, "again": again,
        "pre": pre, "hide": hide, "down": down,
    }
    landed = set()
    for what, i in steps:
        if what == "start":
            send = sends[i]
            if send.kind == "part" and send.stage not in landed:
                landed.add(send.stage)
                for k in ready_of[send.stage]:
                    locals_[k].wait()
            outgoing(i).start()
        elif what == "wait":
            incoming(i).wait_recv()
        else:
            act[what](i)

    for i, send in enumerate(sends):
        if send.kind not in ("mate", "relay"):
            outgoing(i).wait_send()


def on_device(
    tokens, mix_gain, w_bgate, w_cgate, w_value, conv_taps, w_mixout, mlp_gain, w_gate, w_up, w_down
):
    count = len(all_sends())
    anywhere = pl.BlockSpec(memory_space=pl.ANY)
    total, came = pl.pallas_call(
        kernel,
        name="residual_block",
        out_shape=(pltpu.VMEM((H, D), F32), pltpu.VMEM((H, D), BF16)),
        in_specs=[anywhere] * 11,
        out_specs=(pl.BlockSpec(memory_space=pltpu.VMEM),) * 2,
        scratch_shapes=[
            *[pltpu.VMEM((2, 4, 4, 64, width), BF16) for width in WIDTHS],
            pltpu.VMEM((2, T, D), BF16),
            pltpu.VMEM((T, D), BF16),
            pltpu.VMEM((2, T, 512), BF16),
            *[pltpu.VMEM((H, D), BF16)] * 6,
            pltpu.VMEM((H, D), F32),
            pltpu.VMEM((11, T, 256), F32),
            pltpu.VMEM((T, 1408), BF16),
            pltpu.VMEM((1, D), F32),
            pltpu.VMEM((3, D), F32),
            pltpu.VMEM((1, D), F32),
            pltpu.VMEM((T, 256), BF16),
            pltpu.VMEM((T, 256), BF16),
            pltpu.SemaphoreType.DMA((11,)),
            pltpu.SemaphoreType.DMA((count,)),
            pltpu.SemaphoreType.DMA((count,)),
        ],
        compiler_params=pltpu.CompilerParams(
            collective_id=0, has_side_effects=True, vmem_limit_bytes=60 * 2**20
        ),
    )(
        tokens, mix_gain[None], w_bgate, w_cgate, w_value, conv_taps, w_mixout.T,
        mlp_gain[None], w_gate, w_up, w_down.T,
    )
    return (total + 0.5 * came.astype(F32)).astype(BF16)


def solution(mesh):
    finer = Mesh(
        mesh.devices.reshape(mesh.shape["rep"], 2, 4, 4, mesh.shape["tp"]),
        ("rep", "fs_0", "fs_1", "fs_2", "tp"),
    )
    return jax.shard_map(
        on_device,
        mesh=finer,
        in_specs=(
            P(REP_FS_TP, None),
            P(),
            P(FS, "tp"),
            P(FS, "tp"),
            P(FS, "tp"),
            P(),
            P("tp", FS),
            P(),
            P(FS, "tp"),
            P(FS, "tp"),
            P("tp", FS),
        ),
        out_specs=P(REP_FS_TP, None),
        check_vma=False,
    )
```

```python
import heapq

import jax
import jax.numpy as jnp
from jax import lax
from jax.experimental import pallas as pl
from jax.experimental.pallas import tpu as pltpu
from jax.sharding import Mesh
from jax.sharding import PartitionSpec as P

FS = ("fs_0", "fs_1", "fs_2")
REP_FS_TP = ("rep", "fs_0", "fs_1", "fs_2", "tp")
MESH = pl.DeviceIdType.MESH
BF16, F32 = jnp.bfloat16, jnp.float32

D = 2048
T = 640
H = 320
WIDTHS = (1536, 512, 2816, 1408)
LINK = 45.1e3
PAIR = 500.0e3
LATENCY = 3.4
PAIR_LATENCY = 1.8
BACKLOG = 2.95
HOLD = 0.0

RANKS = (
    -2, -2, -2, -2, -3, -4, -4, -4, -4, 0, 88, 187, 1590, 957, 1545, 184, 423, 493, 24, 812,
    36, 637, 1224, 670, 757, 0, 0, 0, 0, 68, 0, 691, 400, 571, 1576, 633, 600, 1738, 120, 0,
    0, 0, 358, 0, 0, 561, 776, 42, 671, 530, 474, 348, 108, 229, 889, 531, 168, 852, 1144,
    819, 31, 0, 366, 555, 1355, 821, 409, 1017, 1145, 1346, 1295, 2765, 1203, 382, 1016, 608,
    553, 920, 1731, 1495, 1297, 624, 879, 366, 595, 2046, 412, 957, 776, 873, 1105, 1602,
    1168, 1061, 1407, 0, 1342, 849, 292, 650, 1034, 1494, 964, 1239, 988, 834, 654, 858, 177,
    976, 1513, 1131, 0, 732, 669, 727, 248, 1074, 687, 1048, 1010, 1056, 1644, -4, -4, -4, -4,
    -4, -4, -4, -4, -4, 1832, 2023, 1566, 2106, 2229, 2086, 2079, 2213, 2709, 2195, 3090,
    2502, 1936, 1397, 2530, 3318, 1319, 1669, 1282, 1291, 1180, 1451, 2163, 2091, 2290, 2416,
    3194, 2408, 2621, 2022, 2447, 2862, 1054, 1191, 2081, 1579, 1751, 1318, 2660, 1630, 2416,
    2667, 1884, 2554, 2715, 1209, 829, 1283, 1872, 1569, 2177, 1888, 2460, 2398, 1997, 1737,
    2884, 1606, 1381, 2229, 1643, 2400, 3414, 2461, 2657, 3025, 2783, 5092, 4152, 4053, 4506,
    4593, 4308, 3832, 1437, 2203, 1824, 3287, 2864, 4034, 3451, 2958, 3064, 4362, 4200, 4078,
    4107, 2520, 1039, 1527, 3538, 2839, 3301, 3279, 1794, 2685, 4717, 3921, 2142, 4068, 1247,
    2118, 1921, 2860, 3493, 3912, 3426, 2120, 2597, 4884, 2976, 2666, 4244,
)

SPANS = ((0, 160), (160, 96), (256, 64))

ALL = ("all",)
ME = ("rel", 0)


def half(k):
    return ("half", k)


def rel(k):
    return ("rel", k)


class Send:
    def __init__(self, kind, way, needs, rank, size, stage=None, quarter=None, at=None, index=None):
        self.kind, self.way, self.needs, self.rank = kind, way, needs, rank
        self.stage, self.quarter, self.at, self.index = stage, quarter, at, index
        self.time = size / (PAIR if way == "pair" else LINK)
        self.latency = PAIR_LATENCY if way == "pair" else LATENCY


def all_sends():
    out = []

    def add(quarter, way, at, needs, rank, pieces):
        at = {"z": ME, "y": ME, "x": ME} | at
        size = pieces * 16 * WIDTHS[stage] * 2
        send = Send("part", way, list(needs), rank, size, stage, quarter, at)
        out.append(send)
        return send

    def other(kind, way, needs, rank, size, index, stage=None):
        send = Send(kind, way, list(needs), rank, size, stage, None, None, index)
        out.append(send)
        return send

    row = D * 2
    for p in range(2):
        token = other("token", "zw", [], -2, 160 * row, p)
        other("relay", "pair", [token], -2, 160 * row, p)
    other("swap", "pair", [], -3, H * row, 0)
    for j in range(2):
        other("mate", "pair", [("mate", j)], -4, H * 1024 * 2, j)
        other("home", "pair", [("home", j)], -4, H * 1024 * 2, j)

    for stage in range(2):
        base = 10 * stage
        orders = (("x", "y"), ("x", "y"), ("y", "x"), ("y", "x"))
        for quarter, (first, second) in enumerate(orders):
            if quarter == 3:
                over = [add(quarter, "zd", {}, [], base, 1)]
                for far in range(2):
                    if far and stage == 0:
                        first, second = second, first
                    z = {"z": rel(far)}
                    start = over if far else []
                    plus = add(quarter, first + "+", z, start, base + far, 1)
                    minus = add(quarter, first + "-", z, start, base + far, 1)
                    if far:
                        on = add(quarter, first + "-", z | {first: rel(1)}, [minus], base + 2, 1)
                    else:
                        on = add(quarter, first + "+", z | {first: rel(-1)}, [plus], base + 2, 1)
                    line = [plus, minus, on] + start
                    z = z | {first: ALL}
                    plus = add(quarter, second + "+", z, line, base + 3, 4)
                    minus = add(quarter, second + "-", z, line, base + 3, 4)
                    z = {"z": rel(far)}
                    on, back = z | {second: rel(-1)}, z | {second: rel(1)}
                    add(quarter, second + "+", on | {first: half(0)}, [plus], base + 4, 2)
                    add(quarter, second + "-", back | {first: half(1)}, [minus], base + 4, 2)
                continue
            forth, back = first + "+", first + "-"
            plus = add(quarter, forth, {}, [], base, 1)
            minus = add(quarter, back, {}, [], base, 1)
            if quarter == 1:
                on = add(quarter, back, {first: rel(1)}, [minus], base + 1, 1)
            else:
                on = add(quarter, forth, {first: rel(-1)}, [plus], base + 1, 1)
            line = [plus, minus, on]
            over = [
                add(quarter, "zd", {first: rel(k)}, needs, base + 1, 1)
                for k, needs in ((0, []), (-1, [plus]), (1, [minus]), (2, [on]))
            ]
            forth, back = second + "+", second + "-"
            if quarter == 0:
                pa = add(quarter, forth, {first: half(0)}, line, base + 2, 2)
                pb = add(quarter, forth, {first: half(1)}, line, base + 3, 2)
                ma = add(quarter, back, {first: half(1)}, line, base + 2, 2)
                mb = add(quarter, back, {first: half(0)}, line, base + 3, 2)
                po = add(quarter, forth, {first: half(0), second: rel(-1)}, [pa], base + 4, 2)
                mo = add(quarter, back, {first: half(1), second: rel(1)}, [ma], base + 4, 2)
                add(quarter, "zd", {first: ALL, second: rel(-1)}, [pa, pb], base + 5, 4)
                add(quarter, "zd", {first: ALL, second: rel(1)}, [ma, mb], base + 5, 4)
                final = "zw" if stage == 3 else "zd"
                add(quarter, final, {first: ALL, second: rel(2)}, [po, mo], base + 6, 4)
            else:
                here, there = {first: ALL}, {first: ALL, "z": rel(1)}
                ph = add(quarter, forth, here, line, base + 3, 4)
                add(quarter, back, here, line, base + 3, 4)
                add(quarter, forth, there, over, base + 4, 4)
                mt = add(quarter, back, there, over, base + 4, 4)
                add(quarter, forth, here | {second: rel(-1)}, [ph], base + 5, 4)
                add(quarter, back, there | {second: rel(1)}, [mt], base + 5, 4)
    for j, (_, n) in enumerate(SPANS):
        other("sum", "zw", [("sum", j)], -4, n * row, j)
        other("again", "pair", [("again", j)], -4, n * row, j)
    for j, step in enumerate((0, 2, 3)):
        other("down", "pair", [("down", step)], -4, H * (512 if j else 1024) * 2, j)
    orders = (("x", "y"), ("y", "x"), ("x", "y"), ("y", "x"))
    for stage in range(2, 4):
        base = 20 + 10 * (stage - 2)
        early = 14 + 8 * (stage - 2)
        wrap = "zw" if stage == 2 else "zd"
        for quarter, (first, second) in enumerate(orders):
            forth, back = first + "+", first + "-"
            plus = add(quarter, forth, {}, [], early, 1)
            minus = add(quarter, back, {}, [], early, 1)
            if quarter < 2:
                on = add(quarter, forth, {first: rel(-1)}, [plus], early, 1)
            else:
                on = add(quarter, back, {first: rel(1)}, [minus], early, 1)
            line = [plus, minus, on]
            forth, back = second + "+", second + "-"
            if quarter < 4 - stage:
                pa = add(quarter, forth, {first: half(0)}, line, base + 2, 2)
                pb = add(quarter, forth, {first: half(1)}, line, base + 3, 2)
                ma = add(quarter, back, {first: half(1)}, line, base + 2, 2)
                mb = add(quarter, back, {first: half(0)}, line, base + 3, 2)
                po = add(quarter, forth, {first: half(0), second: rel(-1)}, [pa], base + 4, 2)
                mo = add(quarter, back, {first: half(1), second: rel(1)}, [ma], base + 4, 2)
                add(quarter, "zw", {}, [], early, 1)
                add(quarter, "zw", {first: rel(-1)}, [plus], early, 1)
                add(quarter, "zw", {first: rel(1)}, [minus], early, 1)
                add(quarter, "zw", {first: rel(2)}, [on], early, 1)
                soon = "zw" if stage == 2 and quarter == 0 else "zd"
                add(quarter, soon, {first: ALL, second: rel(-1)}, [pa, pb], base + 5, 4)
                add(quarter, "zd", {first: ALL, second: rel(1)}, [ma, mb], base + 5, 4)
                final = "zw" if stage == 3 else "zd"
                add(quarter, final, {first: ALL, second: rel(2)}, [po, mo], base + 6, 4)
            else:
                over = [
                    add(quarter, way, {first: rel(k)}, needs, base + 2, 1)
                    for way, k, needs in (
                        (wrap, 0, []), (wrap, -1, [plus]), ("zd", 1, [minus]), (wrap, 2, [on])
                    )
                ]
                here, there = {first: ALL}, {first: ALL, "z": rel(1)}
                ph = add(quarter, forth, here, line, base + 3, 4)
                add(quarter, back, here, line, base + 3, 4)
                add(quarter, forth, there, over, base + 4, 4)
                mt = add(quarter, back, there, over, base + 4, 4)
                add(quarter, forth, here | {second: rel(-1)}, [ph], base + 5, 4)
                add(quarter, back, there | {second: rel(1)}, [mt], base + 5, 4)
    return out


def near(send):
    return (send.way[0] == "z") == (send.at["z"] != ME)


def work_list(sends):
    def kind(name, *index):
        return [s for s in sends if s.kind == name and (not index or s.index in index)]

    def stage(k):
        return [s for s in sends if s.stage == k]

    last = stage(3)
    out = [("norm", k, 1.0, kind("swap")) for k in range(4)]
    out += [("norm", k, 1.0, kind("token") + kind("relay")) for k in range(4, 8)]
    out += [("mix", k, 1.3 if k % 3 == 2 else 0.7, stage(0)) for k in range(6)]
    out += [("mate", k, 1.0, stage(1)) for k in range(2)]
    out += [("sum", k, n / 230, kind("mate")) for k, (_, n) in enumerate(SPANS)]
    out += [("mix", k, 1.3 if k % 3 == 2 else 0.7, []) for k in range(6, 12)]
    out += [("home", k, 1.0, []) for k in range(2)]
    for k, (_, n) in enumerate(SPANS):
        out.append(("again", k, n / 115, kind("home") + kind("sum", k)))
    out += [("pre", k, 0.4, kind("again") + [s for s in stage(2) if near(s)]) for k in range(11)]
    out += [("hide", k, 0.42, stage(2)) for k in range(11)]
    out += [("down", 0, 2.1, [s for s in last if near(s)])]
    out += [("down", k, 1.5 if k == 4 else 0.75, last) for k in range(2, 5)]
    return out


def plan(ranks=RANKS):
    sends = all_sends()
    if ranks:
        for send, rank in zip(sends, ranks, strict=True):
            send.rank = rank
    work = work_list(sends)
    number = {id(send): i for i, send in enumerate(sends)}
    followers, missing = {}, []
    for i, send in enumerate(sends):
        missing.append(len(send.needs))
        for need in send.needs:
            key = need if isinstance(need, tuple) else number[id(need)]
            followers.setdefault(key, []).append(i)
    ready = {send.way: [] for send in sends}
    free = dict.fromkeys(ready, 0.0)
    got, flying, steps, held, now = set(), [], [], [], 0.0

    def release(i):
        if sends[i].kind == "part" and sends[i].stage > 1 and now < HOLD:
            held.append(i)
        else:
            heapq.heappush(ready[sends[i].way], (sends[i].rank, i))

    def arrive(key):
        got.add(key)
        for i in followers.get(key, ()):
            missing[i] -= 1
            if missing[i] == 0:
                release(i)

    def top_up():
        if now >= HOLD:
            while held:
                release(held.pop())
        for way, queue in ready.items():
            while queue and (queue[0][0] < 0 or free[way] - now <= BACKLOG):
                i = heapq.heappop(queue)[1]
                free[way] = max(free[way], now) + sends[i].time
                heapq.heappush(flying, (free[way] + sends[i].latency, i))
                steps.append(("start", i))

    for i, count in enumerate(missing):
        if count == 0:
            release(i)
    top_up()
    step = 0
    needs = [[number[id(need)] for need in piece[3]] for piece in work]
    while flying or step < len(work):
        while flying and flying[0][0] <= now:
            i = heapq.heappop(flying)[1]
            steps.append(("wait", i))
            arrive(i)
            top_up()
        if step < len(work) and got.issuperset(needs[step]):
            name, j, time, _ = work[step]
            step += 1
            steps.append((name, j))
            now += time
            arrive((name, j))
            top_up()
        elif flying:
            now = max(now, flying[0][0])
    return sends, eager(sends, steps, work, number), now


def eager(sends, steps, work, number):
    queues, followed, pieces = {}, set(), {(piece[0], piece[1]): piece for piece in work}
    for what, i in steps:
        if what == "start":
            queues.setdefault(sends[i].way, []).append(i)
    needs = {}
    for i, send in enumerate(sends):
        needs[i] = [n if isinstance(n, tuple) else number[id(n)] for n in send.needs]
        followed.update(needs[i])
    out, got = [], set()

    def start_all():
        for queue in queues.values():
            while queue and got.issuperset(needs[queue[0]]):
                out.append(("start", queue.pop(0)))

    def wait_for(i):
        if i not in got:
            got.add(i)
            out.append(("wait", i))
            start_all()

    start_all()
    for what, i in steps:
        if what == "wait" and i in followed:
            wait_for(i)
        elif what not in ("start", "wait"):
            for need in pieces[what, i][3]:
                wait_for(number[id(need)])
            out.append((what, i))
            got.add((what, i))
            start_all()
    for i in range(len(sends)):
        wait_for(i)
    return out


def region(send, place):
    at = []
    for dim, extent in (("z", 2), ("y", 4), ("x", 4)):
        how = send.at[dim]
        if how == ALL:
            at.append(pl.ds(0, extent))
        elif how[0] == "half":
            at.append(pl.ds(2 * how[1], 2))
        else:
            at.append(pl.ds(lax.rem(place[dim] + how[1] + extent, extent), 1))
    return (*at, pl.ds(16 * send.quarter, 16), pl.ds(0, WIDTHS[send.stage]))


def kernel(
    tokens, gain_one, w_b, w_c, w_v, taps, w_mix, gain_two, w_g, w_u, w_d, total, came_two,
    s0, s1, s2, s3, raw, normed, gated, to_mate, from_mate, summed, mate_sum, to_home, from_home,
    resid, partial, hidden, gain_v, taps_v, gain_two_v, acc_b, acc_c, local_sem, send_sem, recv_sem,
):
    sends, steps, _ = plan()
    buffers = (s0, s1, s2, s3)
    rep, zl, y, x, tp = (lax.axis_index(name) for name in REP_FS_TP)
    me = {"z": zl, "y": y, "x": x}

    def device(way):
        if way == "pair":
            return (rep, zl, y, x, 1 - tp)
        if way == "zd":
            return (rep, 1 - zl, y, x, tp)
        if way == "zw":
            return (1 - rep, 1 - zl, y, x, tp)
        step = 1 if way[1] == "+" else 3
        if way[0] == "x":
            return (rep, zl, y, lax.rem(x + step, 4), tp)
        return (rep, zl, lax.rem(y + step, 4), x, tp)

    def rows_of(core, start=0, n=H):
        return pl.ds(pl.multiple_of(core * H + start, 32), n)

    mine, other = rows_of(tp), rows_of(1 - tp)

    def local(k, src, dst):
        return pltpu.make_async_copy(src, dst, local_sem.at[k])

    def slot(buffer, lo, n):
        return buffer.at[zl, y, x, pl.ds(0, 64), pl.ds(lo, n)]

    def share(weight):
        return weight.at[:, pl.ds(pl.multiple_of(rep * 512, 512), 512)]

    locals_ = [
        local(0, share(w_b), slot(s0, 0, 512)),
        local(1, share(w_c), slot(s0, 512, 512)),
        local(2, share(w_v), slot(s0, 1024, 512)),
        local(3, share(w_mix), slot(s1, 0, 512)),
        local(4, w_g, slot(s2, 0, 1408)),
        local(5, w_u, slot(s2, 1408, 1408)),
        local(6, w_d, slot(s3, 0, 1408)),
        local(7, tokens, raw.at[0, mine, :]),
        local(8, gain_one, gain_v),
        local(9, taps, taps_v),
        local(10, gain_two, gain_two_v),
    ]
    ready_of = ((0, 1, 2), (3,), (4, 5), (6,))
    for copy in locals_:
        copy.start()

    barrier = pltpu.get_barrier_semaphore()
    ways = ("x+", "x-", "y+", "y-", "zd", "zw", "pair")
    for way in ways:
        pl.semaphore_signal(barrier, inc=1, device_id=device(way), device_id_type=MESH)
    pl.semaphore_wait(barrier, len(ways))

    def ends(send, place, core):
        j = send.index
        cols = None if j is None else pl.ds(1024 * (j % 2), 1024)
        if send.kind == "part":
            where = buffers[send.stage].at[region(send, place)]
            return where, where
        if send.kind == "token":
            return tokens.at[pl.ds(160 * j, 160), :], raw.at[1, rows_of(core, 160 * j, 160), :]
        if send.kind == "relay":
            where = raw.at[1, rows_of(core, 160 * j, 160), :]
            return where, where
        if send.kind == "swap":
            return tokens, raw.at[0, rows_of(core), :]
        if send.kind == "mate":
            return to_mate.at[:, cols], from_mate.at[:, cols]
        if send.kind == "sum":
            rows = pl.ds(*SPANS[j])
            return summed.at[rows, :], mate_sum.at[rows, :]
        if send.kind == "home":
            return to_home.at[:, cols], from_home.at[:, cols]
        if send.kind == "again":
            where = normed.at[rows_of(core, *SPANS[j]), :]
            return where, where
        start = 1024 * lax.rem(place["z"] + (j > 0), 2) + (512 if j == 2 else 0)
        lanes = pl.ds(pl.multiple_of(start, 512), 512 if j else 1024)
        return to_mate.at[:, lanes], came_two.at[:, lanes]

    def copy_of(i, place, core):
        src, dst = ends(sends[i], place, core)
        return pltpu.make_async_remote_copy(
            src_ref=src, dst_ref=dst, send_sem=send_sem.at[i], recv_sem=recv_sem.at[i],
            device_id=device(sends[i].way), device_id_type=MESH,
        )

    def outgoing(i):
        return copy_of(i, me, tp)

    def incoming(i):
        way, place = sends[i].way, dict(me)
        if way in ("zd", "zw"):
            place["z"] = 1 - zl
        elif way != "pair":
            place[way[0]] = lax.rem(me[way[0]] + (3 if way[1] == "+" else 1), 4)
        return copy_of(i, place, 1 - tp if way == "pair" else tp)

    def scaled(values, gain):
        factor = lax.rsqrt(jnp.mean(values * values, axis=-1, keepdims=True) + 1e-06)
        return (values * factor * gain).astype(BF16)

    def norm(step):
        c, part = step // 4, step % 4
        if step == 0:
            locals_[7].wait()
            locals_[8].wait()
        if step == 4:
            for i, send in enumerate(sends):
                if send.kind == "relay":
                    outgoing(i).wait_send()
        gain = gain_v[...]

        def chunk(r, carry):
            rows = pl.ds(pl.multiple_of(r * 32, 32), 32)
            values = scaled(raw[c, rows, :].astype(F32), gain)
            if c == 0:
                normed[rows, :] = values
            else:
                raw[c, rows, :] = values
            return carry

        lax.fori_loop(5 * part, 5 * part + 5, chunk, 0)

    def mix(step):
        c, j, k = 1 - step // 6, step // 3 % 2, step % 3
        if step == 0:
            locals_[9].wait()

        def dot(k):
            w = s0[:, :, :, :, pl.ds(512 * k + 256 * j, 256)].reshape(D, 256)
            left = raw[1] if c == 1 else normed[...]
            return jnp.dot(left, w, preferred_element_type=F32).astype(BF16)

        if k < 2:
            (acc_b, acc_c)[k][...] = dot(k)
            return
        mixed = acc_c[...].astype(F32) * dot(2).astype(F32)
        row = lax.broadcasted_iota(jnp.int32, (T, 256), 0)
        one = jnp.where(row >= 1, pltpu.roll(mixed, 1, 0), 0.0)
        two = jnp.where(row >= 2, pltpu.roll(mixed, 2, 0), 0.0)
        lanes = pl.ds(pl.multiple_of(tp * 1024 + rep * 512 + 256 * j, 256), 256)
        tap = [taps_v[pl.ds(k, 1), lanes] for k in range(3)]
        convolved = tap[0] * two + tap[1] * one + tap[2] * mixed
        gated[c, :, pl.ds(256 * j, 256)] = (acc_b[...].astype(F32) * convolved).astype(BF16)

    def block(left, right):
        return lax.dot_general(left, right, (((1,), (1,)), ((), ())), preferred_element_type=F32)

    def product(c, j, away):
        def one(k, carry):
            cols = pl.ds(pl.multiple_of(1024 * j + 256 * k, 256), 256)
            w = s1[j, k].reshape(256, 512)
            away[:, cols] = block(gated[c, other, :], w).astype(BF16)
            resid[:, cols] = block(gated[c, mine, :], w)
            return carry

        lax.fori_loop(0, 4, one, 0)

    def mate(j):
        product(1, j, to_mate)

    def home(j):
        product(0, j, to_home)

    def add_up(p):
        start, n = SPANS[p]

        def chunk(r, carry):
            rows = pl.ds(pl.multiple_of(start + r * 32, 32), 32)
            summed[rows, :] = (resid[rows, :] + from_mate[rows, :].astype(F32)).astype(BF16)
            return carry

        lax.fori_loop(0, n // 32, chunk, 0)

    def again(p):
        start, n = SPANS[p]
        if p == 0:
            locals_[10].wait()
        gain = gain_two_v[...]

        def chunk(r, carry):
            rows = pl.ds(pl.multiple_of(start + r * 32, 32), 32)
            here = pl.ds(pl.multiple_of(tp * H + start + r * 32, 32), 32)
            sums = resid[rows, :] + from_home[rows, :].astype(F32)
            sums = sums + mate_sum[rows, :].astype(F32)
            values = raw[0, here, :].astype(F32) + sums
            resid[rows, :] = values
            normed[here, :] = scaled(values, gain)
            return carry

        lax.fori_loop(0, n // 32, chunk, 0)

    def half_product(k, plane):
        w_gate = s2[plane, :, :, :, pl.ds(128 * k, 128)].reshape(D // 2, 128)
        w_up = s2[plane, :, :, :, pl.ds(1408 + 128 * k, 128)].reshape(D // 2, 128)
        left = normed[:, pl.ds(pl.multiple_of(1024 * plane, 1024), 1024)]
        return jnp.dot(
            left, jnp.concatenate([w_gate, w_up], axis=1), preferred_element_type=F32
        )

    def pre(k):
        partial[k] = half_product(k, zl)

    def hide(k):
        both = partial[k] + half_product(k, 1 - zl)
        gate, up = both[:, :128], both[:, 128:]
        hidden[:, pl.ds(128 * k, 128)] = (gate / (1.0 + jnp.exp(-gate)) * up).astype(BF16)

    def down(step):
        plane = 1 - zl if step else zl

        def both(k, carry):
            cols = pl.ds(pl.multiple_of(1024 * plane + 256 * k, 256), 256)
            acc_b[...] = block(hidden[...], s3[plane, k].reshape(256, 1408)).astype(BF16)
            to_mate[:, cols] = acc_b[other, :]
            total[:, cols] = resid[:, cols] + 0.5 * acc_b[mine, :].astype(F32)
            return carry

        def theirs(k, carry):
            cols = pl.ds(pl.multiple_of(1024 * plane + 256 * k, 256), 256)
            w = s3[plane, k].reshape(256, 1408)
            to_mate[:, cols] = block(hidden[other, :], w).astype(BF16)
            return carry

        def ours(k, carry):
            cols = pl.ds(pl.multiple_of(1024 * plane + 256 * k, 256), 256)
            own = block(hidden[mine, :], s3[plane, k].reshape(256, 1408)).astype(BF16)
            total[:, cols] = resid[:, cols] + 0.5 * own.astype(F32)
            return carry

        if step == 0:
            for i, send in enumerate(sends):
                if send.kind == "mate":
                    outgoing(i).wait_send()
        lo, hi = ((0, 4), None, (0, 2), (2, 4), (0, 4))[step]
        lax.fori_loop(lo, hi, (both, None, theirs, theirs, ours)[step], 0)

    act = {
        "norm": norm, "mix": mix, "mate": mate, "sum": add_up, "home": home, "again": again,
        "pre": pre, "hide": hide, "down": down,
    }
    def settle(which):
        for i, send in enumerate(sends):
            if which(send):
                outgoing(i).wait_send()

    landed = set()
    for what, i in steps:
        if what == "start":
            send = sends[i]
            if send.kind == "part" and send.stage not in landed:
                landed.add(send.stage)
                for k in ready_of[send.stage]:
                    locals_[k].wait()
            outgoing(i).start()
        elif what == "wait":
            incoming(i).wait_recv()
        else:
            act[what](i)
            if (what, i) == ("down", 0):
                settle(lambda s: s.kind not in ("mate", "relay", "down") and s.stage != 3)
            if (what, i) == ("down", 4):
                settle(lambda s: s.stage == 3)
    settle(lambda s: s.kind == "down")


def on_device(
    tokens, mix_gain, w_bgate, w_cgate, w_value, conv_taps, w_mixout, mlp_gain, w_gate, w_up, w_down
):
    count = len(all_sends())
    anywhere = pl.BlockSpec(memory_space=pl.ANY)
    total, came = pl.pallas_call(
        kernel,
        name="residual_block",
        out_shape=(pltpu.VMEM((H, D), F32), pltpu.VMEM((H, D), BF16)),
        in_specs=[anywhere] * 11,
        out_specs=(pl.BlockSpec(memory_space=pltpu.VMEM),) * 2,
        scratch_shapes=[
            *[pltpu.VMEM((2, 4, 4, 64, width), BF16) for width in WIDTHS],
            pltpu.VMEM((2, T, D), BF16),
            pltpu.VMEM((T, D), BF16),
            pltpu.VMEM((2, T, 512), BF16),
            *[pltpu.VMEM((H, D), BF16)] * 6,
            pltpu.VMEM((H, D), F32),
            pltpu.VMEM((11, T, 256), F32),
            pltpu.VMEM((T, 1408), BF16),
            pltpu.VMEM((1, D), F32),
            pltpu.VMEM((3, D), F32),
            pltpu.VMEM((1, D), F32),
            pltpu.VMEM((T, 256), BF16),
            pltpu.VMEM((T, 256), BF16),
            pltpu.SemaphoreType.DMA((11,)),
            pltpu.SemaphoreType.DMA((count,)),
            pltpu.SemaphoreType.DMA((count,)),
        ],
        compiler_params=pltpu.CompilerParams(
            collective_id=0, has_side_effects=True, vmem_limit_bytes=60 * 2**20
        ),
    )(
        tokens, mix_gain[None], w_bgate, w_cgate, w_value, conv_taps, w_mixout.T,
        mlp_gain[None], w_gate, w_up, w_down.T,
    )
    return (total + 0.5 * came.astype(F32)).astype(BF16)


def solution(mesh):
    finer = Mesh(
        mesh.devices.reshape(mesh.shape["rep"], 2, 4, 4, mesh.shape["tp"]),
        ("rep", "fs_0", "fs_1", "fs_2", "tp"),
    )
    return jax.shard_map(
        on_device,
        mesh=finer,
        in_specs=(
            P(REP_FS_TP, None),
            P(),
            P(FS, "tp"),
            P(FS, "tp"),
            P(FS, "tp"),
            P(),
            P("tp", FS),
            P(),
            P(FS, "tp"),
            P(FS, "tp"),
            P("tp", FS),
        ),
        out_specs=P(REP_FS_TP, None),
        check_vma=False,
    )
```
